128 devices in a mesh: sp: 64 (over z, y, x), tp: 2 (over core).
Axes of the slice: x: 4, y: 4, z: 4, core: 2. Of those that a mesh axis runs over, the one named last changes fastest.
Arguments:
- tokens: bfloat16 [24576, 2048], P(('sp', 'tp')), may hold values from -6 to 6
- norm_gain: float32 [2048], replicated, may hold values from 0.1 to 1.9
- w_query: bfloat16 [2048, 1024], P(None, 'tp'), may hold values from -0.125 to 0.125
- w_key: bfloat16 [2048, 1024], P(None, 'tp'), may hold values from -0.125 to 0.125
- w_value: bfloat16 [2048, 2048], P(None, 'tp'), may hold values from -0.125 to 0.125
- w_ogate: bfloat16 [2048, 2048], P(None, 'tp'), may hold values from -0.125 to 0.125
- w_igate: bfloat16 [2048, 8], replicated, may hold values from -0.125 to 0.125
- w_fgate: bfloat16 [2048, 8], replicated, may hold values from -0.125 to 0.125
- conv_query: bfloat16 [4, 1024], replicated, may hold values from -3 to 3
- conv_key: bfloat16 [4, 1024], replicated, may hold values from -3 to 3
- gate_offset: float32 [2, 192, 8], P(None, 'sp', 'tp'), may hold values from -60 to 140, as said below
- head_gain: float32 [2048], replicated, may hold values from 0.1 to 1.9
- w_out: bfloat16 [2048, 2048], P('tp'), may hold values from -0.125 to 0.125
Outputs:
- mixed: bfloat16 [24576, 2048], P(('sp', 'tp'))
The draws below stay inside these ranges and needn't reach their ends.
Inputs may be any that keep to these rules, and one draw needn't show every extreme that they name: `gate_offset`: row 0 is added to the input gate's pre-activation and row 1 to the forget gate's; each entry holds for one block of 128 positions and one head.
All inputs are finite; a program needn't handle non-finite values.
Results may differ from the reference program's by a relative error of at most 0.011.
Values may be sent and summed in bfloat16 or wider, within the bound.
No kernel may reach another device: no remote copies, remote signals or barrier semaphores. Data moves between devices by JAX's collectives and lax.ppermute only.
A program may use at most 128 MiB of HBM per device.

```python
import math
import jax
import jax.numpy as jnp
from jax import lax

D = 2048
HEADS = 8
DQK = 128
DV = 256
CONV = 4
SPAN = 128
TOKENS = 24576
SPANS = 192


def draw_gate_offset(key, part):
    seeds = jax.random.split(jax.random.fold_in(key, 7), 4)
    ranking = jax.random.permutation(seeds[0], HEADS)
    slow_heads = ranking < HEADS // 2
    inputs = jax.random.uniform(seeds[3], (SPANS, HEADS), jnp.float32, -3.0, 1.0)
    fast_level = jax.random.uniform(seeds[1], (HEADS,), jnp.float32, 3.5, 4.5)
    level_base = jnp.where(slow_heads, math.log(TOKENS) + 1.0, fast_level)
    wiggle = jax.random.uniform(seeds[2], (SPANS, HEADS), jnp.float32, -0.7, 0.7)
    return jnp.stack([inputs, level_base[None, :] + wiggle]).astype(jnp.float32)


def level_of(rng, extent, pieces, least, largest):
    loudness, own = 1.0, jax.random.fold_in(rng, 6)
    for dim, shards_of in pieces:
        heights = jnp.exp(jax.random.uniform(jax.random.fold_in(own, dim), (shards_of,), jnp.float32, least / len(pieces), largest / len(pieces)))
        loudness = loudness * jnp.repeat(heights, extent[dim] // shards_of).reshape([-1 if axis == dim else 1 for axis in range(len(extent))])
    return loudness


def noise(rng, dims, scale, bound, pieces=(), held_as=jnp.bfloat16):
    gain = level_of(rng, dims, pieces, -0.22, 0.18) if pieces else 1.0
    drawn = jax.random.normal(rng, dims, jnp.float32) * scale * gain
    return jnp.minimum(jnp.maximum(drawn, -bound), bound).astype(held_as)


def setup_inputs(seed: int = 0) -> dict:
    key_of = jax.random.split(jax.random.key(seed), 14)
    tokens = noise(key_of[0], (TOKENS, D), 1.0, 6.0, ((0, 128),))
    norm_gain = jnp.clip(1.0 + 0.18 * jax.random.normal(key_of[1], (D,), jnp.float32), 0.1, 1.9)
    w_query = noise(key_of[2], (D, HEADS * DQK), D ** -0.5, 0.125, ((1, 2),))
    w_key = noise(key_of[3], (D, HEADS * DQK), D ** -0.5, 0.125, ((1, 2),))
    w_value = noise(key_of[4], (D, HEADS * DV), D ** -0.5, 0.125, ((1, 2),))
    w_ogate = noise(key_of[5], (D, HEADS * DV), D ** -0.5, 0.125, ((1, 2),))
    w_igate = noise(key_of[6], (D, HEADS), D ** -0.5, 0.125)
    w_fgate = noise(key_of[7], (D, HEADS), D ** -0.5, 0.125)
    conv_query = noise(key_of[8], (CONV, HEADS * DQK), CONV ** -0.5, 3.0)
    conv_key = noise(key_of[9], (CONV, HEADS * DQK), CONV ** -0.5, 3.0)
    gate_offset = draw_gate_offset(jax.random.fold_in(key_of[13], 71), 0)
    head_gain = jnp.clip(1.0 + 0.18 * jax.random.normal(key_of[11], (HEADS * DV,), jnp.float32), 0.1, 1.9)
    w_out = noise(key_of[12], (HEADS * DV, D), (HEADS * DV) ** -0.5, 0.125, ((0, 2),))
    return {"tokens": tokens, "norm_gain": norm_gain, "w_query": w_query, "w_key": w_key, "w_value": w_value, "w_ogate": w_ogate, "w_igate": w_igate, "w_fgate": w_fgate, "conv_query": conv_query, "conv_key": conv_key, "gate_offset": gate_offset, "head_gain": head_gain, "w_out": w_out}


EPS = 1e-06
HIGHEST = lax.Precision.HIGHEST

def normalize_rows(values, gain_vec):
    widened = values.astype(jnp.float32)
    scaled = widened * lax.rsqrt(lax.optimization_barrier(jnp.mean(widened * widened, axis=-1, keepdims=True)) + EPS)
    return (scaled * gain_vec.astype(jnp.float32)).astype(jnp.bfloat16)

def causal_mix(values, weight):
    tap_count = weight.shape[0]
    seq_len = values.shape[0]
    leading = jnp.zeros((tap_count - 1, values.shape[1]), values.dtype)
    padded = jnp.concatenate([leading, values], axis=0).astype(jnp.float32)
    mixed_sum = jnp.zeros((seq_len, values.shape[1]), jnp.float32)
    for tap_index in range(tap_count):
        mixed_sum = mixed_sum + weight[tap_index].astype(jnp.float32) * padded[tap_index:tap_index + seq_len]
    return mixed_sum

def block_step(carried, inputs):
    states, norm_vec, levels = carried
    query_blk, key_blk, value_blk, gate_blk, forget_blk = inputs
    cumulative = jnp.cumsum(forget_blk, axis=0).T
    gate_rows = gate_blk.T
    span_len = cumulative.shape[1]
    causal = jnp.tril(jnp.ones((span_len, span_len), dtype=bool))
    log_weight = jnp.where(causal[None], cumulative[:, :, None] - cumulative[:, None, :] + gate_rows[:, None, :], -jnp.inf)
    carried_log = cumulative + levels[:, None]
    running_top = jnp.maximum(carried_log, lax.optimization_barrier(jnp.max(log_weight, axis=-1)))
    inner_weight = jnp.exp(log_weight - running_top[:, :, None])
    carried_scale = jnp.exp(carried_log - running_top)
    query_wide = query_blk.astype(jnp.float32)
    key_wide = key_blk.astype(jnp.float32)
    scores = jnp.einsum('thd,shd->hts', query_wide, key_wide, precision=HIGHEST) * inner_weight
    scores_low = lax.optimization_barrier(scores.astype(jnp.bfloat16)).astype(jnp.float32)
    numerator = carried_scale[:, :, None] * jnp.einsum('thd,hde->hte', query_wide, states, precision=HIGHEST)
    numerator = numerator + jnp.einsum('hts,she->hte', scores_low, value_blk.astype(jnp.float32), precision=HIGHEST)
    denominator = carried_scale * jnp.einsum('thd,hd->ht', query_wide, norm_vec, precision=HIGHEST) + lax.optimization_barrier(jnp.sum(scores, axis=-1))
    cell_out = numerator / jnp.maximum(jnp.abs(denominator), jnp.exp(-running_top))[:, :, None]
    last_log = cumulative[:, -1]
    write_log = last_log[:, None] - cumulative + gate_rows
    new_levels = jnp.maximum(last_log + levels, lax.optimization_barrier(jnp.max(write_log, axis=-1)))
    decay_scale = jnp.exp(last_log + levels - new_levels)
    write_weight = jnp.exp(write_log - new_levels[:, None])
    weighted = write_weight.T[:, :, None] * key_wide
    weighted_low = lax.optimization_barrier(weighted.astype(jnp.bfloat16)).astype(jnp.float32)
    new_states = decay_scale[:, None, None] * states + jnp.einsum('shd,she->hde', weighted_low, value_blk.astype(jnp.float32), precision=HIGHEST)
    new_norm = decay_scale[:, None] * norm_vec + lax.optimization_barrier(jnp.sum(weighted, axis=0))
    return ((new_states, new_norm, new_levels), jnp.transpose(cell_out, (1, 0, 2)))

def reference(tokens, norm_gain, w_query, w_key, w_value, w_ogate, w_igate, w_fgate, conv_query, conv_key, gate_offset, head_gain, w_out):
    normed = normalize_rows(tokens, norm_gain)
    query_pre = jnp.dot(normed, w_query, preferred_element_type=jnp.float32).astype(jnp.bfloat16)
    key_pre = jnp.dot(normed, w_key, preferred_element_type=jnp.float32).astype(jnp.bfloat16)
    value_pre = jnp.dot(normed, w_value, preferred_element_type=jnp.float32).astype(jnp.bfloat16)
    ogate_pre = jnp.dot(normed, w_ogate, preferred_element_type=jnp.float32).astype(jnp.bfloat16)
    input_pre = jnp.dot(normed, w_igate, preferred_element_type=jnp.float32)
    forget_pre = jnp.dot(normed, w_fgate, preferred_element_type=jnp.float32)
    input_gate = input_pre + jnp.repeat(gate_offset[0], SPAN, axis=0)
    log_forget = jax.nn.log_sigmoid(forget_pre + jnp.repeat(gate_offset[1], SPAN, axis=0))
    query_rows = jax.nn.silu(causal_mix(query_pre, conv_query)).astype(jnp.bfloat16).reshape(TOKENS, HEADS, DQK)
    key_rows = (jax.nn.silu(causal_mix(key_pre, conv_key)) * DQK ** (-0.5)).astype(jnp.bfloat16).reshape(TOKENS, HEADS, DQK)
    value_rows = value_pre.reshape(TOKENS, HEADS, DV)
    blocks = TOKENS // SPAN
    blocked = (query_rows.reshape(blocks, SPAN, HEADS, DQK), key_rows.reshape(blocks, SPAN, HEADS, DQK), value_rows.reshape(blocks, SPAN, HEADS, DV), input_gate.reshape(blocks, SPAN, HEADS), log_forget.reshape(blocks, SPAN, HEADS))
    initial = (jnp.zeros((HEADS, DQK, DV), jnp.float32), jnp.zeros((HEADS, DQK), jnp.float32), jnp.zeros((HEADS,), jnp.float32))
    _, cell_blocks = lax.scan(block_step, initial, blocked)
    cell_out = cell_blocks.reshape(TOKENS, HEADS, DV)
    cell_out = cell_out * lax.rsqrt(lax.optimization_barrier(jnp.mean(cell_out * cell_out, axis=-1, keepdims=True)) + EPS)
    hidden = cell_out.reshape(TOKENS, HEADS * DV) * head_gain.astype(jnp.float32) * jax.nn.sigmoid(ogate_pre.astype(jnp.float32))
    hidden = hidden.astype(jnp.bfloat16)
    return jnp.dot(hidden, w_out, preferred_element_type=jnp.float32).astype(jnp.bfloat16)
```

```python
import functools

import jax
import jax.numpy as jnp
from jax import lax
from jax.experimental import pallas as pl
from jax.experimental.pallas import tpu as pltpu
from jax.sharding import Mesh
from jax.sharding import PartitionSpec as P

SPAN = 128
SP = ("sp_0", "sp_1", "sp_2")
SP_TP = ("sp_0", "sp_1", "sp_2", "tp")
EPS = 1e-06
EMPTY = -1e30
TAIL = 16
HEADS = 4
DQK = 128
DV = 256
WIDTH = DV + 128
BLOCKS = 3
ROWS = BLOCKS * SPAN
HALF = ROWS // 2
HIGHEST = lax.Precision.HIGHEST
BF = jnp.bfloat16
F32 = jnp.float32
MIB = 1 << 20


def in_vmem():
    return pl.BlockSpec(memory_space=pltpu.VMEM)


def in_hbm():
    return pl.BlockSpec(memory_space=pl.ANY)


def call(kernel, outs, ins, scratch=(), flops=0, limit=40):
    return pl.pallas_call(
        kernel,
        out_shape=outs,
        in_specs=ins,
        out_specs=jax.tree.map(lambda _: in_vmem(), outs),
        scratch_shapes=list(scratch),
        cost_estimate=pl.CostEstimate(flops=flops, transcendentals=0, bytes_accessed=1 << 20),
        compiler_params=pltpu.CompilerParams(vmem_limit_bytes=limit * MIB),
    )


def thirds(x):
    hi = x.astype(BF).astype(F32)
    rest = x - hi
    mid = rest.astype(BF).astype(F32)
    return hi, mid, (rest - mid).astype(BF).astype(F32)


def lane_of(shape):
    return lax.broadcasted_iota(jnp.int32, shape, len(shape) - 1)


def mixed_rows(pre_ref, taps, lanes, first, rows):
    acc = None
    for j in range(4):
        term = taps[j : j + 1, lanes] * pre_ref[pl.ds(first + TAIL - 3 + j, rows), lanes]
        acc = term if acc is None else acc + term
    return acc * (1.0 / (1.0 + jnp.exp(-acc)))


def summary_kernel(own_ref, oth_ref, one_ref, two_ref, gain_ref, wk_hbm, wv_hbm, wg_ref, taps_ref, offs_ref,
                   key_ref, value_ref, logs_ref, piece_ref, rows_ref, wk_ref, wv_ref, pre_ref, sems):
    wide = HEADS * DV // 2
    copies = [pltpu.make_async_copy(wk_hbm, wk_ref, sems.at[0])]
    for c in range(2):
        cols = pl.ds(c * wide, wide)
        copies.append(pltpu.make_async_copy(wv_hbm.at[:, cols], wv_ref.at[:, cols], sems.at[1 + c]))
    for copy in copies:
        copy.start()
    tp = lax.axis_index("tp")
    gain = gain_ref[...]

    def normalized(x):
        x = x.astype(F32)
        scale = lax.rsqrt(jnp.mean(x * x, axis=-1, keepdims=True) + EPS)
        return (x * scale * gain).astype(BF)

    rows_ref[0:TAIL, :] = normalized(one_ref[...] + two_ref[...])
    for ref, at in ((own_ref, tp), (oth_ref, 1 - tp)):
        for part in range(HALF // 48):
            to = pl.multiple_of(TAIL + at * HALF + part * 48, 16)
            rows_ref[pl.ds(to, 48), :] = normalized(ref[part * 48 : part * 48 + 48, :])
    own = pl.ds(TAIL, ROWS)
    gates = jnp.dot(rows_ref[own, :], wg_ref[...], preferred_element_type=F32)
    copies[0].wait()
    pre_ref[...] = jnp.dot(rows_ref[...], wk_ref[...], preferred_element_type=F32).astype(BF).astype(F32)

    lane = lane_of((SPAN, 128))
    tri = (lax.broadcasted_iota(jnp.int32, (SPAN, SPAN), 0) >= lax.broadcasted_iota(jnp.int32, (SPAN, SPAN), 1)).astype(F32)
    gate, inside, totals = [], [], []
    for b in range(BLOCKS):
        g = gates[b * SPAN : (b + 1) * SPAN] + offs_ref[b : b + 1, :]
        soft = jnp.minimum(g, 0.0) - jnp.log1p(jnp.exp(-jnp.abs(g)))
        total = jnp.dot(tri, soft, precision=HIGHEST, preferred_element_type=F32)
        logs_ref[b * SPAN : (b + 1) * SPAN, :] = jnp.where(lane < HEADS, g, total)
        total = pltpu.roll(total, 128 - HEADS, 1)
        gate.append(g)
        inside.append(total)
        totals.append(total[SPAN - 1 : SPAN, :])
    write, level = [], None
    later = jnp.zeros_like(totals[0])
    for b in reversed(range(BLOCKS)):
        w = (totals[b] - inside[b]) + later + gate[b]
        later = later + totals[b]
        write.insert(0, w)
        top = jnp.max(w, axis=0, keepdims=True)
        level = top if level is None else jnp.maximum(level, top)
    weight = [jnp.exp(w - level) for w in write]
    numbers = thirds(later) + thirds(level)

    taps = taps_ref[:, pl.ds(pl.multiple_of(tp * (HEADS * DQK), 128), HEADS * DQK)].astype(F32)
    for h in range(HEADS):
        lanes = slice(h * DQK, (h + 1) * DQK)
        for b in range(BLOCKS):
            rows = slice(b * SPAN, (b + 1) * SPAN)
            key_ref[rows, lanes] = (mixed_rows(pre_ref, taps, lanes, b * SPAN, SPAN) * DQK**-0.5).astype(BF)
    for c in range(2):
        copies[1 + c].wait()
        cols = slice(c * wide, (c + 1) * wide)
        value_ref[:, cols] = jnp.dot(rows_ref[own, :], wv_ref[:, cols], preferred_element_type=F32).astype(BF)
    ones = jnp.ones((ROWS, 128), BF)
    dims = (((0,), (0,)), ((), ()))
    for h in range(HEADS):
        lanes = slice(h * DQK, (h + 1) * DQK)
        weighted = jnp.concatenate(
            [
                (key_ref[b * SPAN : (b + 1) * SPAN, lanes].astype(F32) * weight[b][:, h : h + 1]).astype(BF)
                for b in range(BLOCKS)
            ],
            axis=0,
        )
        memory = lax.dot_general(weighted, value_ref[:, h * DV : (h + 1) * DV], dims, preferred_element_type=F32)
        extra = lax.dot_general(weighted, ones, dims, preferred_element_type=F32)
        for n, number in enumerate(numbers):
            extra = jnp.where(lane == n + 1, number[:, h : h + 1], extra)
        out = slice(h * DQK, (h + 1) * DQK)
        piece_ref[out, :DV] = memory.astype(BF)
        piece_ref[out, DV:] = extra.astype(BF)


def prefix_kernel(piece_ref, out_ref, wide_ref, done_ref):
    count = piece_ref.shape[0]
    wide_ref[...] = piece_ref[...].astype(F32)
    extra = wide_ref[:, 0, DV:]
    lane = lane_of((count, 128))

    def number(first):
        return jnp.sum(jnp.where((lane >= first) & (lane < first + 3), extra, 0.0), axis=1, keepdims=True)

    forget, level = number(1), number(4)
    down = lax.broadcasted_iota(jnp.int32, (count, count), 0)
    over = lax.broadcasted_iota(jnp.int32, (count, count), 1)
    steps = jnp.where(down > over, forget, jnp.where(down == over, level, 0.0))
    earlier = over < down
    logs = jnp.dot(earlier.astype(F32), steps, precision=HIGHEST, preferred_element_type=F32)
    logs = jnp.where(earlier, logs, EMPTY)
    top = jnp.max(logs, axis=1, keepdims=True)
    weight = jnp.where(earlier, jnp.exp(logs - top), 0.0)
    high = weight.astype(BF)
    low = (weight - high.astype(F32)).astype(BF)
    marks = thirds(top)
    lane = lane_of((count, WIDTH))
    for r in range(8):
        part = wide_ref[:, r, :].astype(BF)
        state = jnp.dot(high, part, preferred_element_type=F32) + jnp.dot(low, part, preferred_element_type=F32)
        for n, mark in enumerate(marks):
            state = jnp.where(lane == DV + 1 + n, mark, state)
        done_ref[:, r, :] = state
    out_ref[...] = done_ref[...].astype(BF)


def query_kernel(rows_ref, wq_hbm, wo_hbm, taps_ref, gain_ref, query_ref, ogate_ref, wq_ref, wo_ref, pre_ref, sems):
    wide = HEADS * DV // 2
    copies = [pltpu.make_async_copy(wq_hbm, wq_ref, sems.at[0])]
    for c in range(2):
        cols = pl.ds(c * wide, wide)
        copies.append(pltpu.make_async_copy(wo_hbm.at[:, cols], wo_ref.at[:, cols], sems.at[1 + c]))
    for copy in copies:
        copy.start()
    tp = lax.axis_index("tp")
    taps = taps_ref[:, pl.ds(pl.multiple_of(tp * (HEADS * DQK), 128), HEADS * DQK)].astype(F32)
    gain = gain_ref[:, pl.ds(pl.multiple_of(tp * (HEADS * DV), 128), HEADS * DV)]
    copies[0].wait()
    pre_ref[...] = jnp.dot(rows_ref[...], wq_ref[...], preferred_element_type=F32).astype(BF).astype(F32)
    for h in range(HEADS):
        lanes = slice(h * DQK, (h + 1) * DQK)
        for b in range(BLOCKS):
            rows = slice(b * SPAN, (b + 1) * SPAN)
            query_ref[rows, lanes] = mixed_rows(pre_ref, taps, lanes, b * SPAN, SPAN).astype(BF)
    for c in range(2):
        copies[1 + c].wait()
        cols = slice(c * wide, (c + 1) * wide)
        pre = jnp.dot(rows_ref[pl.ds(TAIL, ROWS), :], wo_ref[:, cols], preferred_element_type=F32).astype(BF).astype(F32)
        ogate_ref[:, cols] = gain[:, cols] / (1.0 + jnp.exp(-pre))


def local_kernel(query_ref, key_ref, value_ref, logs_ref, numer_ref, stats_ref):
    lane = lane_of((SPAN, 128))
    cols = [logs_ref[b * SPAN : (b + 1) * SPAN, :] for b in range(BLOCKS)]
    flat = [c.T for c in cols]
    ends = [c[SPAN - 1 : SPAN, :] for c in cols]
    causal = lax.broadcasted_iota(jnp.int32, (SPAN, SPAN), 0) >= lax.broadcasted_iota(jnp.int32, (SPAN, SPAN), 1)
    stats = []
    before = jnp.zeros_like(ends[0])
    for b in range(BLOCKS):
        carried = pltpu.roll(cols[b] + before, HEADS, 1)
        before = before + ends[b]
        stats.append(jnp.where((lane >= 2 * HEADS) & (lane < 3 * HEADS), carried, 0.0))
    nt = (((1,), (1,)), ((), ()))
    for h in range(HEADS):
        head = slice(h * DQK, (h + 1) * DQK)
        for t in range(BLOCKS):
            rows = slice(t * SPAN, (t + 1) * SPAN)
            seen = (t + 1) * SPAN
            now = cols[t][:, HEADS + h : HEADS + h + 1]
            logs = []
            for s in range(t + 1):
                gate = flat[s][h : h + 1, :]
                past = flat[s][HEADS + h : HEADS + h + 1, :]
                if s == t:
                    logs.append(jnp.where(causal, (now - past) + gate, EMPTY))
                else:
                    rest = ends[s][:, HEADS + h : HEADS + h + 1] - past
                    for c in range(s + 1, t):
                        rest = rest + ends[c][:, HEADS + h : HEADS + h + 1]
                    logs.append(now + (rest + gate))
            top = None
            for x in logs:
                peak = jnp.max(x, axis=1, keepdims=True)
                top = peak if top is None else jnp.maximum(top, peak)
            weight = jnp.concatenate([jnp.exp(x - top) for x in logs], axis=1)
            scores = (
                lax.dot_general(query_ref[rows, head], key_ref[:seen, head], nt, preferred_element_type=F32) * weight
            )
            denom = jnp.sum(scores, axis=1, keepdims=True)
            numer_ref[rows, h * DV : (h + 1) * DV] = jnp.dot(
                scores.astype(BF), value_ref[:seen, h * DV : (h + 1) * DV], preferred_element_type=F32
            )
            stats[t] = jnp.where(lane == h, denom, jnp.where(lane == HEADS + h, top, stats[t]))
    for t in range(BLOCKS):
        stats_ref[t * SPAN : (t + 1) * SPAN, :] = stats[t]


def hidden_rows(first, query_ref, ogate_ref, state_ref, numer_ref, stats_ref, hidden_ref):
    rows = pl.ds(pl.multiple_of(first, 16), HALF)
    lane = lane_of((HALF, 128))
    stats = stats_ref[rows, :]
    place = lane_of((DQK, 128))
    norms, level = [], jnp.zeros((1, 128), F32)
    for h in range(HEADS):
        extra = state_ref[h * DQK : (h + 1) * DQK, DV:].astype(F32)
        norms.append(jnp.where(place == h, extra[:, 0:1], 0.0).astype(BF))
        mark = extra[0:1, 1:2] + extra[0:1, 2:3] + extra[0:1, 3:4]
        level = jnp.where(lane_of((1, 128)) == h, mark, level)
    norms = jnp.concatenate(norms, axis=0)
    query = query_ref[rows, :]
    read_norm = jnp.dot(query, norms, preferred_element_type=F32)
    top = pltpu.roll(stats, 128 - HEADS, 1)
    carried = pltpu.roll(stats, 128 - 2 * HEADS, 1) + level
    peak = jnp.maximum(carried, top)
    one = jnp.exp(carried - peak)
    two = jnp.exp(top - peak)
    denom = one * read_norm + two * stats
    denom = jnp.maximum(jnp.abs(denom), jnp.exp(-peak))
    one = one / denom
    two = two / denom
    for h in range(HEADS):
        wide = slice(h * DV, (h + 1) * DV)
        read = jnp.dot(
            query[:, h * DQK : (h + 1) * DQK], state_ref[h * DQK : (h + 1) * DQK, :DV], preferred_element_type=F32
        )
        cell = one[:, h : h + 1] * read + two[:, h : h + 1] * numer_ref[rows, wide]
        scale = lax.rsqrt(jnp.mean(cell * cell, axis=-1, keepdims=True) + EPS)
        hidden_ref[:, wide] = (cell * scale * ogate_ref[rows, wide]).astype(BF)


def sent_kernel(query_ref, ogate_ref, state_ref, numer_ref, stats_ref, wout_ref, out_ref, hidden_ref):
    first = (1 - lax.axis_index("tp")) * HALF
    hidden_rows(first, query_ref, ogate_ref, state_ref, numer_ref, stats_ref, hidden_ref)
    out_ref[...] = jnp.dot(hidden_ref[...], wout_ref[...], preferred_element_type=F32).astype(BF)


def kept_kernel(query_ref, ogate_ref, state_ref, numer_ref, stats_ref, wout_ref, out_ref, hidden_ref):
    first = lax.axis_index("tp") * HALF
    hidden_rows(first, query_ref, ogate_ref, state_ref, numer_ref, stats_ref, hidden_ref)
    out_ref[...] = jnp.dot(hidden_ref[...], wout_ref[...], preferred_element_type=F32)


def body(
    tokens, norm_gain, w_query, w_key, w_value, w_ogate, w_igate, w_fgate, conv_query, conv_key, gate_offset, head_gain, w_out
):
    tp = lax.axis_index("tp")
    width = tokens.shape[1]
    first = tp * HEADS
    stretches = lax.axis_size(SP)
    shape = jax.ShapeDtypeStruct
    other = lax.ppermute(tokens, "tp", [(0, 1), (1, 0)])
    last = tokens[HALF - TAIL :]
    to_second = lax.ppermute(last, SP_TP, [(2 * i + 1, 2 * i + 3) for i in range(stretches - 1)])
    to_first = lax.ppermute(last, SP_TP, [(2 * i + 1, 2 * i + 2) for i in range(stretches - 1)])
    w_gates = jnp.concatenate(
        [lax.dynamic_slice_in_dim(w_igate, first, HEADS, 1), lax.dynamic_slice_in_dim(w_fgate, first, HEADS, 1)], axis=1
    )
    w_gates = jnp.pad(w_gates, ((0, 0), (0, 128 - 2 * HEADS)))
    offsets = jnp.concatenate([gate_offset[0], gate_offset[1]], axis=1)
    offsets = jnp.pad(offsets, ((0, 0), (0, 128 - 2 * HEADS)))
    gain = norm_gain.reshape(1, -1)
    head_gain = head_gain.reshape(1, -1)
    v, m = in_vmem(), in_hbm()
    key, value, logs, pieces, rows = call(
        summary_kernel,
        (
            shape((ROWS, HEADS * DQK), BF),
            shape((ROWS, HEADS * DV), BF),
            shape((ROWS, 128), F32),
            shape((HEADS * DQK, WIDTH), BF),
            shape((TAIL + ROWS, width), BF),
        ),
        [v, v, v, v, v, m, m, v, v, v],
        [
            pltpu.VMEM((width, HEADS * DQK), BF),
            pltpu.VMEM((width, HEADS * DV), BF),
            pltpu.VMEM((TAIL + ROWS, HEADS * DQK), F32),
            pltpu.SemaphoreType.DMA((3,)),
        ],
        flops=3_000_000_000,
    )(tokens, other, to_first, to_second, gain, w_key, w_value, w_gates, conv_key, offsets)
    pieces = pieces.reshape(stretches, 8, WIDTH)
    pieces = lax.all_to_all(pieces, SP, 0, 0, tiled=True)
    query, ogate = call(
        query_kernel,
        (shape((ROWS, HEADS * DQK), BF), shape((ROWS, HEADS * DV), F32)),
        [v, m, m, v, v],
        [
            pltpu.VMEM((width, HEADS * DQK), BF),
            pltpu.VMEM((width, HEADS * DV), BF),
            pltpu.VMEM((TAIL + ROWS, HEADS * DQK), F32),
            pltpu.SemaphoreType.DMA((3,)),
        ],
        flops=3_000_000_000,
    )(rows, w_query, w_ogate, conv_query, head_gain)
    state = call(
        prefix_kernel,
        shape((stretches, 8, WIDTH), BF),
        [v],
        [pltpu.VMEM((stretches, 8, WIDTH), F32), pltpu.VMEM((stretches, 8, WIDTH), F32)],
        flops=100_000_000,
    )(pieces)
    state = lax.all_to_all(state, SP, 0, 0, tiled=True).reshape(HEADS * DQK, WIDTH)
    numer, stats = call(
        local_kernel,
        (shape((ROWS, HEADS * DV), F32), shape((ROWS, 128), F32)),
        [v, v, v, v],
        flops=1_000_000_000,
    )(query, key, value, logs)
    hidden = pltpu.VMEM((HALF, HEADS * DV), BF)
    sent = call(sent_kernel, shape((HALF, width), BF), [v] * 6, [hidden], flops=1_000_000_000)(
        query, ogate, state, numer, stats, w_out
    )
    got = lax.ppermute(sent, "tp", [(0, 1), (1, 0)])
    kept = call(kept_kernel, shape((HALF, width), F32), [v] * 6, [hidden], flops=1_000_000_000)(
        query, ogate, state, numer, stats, w_out
    )
    return (kept + got.astype(F32)).astype(BF)


def solution(mesh):
    split = Mesh(mesh.devices.reshape(4, 4, 4, mesh.shape["tp"]), ("sp_0", "sp_1", "sp_2", "tp"))
    placed = (
        P(SP_TP, None),
        P(),
        P(None, "tp"),
        P(None, "tp"),
        P(None, "tp"),
        P(None, "tp"),
        P(),
        P(),
        P(),
        P(),
        P(None, SP, "tp"),
        P(),
        P("tp", None),
    )
    return jax.shard_map(
        body, mesh=split, in_specs=placed, out_specs=P(SP_TP, None), check_vma=False
    )
```

```python
import functools

import jax
import jax.numpy as jnp
from jax import lax
from jax.experimental import pallas as pl
from jax.experimental.pallas import tpu as pltpu
from jax.sharding import Mesh
from jax.sharding import PartitionSpec as P

SPAN = 128
SP = ("sp_0", "sp_1", "sp_2")
SP_TP = ("sp_0", "sp_1", "sp_2", "tp")
EPS = 1e-06
EMPTY = -1e30
TAIL = 16
HEADS = 4
DQK = 128
DV = 256
WIDTH = DV + 128
BLOCKS = 3
ROWS = BLOCKS * SPAN
HALF = ROWS // 2
HIGHEST = lax.Precision.HIGHEST
BF = jnp.bfloat16
F32 = jnp.float32
MIB = 1 << 20


def call(kernel, outs, out_spaces, spaces, scratch=(), flops=0, limit=8):
    def spec(space):
        return pl.BlockSpec(memory_space=pltpu.VMEM if space is None else space)

    def placed(like, space):
        return like if space is None else space(like.shape, like.dtype)

    several = isinstance(outs, tuple)
    run = pl.pallas_call(
        kernel,
        out_shape=tuple(map(placed, outs, out_spaces)) if several else placed(outs, out_spaces),
        in_specs=[spec(space) for space in spaces],
        out_specs=tuple(map(spec, out_spaces)) if several else spec(out_spaces),
        scratch_shapes=list(scratch),
        cost_estimate=pl.CostEstimate(flops=flops, transcendentals=0, bytes_accessed=1 << 20),
        compiler_params=pltpu.CompilerParams(vmem_limit_bytes=limit * MIB),
    )

    def kept(x, space):
        return x if space is None else pltpu.with_memory_space_constraint(x, space)

    return lambda *args: run(*map(kept, args, spaces))


def started(pairs, sems):
    copies = [pltpu.make_async_copy(src, dst, sems.at[n]) for n, (src, dst) in enumerate(pairs)]
    for copy in copies:
        copy.start()
    return copies


def thirds(x):
    hi = x.astype(BF).astype(F32)
    rest = x - hi
    mid = rest.astype(BF).astype(F32)
    return hi, mid, (rest - mid).astype(BF).astype(F32)


def lane_of(shape):
    return lax.broadcasted_iota(jnp.int32, shape, len(shape) - 1)


def mixed_rows(pre_ref, taps, lanes, first, rows):
    acc = None
    for j in range(4):
        term = taps[j : j + 1, lanes] * pre_ref[pl.ds(first + TAIL - 3 + j, rows), lanes]
        acc = term if acc is None else acc + term
    return acc * (1.0 / (1.0 + jnp.exp(-acc)))


def summary_kernel(own_ref, oth_ref, one_ref, two_ref, gain_ref, wk_hbm, wv_hbm, wg_ref, taps_ref, offs_ref,
                   key_out, value_out, logs_out, piece_ref, rows_out,
                   key_ref, value_ref, logs_ref, rows_ref, wk_ref, wv_ref, pre_ref, sems, out_sems):
    wide = HEADS * DV // 2
    copies = started(
        [(wk_hbm, wk_ref)]
        + [(wv_hbm.at[:, pl.ds(c * wide, wide)], wv_ref.at[:, pl.ds(c * wide, wide)]) for c in range(2)],
        sems,
    )
    outs = [
        pltpu.make_async_copy(src, dst, out_sems.at[n])
        for n, (src, dst) in enumerate(
            [(rows_ref, rows_out), (logs_ref, logs_out), (key_ref, key_out), (value_ref, value_out)]
        )
    ]
    tp = lax.axis_index("tp")
    gain = gain_ref[...]

    def normalized(x):
        x = x.astype(F32)
        scale = lax.rsqrt(jnp.mean(x * x, axis=-1, keepdims=True) + EPS)
        return (x * scale * gain).astype(BF)

    rows_ref[0:TAIL, :] = normalized(one_ref[...] + two_ref[...])
    for ref, at in ((own_ref, tp), (oth_ref, 1 - tp)):
        for part in range(HALF // 48):
            to = pl.multiple_of(TAIL + at * HALF + part * 48, 16)
            rows_ref[pl.ds(to, 48), :] = normalized(ref[part * 48 : part * 48 + 48, :])
    outs[0].start()
    own = pl.ds(TAIL, ROWS)
    gates = jnp.dot(rows_ref[own, :], wg_ref[...], preferred_element_type=F32)
    copies[0].wait()
    pre_ref[...] = jnp.dot(rows_ref[...], wk_ref[...], preferred_element_type=F32).astype(BF).astype(F32)

    lane = lane_of((SPAN, 128))
    tri = (lax.broadcasted_iota(jnp.int32, (SPAN, SPAN), 0) >= lax.broadcasted_iota(jnp.int32, (SPAN, SPAN), 1)).astype(F32)
    gate, inside, totals = [], [], []
    for b in range(BLOCKS):
        g = gates[b * SPAN : (b + 1) * SPAN] + offs_ref[b : b + 1, :]
        soft = jnp.minimum(g, 0.0) - jnp.log1p(jnp.exp(-jnp.abs(g)))
        total = jnp.dot(tri, soft, precision=HIGHEST, preferred_element_type=F32)
        logs_ref[b * SPAN : (b + 1) * SPAN, :] = jnp.where(lane < HEADS, g, total)
        total = pltpu.roll(total, 128 - HEADS, 1)
        gate.append(g)
        inside.append(total)
        totals.append(total[SPAN - 1 : SPAN, :])
    outs[1].start()
    write, level = [], None
    later = jnp.zeros_like(totals[0])
    for b in reversed(range(BLOCKS)):
        w = (totals[b] - inside[b]) + later + gate[b]
        later = later + totals[b]
        write.insert(0, w)
        top = jnp.max(w, axis=0, keepdims=True)
        level = top if level is None else jnp.maximum(level, top)
    weight = [jnp.exp(w - level) for w in write]
    numbers = thirds(later) + thirds(level)

    taps = taps_ref[:, pl.ds(pl.multiple_of(tp * (HEADS * DQK), 128), HEADS * DQK)].astype(F32)
    for h in range(HEADS):
        lanes = slice(h * DQK, (h + 1) * DQK)
        for b in range(BLOCKS):
            rows = slice(b * SPAN, (b + 1) * SPAN)
            key_ref[rows, lanes] = (mixed_rows(pre_ref, taps, lanes, b * SPAN, SPAN) * DQK**-0.5).astype(BF)
    outs[2].start()
    for c in range(2):
        copies[1 + c].wait()
        cols = slice(c * wide, (c + 1) * wide)
        value_ref[:, cols] = jnp.dot(rows_ref[own, :], wv_ref[:, cols], preferred_element_type=F32).astype(BF)
    outs[3].start()
    ones = jnp.ones((ROWS, 128), BF)
    dims = (((0,), (0,)), ((), ()))
    for h in range(HEADS):
        lanes = slice(h * DQK, (h + 1) * DQK)
        weighted = jnp.concatenate(
            [
                (key_ref[b * SPAN : (b + 1) * SPAN, lanes].astype(F32) * weight[b][:, h : h + 1]).astype(BF)
                for b in range(BLOCKS)
            ],
            axis=0,
        )
        memory = lax.dot_general(weighted, value_ref[:, h * DV : (h + 1) * DV], dims, preferred_element_type=F32)
        extra = lax.dot_general(weighted, ones, dims, preferred_element_type=F32)
        for n, number in enumerate(numbers):
            extra = jnp.where(lane == n + 1, number[:, h : h + 1], extra)
        out = slice(h * DQK, (h + 1) * DQK)
        piece_ref[out, :DV] = memory.astype(BF)
        piece_ref[out, DV:] = extra.astype(BF)
    for copy in outs:
        copy.wait()


def prefix_kernel(piece_ref, out_ref, wide_ref, done_ref):
    count = piece_ref.shape[0]
    wide_ref[...] = piece_ref[...].astype(F32)
    extra = wide_ref[:, 0, DV:]
    lane = lane_of((count, 128))

    def number(first):
        return jnp.sum(jnp.where((lane >= first) & (lane < first + 3), extra, 0.0), axis=1, keepdims=True)

    forget, level = number(1), number(4)
    down = lax.broadcasted_iota(jnp.int32, (count, count), 0)
    over = lax.broadcasted_iota(jnp.int32, (count, count), 1)
    steps = jnp.where(down > over, forget, jnp.where(down == over, level, 0.0))
    earlier = over < down
    logs = jnp.dot(earlier.astype(F32), steps, precision=HIGHEST, preferred_element_type=F32)
    logs = jnp.where(earlier, logs, EMPTY)
    top = jnp.max(logs, axis=1, keepdims=True)
    weight = jnp.where(earlier, jnp.exp(logs - top), 0.0)
    high = weight.astype(BF)
    low = (weight - high.astype(F32)).astype(BF)
    marks = thirds(top)
    lane = lane_of((count, WIDTH))
    for r in range(8):
        part = wide_ref[:, r, :].astype(BF)
        state = jnp.dot(high, part, preferred_element_type=F32) + jnp.dot(low, part, preferred_element_type=F32)
        for n, mark in enumerate(marks):
            state = jnp.where(lane == DV + 1 + n, mark, state)
        done_ref[:, r, :] = state
    out_ref[...] = done_ref[...].astype(BF)


def local_kernel(rows_hbm, wq_hbm, key_hbm, value_hbm, logs_hbm, taps_ref,
                 query_out, numer_out, stats_out,
                 rows_ref, wq_ref, key_ref, value_ref, logs_ref, pre_ref, query_ref, numer_ref, stats_ref, sems, out_sems):
    copies = started(
        [(rows_hbm, rows_ref), (wq_hbm, wq_ref), (logs_hbm, logs_ref), (key_hbm, key_ref), (value_hbm, value_ref)], sems
    )
    tp = lax.axis_index("tp")
    taps = taps_ref[:, pl.ds(pl.multiple_of(tp * (HEADS * DQK), 128), HEADS * DQK)].astype(F32)
    copies[0].wait()
    copies[1].wait()
    pre_ref[...] = jnp.dot(rows_ref[...], wq_ref[...], preferred_element_type=F32).astype(BF).astype(F32)
    for h in range(HEADS):
        lanes = slice(h * DQK, (h + 1) * DQK)
        for b in range(BLOCKS):
            rows = slice(b * SPAN, (b + 1) * SPAN)
            query_ref[rows, lanes] = mixed_rows(pre_ref, taps, lanes, b * SPAN, SPAN).astype(BF)
    outs = [pltpu.make_async_copy(query_ref, query_out, out_sems.at[0])]
    outs[0].start()
    for copy in copies[2:]:
        copy.wait()
    lane = lane_of((SPAN, 128))
    cols = [logs_ref[b * SPAN : (b + 1) * SPAN, :] for b in range(BLOCKS)]
    flat = [c.T for c in cols]
    ends = [c[SPAN - 1 : SPAN, :] for c in cols]
    causal = lax.broadcasted_iota(jnp.int32, (SPAN, SPAN), 0) >= lax.broadcasted_iota(jnp.int32, (SPAN, SPAN), 1)
    stats = []
    before = jnp.zeros_like(ends[0])
    for b in range(BLOCKS):
        carried = pltpu.roll(cols[b] + before, HEADS, 1)
        before = before + ends[b]
        stats.append(jnp.where((lane >= 2 * HEADS) & (lane < 3 * HEADS), carried, 0.0))
    nt = (((1,), (1,)), ((), ()))
    for h in range(HEADS):
        head = slice(h * DQK, (h + 1) * DQK)
        wide = slice(h * DV, (h + 1) * DV)
        for t in range(BLOCKS):
            rows = slice(t * SPAN, (t + 1) * SPAN)
            seen = (t + 1) * SPAN
            now = cols[t][:, HEADS + h : HEADS + h + 1]
            logs = []
            for s in range(t + 1):
                gate = flat[s][h : h + 1, :]
                past = flat[s][HEADS + h : HEADS + h + 1, :]
                if s == t:
                    logs.append(jnp.where(causal, (now - past) + gate, EMPTY))
                else:
                    rest = ends[s][:, HEADS + h : HEADS + h + 1] - past
                    for c in range(s + 1, t):
                        rest = rest + ends[c][:, HEADS + h : HEADS + h + 1]
                    logs.append(now + (rest + gate))
            top = None
            for x in logs:
                peak = jnp.max(x, axis=1, keepdims=True)
                top = peak if top is None else jnp.maximum(top, peak)
            weight = jnp.concatenate([jnp.exp(x - top) for x in logs], axis=1)
            scores = (
                lax.dot_general(query_ref[rows, head], key_ref[:seen, head], nt, preferred_element_type=F32) * weight
            )
            denom = jnp.sum(scores, axis=1, keepdims=True)
            numer_ref[rows, wide] = jnp.dot(scores.astype(BF), value_ref[:seen, wide], preferred_element_type=F32)
            stats[t] = jnp.where(lane == h, denom, jnp.where(lane == HEADS + h, top, stats[t]))
        outs.append(
            pltpu.make_async_copy(
                numer_ref.at[:, pl.ds(h * DV, DV)], numer_out.at[:, pl.ds(h * DV, DV)], out_sems.at[1 + h]
            )
        )
        outs[-1].start()
    for t in range(BLOCKS):
        stats_ref[t * SPAN : (t + 1) * SPAN, :] = stats[t]
    outs.append(pltpu.make_async_copy(stats_ref, stats_out, out_sems.at[1 + HEADS]))
    outs[-1].start()
    for copy in outs:
        copy.wait()


def gate_kernel(rows_hbm, wo_hbm, gain_ref, query_hbm, numer_hbm, stats_hbm, wout_hbm,
                ogate_ref, query_ref, numer_ref, stats_ref, wout_ref, rows_ref, wo_ref, sems):
    wide = HEADS * DV // 2
    copies = started(
        [(rows_hbm, rows_ref)]
        + [(wo_hbm.at[:, pl.ds(c * wide, wide)], wo_ref.at[:, pl.ds(c * wide, wide)]) for c in range(2)]
        + [(query_hbm, query_ref), (numer_hbm, numer_ref), (stats_hbm, stats_ref), (wout_hbm, wout_ref)],
        sems,
    )
    tp = lax.axis_index("tp")
    gain = gain_ref[:, pl.ds(pl.multiple_of(tp * (HEADS * DV), 128), HEADS * DV)]
    copies[0].wait()
    for c in range(2):
        copies[1 + c].wait()
        cols = slice(c * wide, (c + 1) * wide)
        pre = jnp.dot(rows_ref[pl.ds(TAIL, ROWS), :], wo_ref[:, cols], preferred_element_type=F32).astype(BF).astype(F32)
        ogate_ref[:, cols] = gain[:, cols] / (1.0 + jnp.exp(-pre))
    for copy in copies[3:]:
        copy.wait()


def hidden_rows(first, query_ref, ogate_ref, state_ref, numer_ref, stats_ref, hidden_ref):
    rows = pl.ds(pl.multiple_of(first, 16), HALF)
    lane = lane_of((HALF, 128))
    stats = stats_ref[rows, :]
    place = lane_of((DQK, 128))
    norms, level = [], jnp.zeros((1, 128), F32)
    for h in range(HEADS):
        extra = state_ref[h * DQK : (h + 1) * DQK, DV:].astype(F32)
        norms.append(jnp.where(place == h, extra[:, 0:1], 0.0).astype(BF))
        mark = extra[0:1, 1:2] + extra[0:1, 2:3] + extra[0:1, 3:4]
        level = jnp.where(lane_of((1, 128)) == h, mark, level)
    norms = jnp.concatenate(norms, axis=0)
    query = query_ref[rows, :]
    read_norm = jnp.dot(query, norms, preferred_element_type=F32)
    top = pltpu.roll(stats, 128 - HEADS, 1)
    carried = pltpu.roll(stats, 128 - 2 * HEADS, 1) + level
    peak = jnp.maximum(carried, top)
    one = jnp.exp(carried - peak)
    two = jnp.exp(top - peak)
    denom = one * read_norm + two * stats
    denom = jnp.maximum(jnp.abs(denom), jnp.exp(-peak))
    one = one / denom
    two = two / denom
    for h in range(HEADS):
        wide = slice(h * DV, (h + 1) * DV)
        read = jnp.dot(
            query[:, h * DQK : (h + 1) * DQK], state_ref[h * DQK : (h + 1) * DQK, :DV], preferred_element_type=F32
        )
        cell = one[:, h : h + 1] * read + two[:, h : h + 1] * numer_ref[rows, wide]
        scale = lax.rsqrt(jnp.mean(cell * cell, axis=-1, keepdims=True) + EPS)
        hidden_ref[:, wide] = (cell * scale * ogate_ref[rows, wide]).astype(BF)


def sent_kernel(query_ref, ogate_ref, state_ref, numer_ref, stats_ref, wout_ref, out_ref, hidden_ref):
    first = (1 - lax.axis_index("tp")) * HALF
    hidden_rows(first, query_ref, ogate_ref, state_ref, numer_ref, stats_ref, hidden_ref)
    out_ref[...] = jnp.dot(hidden_ref[...], wout_ref[...], preferred_element_type=F32).astype(BF)


def kept_kernel(query_ref, ogate_ref, state_ref, numer_ref, stats_ref, wout_ref, out_ref, hidden_ref):
    first = lax.axis_index("tp") * HALF
    hidden_rows(first, query_ref, ogate_ref, state_ref, numer_ref, stats_ref, hidden_ref)
    out_ref[...] = jnp.dot(hidden_ref[...], wout_ref[...], preferred_element_type=F32)


def body(
    tokens, norm_gain, w_query, w_key, w_value, w_ogate, w_igate, w_fgate, conv_query, conv_key, gate_offset, head_gain, w_out
):
    tp = lax.axis_index("tp")
    width = tokens.shape[1]
    first = tp * HEADS
    stretches = lax.axis_size(SP)
    shape = jax.ShapeDtypeStruct
    other = lax.ppermute(tokens, "tp", [(0, 1), (1, 0)])
    last = tokens[HALF - TAIL :]
    to_second = lax.ppermute(last, SP_TP, [(2 * i + 1, 2 * i + 3) for i in range(stretches - 1)])
    to_first = lax.ppermute(last, SP_TP, [(2 * i + 1, 2 * i + 2) for i in range(stretches - 1)])
    w_gates = jnp.concatenate(
        [lax.dynamic_slice_in_dim(w_igate, first, HEADS, 1), lax.dynamic_slice_in_dim(w_fgate, first, HEADS, 1)], axis=1
    )
    w_gates = jnp.pad(w_gates, ((0, 0), (0, 128 - 2 * HEADS)))
    offsets = jnp.concatenate([gate_offset[0], gate_offset[1]], axis=1)
    offsets = jnp.pad(offsets, ((0, 0), (0, 128 - 2 * HEADS)))
    gain = norm_gain.reshape(1, -1)
    head_gain = head_gain.reshape(1, -1)
    v, m, n = pltpu.VMEM, pltpu.HBM, None
    dma = pltpu.SemaphoreType.DMA
    key_shape, value_shape = shape((ROWS, HEADS * DQK), BF), shape((ROWS, HEADS * DV), BF)
    logs_shape, wide_shape = shape((ROWS, 128), F32), shape((ROWS, HEADS * DV), F32)
    rows_shape, pre_shape = shape((TAIL + ROWS, width), BF), shape((TAIL + ROWS, HEADS * DQK), F32)

    def room(like):
        return pltpu.VMEM(like.shape, like.dtype)

    key, value, logs, pieces, rows = call(
        summary_kernel,
        (key_shape, value_shape, logs_shape, shape((HEADS * DQK, WIDTH), BF), rows_shape),
        (m, m, m, n, m),
        [n, n, n, n, n, m, m, n, n, n],
        [room(key_shape), room(value_shape), room(logs_shape), room(rows_shape), room(w_key), room(w_value), room(pre_shape), dma((3,)), dma((4,))],
        flops=3_000_000_000,
        limit=20,
    )(tokens, other, to_first, to_second, gain, w_key, w_value, w_gates, conv_key, offsets)
    pieces = lax.all_to_all(pieces.reshape(stretches, 8, WIDTH), SP, 0, 0, tiled=True)
    query, numer, stats = call(
        local_kernel,
        (key_shape, wide_shape, logs_shape),
        (m, m, m),
        [m, m, m, m, m, n],
        [room(rows_shape), room(w_query), room(key_shape), room(value_shape), room(logs_shape), room(pre_shape), room(key_shape), room(wide_shape), room(logs_shape), dma((5,)), dma((2 + HEADS,))],
        flops=3_000_000_000,
        limit=16,
    )(rows, w_query, key, value, logs, conv_query)
    pieces, query, numer, stats = lax.optimization_barrier((pieces, query, numer, stats))
    state = call(
        prefix_kernel,
        shape((stretches, 8, WIDTH), BF),
        n,
        [n],
        [pltpu.VMEM((stretches, 8, WIDTH), F32), pltpu.VMEM((stretches, 8, WIDTH), F32)],
        flops=100_000_000,
    )(pieces)
    state, query, numer, stats = lax.optimization_barrier((state, query, numer, stats))
    state = lax.all_to_all(state, SP, 0, 0, tiled=True).reshape(HEADS * DQK, WIDTH)
    ogate, query, numer, stats, w_last = call(
        gate_kernel,
        (wide_shape, key_shape, wide_shape, logs_shape, shape(w_out.shape, BF)),
        (v, v, v, v, v),
        [m, m, n, m, m, m, m],
        [room(rows_shape), room(w_ogate), dma((7,))],
        flops=3_000_000_000,
        limit=10,
    )(rows, w_ogate, head_gain, query, numer, stats, w_out)
    hidden = pltpu.VMEM((HALF, HEADS * DV), BF)
    sent = call(sent_kernel, shape((HALF, width), BF), n, [v, v, n, v, v, v], [hidden], flops=1_000_000_000, limit=8)(
        query, ogate, state, numer, stats, w_last
    )
    got = lax.ppermute(sent, "tp", [(0, 1), (1, 0)])
    kept = call(kept_kernel, shape((HALF, width), F32), n, [v, v, n, v, v, v], [hidden], flops=1_000_000_000, limit=8)(
        query, ogate, state, numer, stats, w_last
    )
    return (kept + got.astype(F32)).astype(BF)


def solution(mesh):
    split = Mesh(mesh.devices.reshape(4, 4, 4, mesh.shape["tp"]), ("sp_0", "sp_1", "sp_2", "tp"))
    placed = (
        P(SP_TP, None),
        P(),
        P(None, "tp"),
        P(None, "tp"),
        P(None, "tp"),
        P(None, "tp"),
        P(),
        P(),
        P(),
        P(),
        P(None, SP, "tp"),
        P(),
        P("tp", None),
    )
    return jax.shard_map(
        body, mesh=split, in_specs=placed, out_specs=P(SP_TP, None), check_vma=False
    )
```

```python
import functools

import jax
import jax.numpy as jnp
from jax import lax
from jax.experimental import pallas as pl
from jax.experimental.pallas import tpu as pltpu
from jax.sharding import Mesh
from jax.sharding import PartitionSpec as P

SPAN = 128
SP = ("sp_0", "sp_1", "sp_2")
SP_TP = ("sp_0", "sp_1", "sp_2", "tp")
EPS = 1e-06
EMPTY = -1e30
TAIL = 16
HEADS = 4
DQK = 128
DV = 256
WIDTH = DV + 128
BLOCKS = 3
ROWS = BLOCKS * SPAN
HALF = ROWS // 2
HIGHEST = lax.Precision.HIGHEST
BF = jnp.bfloat16
F32 = jnp.float32
MIB = 1 << 20


def call(kernel, outs, out_spaces, spaces, scratch=(), flops=0, limit=8):
    def spec(space):
        return pl.BlockSpec(memory_space=pltpu.VMEM if space is None else space)

    def placed(like, space):
        return like if space is None else space(like.shape, like.dtype)

    several = isinstance(outs, tuple)
    run = pl.pallas_call(
        kernel,
        out_shape=tuple(map(placed, outs, out_spaces)) if several else placed(outs, out_spaces),
        in_specs=[spec(space) for space in spaces],
        out_specs=tuple(map(spec, out_spaces)) if several else spec(out_spaces),
        scratch_shapes=list(scratch),
        cost_estimate=pl.CostEstimate(flops=flops, transcendentals=0, bytes_accessed=1 << 20),
        compiler_params=pltpu.CompilerParams(vmem_limit_bytes=limit * MIB),
    )

    def kept(x, space):
        return x if space is None else pltpu.with_memory_space_constraint(x, space)

    return lambda *args: run(*map(kept, args, spaces))


def started(pairs, sems):
    copies = [pltpu.make_async_copy(src, dst, sems.at[n]) for n, (src, dst) in enumerate(pairs)]
    for copy in copies:
        copy.start()
    return copies


def thirds(x):
    hi = x.astype(BF).astype(F32)
    rest = x - hi
    mid = rest.astype(BF).astype(F32)
    return hi, mid, (rest - mid).astype(BF).astype(F32)


def lane_of(shape):
    return lax.broadcasted_iota(jnp.int32, shape, len(shape) - 1)


def mixed_rows(pre_ref, taps, lanes, first, rows):
    acc = None
    for j in range(4):
        term = taps[j : j + 1, lanes] * pre_ref[pl.ds(first + TAIL - 3 + j, rows), lanes]
        acc = term if acc is None else acc + term
    return acc * (1.0 / (1.0 + jnp.exp(-acc)))


def normalized(x, gain):
    x = x.astype(F32)
    scale = lax.rsqrt(jnp.mean(x * x, axis=-1, keepdims=True) + EPS)
    return (x * scale * gain).astype(BF)


def fetch_kernel(own_ref, gain_ref, wk_hbm, wv_hbm, rows_ref, wk_ref, wv_ref, sems):
    wide = HEADS * DV // 2
    copies = started(
        [(wk_hbm, wk_ref)]
        + [(wv_hbm.at[:, pl.ds(c * wide, wide)], wv_ref.at[:, pl.ds(c * wide, wide)]) for c in range(2)],
        sems,
    )
    gain = gain_ref[...]
    for part in range(HALF // 48):
        rows_ref[part * 48 : part * 48 + 48, :] = normalized(own_ref[part * 48 : part * 48 + 48, :], gain)
    for copy in copies:
        copy.wait()


def summary_kernel(own_ref, oth_ref, one_ref, two_ref, gain_ref, wk_ref, wv_ref, wg_ref, taps_ref, offs_ref,
                   key_out, value_out, logs_out, piece_ref, rows_ref, pre_ref, key_ref, value_ref, logs_ref, sems):
    outs = [
        pltpu.make_async_copy(src, dst, sems.at[n])
        for n, (src, dst) in enumerate([(logs_ref, logs_out), (key_ref, key_out), (value_ref, value_out)])
    ]
    tp = lax.axis_index("tp")
    gain = gain_ref[...]
    rows_ref[0:TAIL, :] = normalized(one_ref[...] + two_ref[...], gain)
    mine = pl.multiple_of(TAIL + tp * HALF, 16)
    rows_ref[pl.ds(mine, HALF), :] = own_ref[...]
    for part in range(HALF // 48):
        to = pl.multiple_of(TAIL + (1 - tp) * HALF + part * 48, 16)
        rows_ref[pl.ds(to, 48), :] = normalized(oth_ref[part * 48 : part * 48 + 48, :], gain)
    own = pl.ds(TAIL, ROWS)
    gates = jnp.dot(rows_ref[own, :], wg_ref[...], preferred_element_type=F32)
    pre_ref[...] = jnp.dot(rows_ref[...], wk_ref[...], preferred_element_type=F32).astype(BF).astype(F32)

    lane = lane_of((SPAN, 128))
    tri = (lax.broadcasted_iota(jnp.int32, (SPAN, SPAN), 0) >= lax.broadcasted_iota(jnp.int32, (SPAN, SPAN), 1)).astype(F32)
    gate, inside, totals = [], [], []
    for b in range(BLOCKS):
        g = gates[b * SPAN : (b + 1) * SPAN] + offs_ref[b : b + 1, :]
        soft = jnp.minimum(g, 0.0) - jnp.log1p(jnp.exp(-jnp.abs(g)))
        total = jnp.dot(tri, soft, precision=HIGHEST, preferred_element_type=F32)
        logs_ref[b * SPAN : (b + 1) * SPAN, :] = jnp.where(lane < HEADS, g, total)
        total = pltpu.roll(total, 128 - HEADS, 1)
        gate.append(g)
        inside.append(total)
        totals.append(total[SPAN - 1 : SPAN, :])
    outs[0].start()
    write, level = [], None
    later = jnp.zeros_like(totals[0])
    for b in reversed(range(BLOCKS)):
        w = (totals[b] - inside[b]) + later + gate[b]
        later = later + totals[b]
        write.insert(0, w)
        top = jnp.max(w, axis=0, keepdims=True)
        level = top if level is None else jnp.maximum(level, top)
    weight = [jnp.exp(w - level) for w in write]
    numbers = thirds(later) + thirds(level)

    taps = taps_ref[:, pl.ds(pl.multiple_of(tp * (HEADS * DQK), 128), HEADS * DQK)].astype(F32)
    for h in range(HEADS):
        lanes = slice(h * DQK, (h + 1) * DQK)
        for b in range(BLOCKS):
            rows = slice(b * SPAN, (b + 1) * SPAN)
            key_ref[rows, lanes] = (mixed_rows(pre_ref, taps, lanes, b * SPAN, SPAN) * DQK**-0.5).astype(BF)
    outs[1].start()
    value_ref[...] = jnp.dot(rows_ref[own, :], wv_ref[...], preferred_element_type=F32).astype(BF)
    outs[2].start()
    ones = jnp.ones((ROWS, 128), BF)
    dims = (((0,), (0,)), ((), ()))
    for h in range(HEADS):
        lanes = slice(h * DQK, (h + 1) * DQK)
        weighted = jnp.concatenate(
            [
                (key_ref[b * SPAN : (b + 1) * SPAN, lanes].astype(F32) * weight[b][:, h : h + 1]).astype(BF)
                for b in range(BLOCKS)
            ],
            axis=0,
        )
        memory = lax.dot_general(weighted, value_ref[:, h * DV : (h + 1) * DV], dims, preferred_element_type=F32)
        extra = lax.dot_general(weighted, ones, dims, preferred_element_type=F32)
        for n, number in enumerate(numbers):
            extra = jnp.where(lane == n + 1, number[:, h : h + 1], extra)
        out = slice(h * DQK, (h + 1) * DQK)
        piece_ref[out, :DV] = memory.astype(BF)
        piece_ref[out, DV:] = extra.astype(BF)
    for copy in outs:
        copy.wait()


def prefix_kernel(piece_ref, out_ref):
    count = piece_ref.shape[0] // 8
    tall = piece_ref.shape[0]

    def iota(shape, dim):
        return lax.broadcasted_iota(jnp.int32, shape, dim)

    def ones_where(test):
        return jnp.where(test, 1.0, 0.0).astype(BF)

    first = ones_where(iota((count, tall), 1) == 8 * iota((count, tall), 0))
    down = iota((tall, count), 0) - 8 * iota((tall, count), 1)
    spread = ones_where((down >= 0) & (down < 8))
    over = iota((count, tall), 1) - 8 * iota((count, tall), 0)
    spread_over = ones_where((over >= 0) & (over < 8))
    extra = jnp.dot(first, piece_ref[:, DV:], preferred_element_type=F32)
    lane = lane_of((count, 128))

    def number(at):
        return jnp.sum(jnp.where((lane >= at) & (lane < at + 3), extra, 0.0), axis=1, keepdims=True)

    forget, level = number(1), number(4)
    down, over = iota((count, count), 0), iota((count, count), 1)
    steps = jnp.where(down > over, forget, jnp.where(down == over, level, 0.0))
    earlier = over < down
    logs = jnp.dot(jnp.where(earlier, 1.0, 0.0), steps, precision=HIGHEST, preferred_element_type=F32)
    logs = jnp.where(earlier, logs, EMPTY)
    top = jnp.max(logs, axis=1, keepdims=True)
    weight = jnp.where(earlier, jnp.exp(logs - top), 0.0).astype(BF)
    weight = jnp.dot(weight, spread_over, preferred_element_type=F32).astype(BF)
    weight = jnp.dot(spread, weight, preferred_element_type=F32)
    same = (iota((tall, tall), 0) & 7) == (iota((tall, tall), 1) & 7)
    weight = jnp.where(same, weight, 0.0).astype(BF)
    marks = jnp.zeros((count, 128), F32)
    for n, mark in enumerate(thirds(top)):
        marks = jnp.where(lane == n + 1, mark, marks)
    marks = jnp.dot(spread, marks.astype(BF), preferred_element_type=F32)
    state = jnp.dot(weight, piece_ref[...], preferred_element_type=F32)
    lane = lane_of((tall, 128))
    out_ref[:, :DV] = state[:, :DV].astype(BF)
    out_ref[:, DV:] = jnp.where((lane >= 1) & (lane < 4), marks, state[:, DV:]).astype(BF)


def local_kernel(rows_ref, wq_hbm, key_hbm, value_hbm, logs_hbm, taps_ref,
                 query_ref, numer_ref, stats_ref, wq_ref, pre_ref, key_ref, value_ref, logs_ref, sems):
    copies = started([(wq_hbm, wq_ref), (logs_hbm, logs_ref), (key_hbm, key_ref), (value_hbm, value_ref)], sems)
    tp = lax.axis_index("tp")
    taps = taps_ref[:, pl.ds(pl.multiple_of(tp * (HEADS * DQK), 128), HEADS * DQK)].astype(F32)
    copies[0].wait()
    pre_ref[...] = jnp.dot(rows_ref[...], wq_ref[...], preferred_element_type=F32).astype(BF).astype(F32)
    for h in range(HEADS):
        lanes = slice(h * DQK, (h + 1) * DQK)
        for b in range(BLOCKS):
            rows = slice(b * SPAN, (b + 1) * SPAN)
            query_ref[rows, lanes] = mixed_rows(pre_ref, taps, lanes, b * SPAN, SPAN).astype(BF)
    for copy in copies[1:]:
        copy.wait()
    lane = lane_of((SPAN, 128))
    cols = [logs_ref[b * SPAN : (b + 1) * SPAN, :] for b in range(BLOCKS)]
    flat = [c.T for c in cols]
    ends = [c[SPAN - 1 : SPAN, :] for c in cols]
    causal = lax.broadcasted_iota(jnp.int32, (SPAN, SPAN), 0) >= lax.broadcasted_iota(jnp.int32, (SPAN, SPAN), 1)
    stats = []
    before = jnp.zeros_like(ends[0])
    for b in range(BLOCKS):
        carried = pltpu.roll(cols[b] + before, HEADS, 1)
        before = before + ends[b]
        stats.append(jnp.where((lane >= 2 * HEADS) & (lane < 3 * HEADS), carried, 0.0))
    nt = (((1,), (1,)), ((), ()))
    for h in range(HEADS):
        head = slice(h * DQK, (h + 1) * DQK)
        wide = slice(h * DV, (h + 1) * DV)
        for t in range(BLOCKS):
            rows = slice(t * SPAN, (t + 1) * SPAN)
            seen = (t + 1) * SPAN
            now = cols[t][:, HEADS + h : HEADS + h + 1]
            logs = []
            for s in range(t + 1):
                gate = flat[s][h : h + 1, :]
                past = flat[s][HEADS + h : HEADS + h + 1, :]
                if s == t:
                    logs.append(jnp.where(causal, (now - past) + gate, EMPTY))
                else:
                    rest = ends[s][:, HEADS + h : HEADS + h + 1] - past
                    for c in range(s + 1, t):
                        rest = rest + ends[c][:, HEADS + h : HEADS + h + 1]
                    logs.append(now + (rest + gate))
            top = None
            for x in logs:
                peak = jnp.max(x, axis=1, keepdims=True)
                top = peak if top is None else jnp.maximum(top, peak)
            weight = jnp.concatenate([jnp.exp(x - top) for x in logs], axis=1)
            scores = (
                lax.dot_general(query_ref[rows, head], key_ref[:seen, head], nt, preferred_element_type=F32) * weight
            )
            denom = jnp.sum(scores, axis=1, keepdims=True)
            numer = jnp.dot(scores.astype(BF), value_ref[:seen, wide], preferred_element_type=F32)
            numer_ref[rows, wide] = numer.astype(BF)
            stats[t] = jnp.where(lane == h, denom, jnp.where(lane == HEADS + h, top, stats[t]))
    for t in range(BLOCKS):
        stats_ref[t * SPAN : (t + 1) * SPAN, :] = stats[t]


def gate_kernel(rows_ref, wo_hbm, gain_ref, ogate_ref, wo_ref, sems):
    wide = HEADS * DV // 4
    copies = started(
        [(wo_hbm.at[:, pl.ds(c * wide, wide)], wo_ref.at[:, pl.ds(c * wide, wide)]) for c in range(4)],
        sems,
    )
    tp = lax.axis_index("tp")
    gain = gain_ref[:, pl.ds(pl.multiple_of(tp * (HEADS * DV), 128), HEADS * DV)]
    for c in range(4):
        copies[c].wait()
        cols = slice(c * wide, (c + 1) * wide)
        pre = jnp.dot(rows_ref[pl.ds(TAIL, ROWS), :], wo_ref[:, cols], preferred_element_type=F32).astype(BF).astype(F32)
        ogate_ref[:, cols] = (gain[:, cols] / (1.0 + jnp.exp(-pre))).astype(BF)


def hidden_rows(first, query_ref, ogate_ref, state_ref, numer_ref, stats_ref, hidden_ref):
    rows = pl.ds(pl.multiple_of(first, 16), HALF)
    lane = lane_of((HALF, 128))
    stats = stats_ref[rows, :]
    place = lane_of((DQK, 128))
    norms, level = [], jnp.zeros((1, 128), F32)
    for h in range(HEADS):
        extra = state_ref[h * DQK : (h + 1) * DQK, DV:].astype(F32)
        norms.append(jnp.where(place == h, extra[:, 0:1], 0.0).astype(BF))
        mark = extra[0:1, 1:2] + extra[0:1, 2:3] + extra[0:1, 3:4]
        level = jnp.where(lane_of((1, 128)) == h, mark, level)
    norms = jnp.concatenate(norms, axis=0)
    query = query_ref[rows, :]
    read_norm = jnp.dot(query, norms, preferred_element_type=F32)
    top = pltpu.roll(stats, 128 - HEADS, 1)
    carried = pltpu.roll(stats, 128 - 2 * HEADS, 1) + level
    peak = jnp.maximum(carried, top)
    one = jnp.exp(carried - peak)
    two = jnp.exp(top - peak)
    denom = one * read_norm + two * stats
    denom = jnp.maximum(jnp.abs(denom), jnp.exp(-peak))
    one = one / denom
    two = two / denom
    for h in range(HEADS):
        wide = slice(h * DV, (h + 1) * DV)
        read = jnp.dot(
            query[:, h * DQK : (h + 1) * DQK], state_ref[h * DQK : (h + 1) * DQK, :DV], preferred_element_type=F32
        )
        cell = one[:, h : h + 1] * read + two[:, h : h + 1] * numer_ref[rows, wide].astype(F32)
        scale = lax.rsqrt(jnp.mean(cell * cell, axis=-1, keepdims=True) + EPS)
        hidden_ref[:, wide] = (cell * scale * ogate_ref[rows, wide].astype(F32)).astype(BF)


def sent_kernel(query_ref, ogate_ref, state_ref, numer_ref, stats_ref, wout_hbm, out_ref, wout_ref, hidden_ref, sems):
    deep = HEADS * DV // 2
    copies = started(
        [(wout_hbm.at[pl.ds(c * deep, deep)], wout_ref.at[pl.ds(c * deep, deep)]) for c in range(2)], sems
    )
    first = (1 - lax.axis_index("tp")) * HALF
    hidden_rows(first, query_ref, ogate_ref, state_ref, numer_ref, stats_ref, hidden_ref)
    copies[0].wait()
    part = jnp.dot(hidden_ref[:, :deep], wout_ref[:deep, :], preferred_element_type=F32)
    copies[1].wait()
    out_ref[...] = (part + jnp.dot(hidden_ref[:, deep:], wout_ref[deep:, :], preferred_element_type=F32)).astype(BF)


def kept_kernel(query_ref, ogate_ref, state_ref, numer_ref, stats_ref, wout_ref, out_ref, hidden_ref):
    first = lax.axis_index("tp") * HALF
    hidden_rows(first, query_ref, ogate_ref, state_ref, numer_ref, stats_ref, hidden_ref)
    out_ref[...] = jnp.dot(hidden_ref[...], wout_ref[...], preferred_element_type=F32)


def body(
    tokens, norm_gain, w_query, w_key, w_value, w_ogate, w_igate, w_fgate, conv_query, conv_key, gate_offset, head_gain, w_out
):
    tp = lax.axis_index("tp")
    width = tokens.shape[1]
    first = tp * HEADS
    stretches = lax.axis_size(SP)
    shape = jax.ShapeDtypeStruct
    other = lax.ppermute(tokens, "tp", [(0, 1), (1, 0)])
    last = tokens[HALF - TAIL :]
    to_second = lax.ppermute(last, SP_TP, [(2 * i + 1, 2 * i + 3) for i in range(stretches - 1)])
    to_first = lax.ppermute(last, SP_TP, [(2 * i + 1, 2 * i + 2) for i in range(stretches - 1)])
    w_gates = jnp.concatenate(
        [lax.dynamic_slice_in_dim(w_igate, first, HEADS, 1), lax.dynamic_slice_in_dim(w_fgate, first, HEADS, 1)], axis=1
    )
    w_gates = jnp.pad(w_gates, ((0, 0), (0, 128 - 2 * HEADS)))
    offsets = jnp.concatenate([gate_offset[0], gate_offset[1]], axis=1)
    offsets = jnp.pad(offsets, ((0, 0), (0, 128 - 2 * HEADS)))
    gain = norm_gain.reshape(1, -1)
    head_gain = head_gain.reshape(1, -1)
    v, m, n = pltpu.VMEM, pltpu.HBM, None
    dma = pltpu.SemaphoreType.DMA
    key_shape, value_shape = shape((ROWS, HEADS * DQK), BF), shape((ROWS, HEADS * DV), BF)
    logs_shape, wide_shape = shape((ROWS, 128), F32), shape((ROWS, HEADS * DV), F32)
    rows_shape, pre_shape = shape((TAIL + ROWS, width), BF), shape((TAIL + ROWS, HEADS * DQK), F32)

    def room(like):
        return pltpu.VMEM(like.shape, like.dtype)

    own, wk, wv = call(
        fetch_kernel,
        (shape(tokens.shape, BF), shape(w_key.shape, BF), shape(w_value.shape, BF)),
        (v, v, v),
        [n, n, m, m],
        [dma((3,))],
        flops=1_000_000_000,
    )(tokens, gain, w_key, w_value)
    key, value, logs, pieces, rows = call(
        summary_kernel,
        (key_shape, value_shape, logs_shape, shape((HEADS * DQK, WIDTH), BF), rows_shape),
        (m, m, m, n, v),
        [v, n, n, n, n, v, v, n, n, n],
        [room(pre_shape), room(key_shape), room(value_shape), room(logs_shape), dma((3,))],
        flops=3_000_000_000,
    )(own, other, to_first, to_second, gain, wk, wv, w_gates, conv_key, offsets)
    pieces = lax.all_to_all(pieces.reshape(stretches, 8, WIDTH), SP, 0, 0, tiled=True)
    query, numer, stats = call(
        local_kernel,
        (key_shape, value_shape, logs_shape),
        (v, v, v),
        [v, m, m, m, m, n],
        [room(w_query), room(pre_shape), room(key_shape), room(value_shape), room(logs_shape), dma((4,))],
        flops=3_000_000_000,
    )(rows, w_query, key, value, logs, conv_query)
    pieces, query, numer, stats = lax.optimization_barrier((pieces, query, numer, stats))
    piece_shape = shape((stretches * 8, WIDTH), BF)
    state = call(prefix_kernel, piece_shape, n, [n], flops=100_000_000)(pieces.reshape(piece_shape.shape))
    state, query, numer, stats, rows = lax.optimization_barrier((state, query, numer, stats, rows))
    state = lax.all_to_all(state.reshape(stretches, 8, WIDTH), SP, 0, 0, tiled=True).reshape(HEADS * DQK, WIDTH)
    ogate = call(
        gate_kernel, value_shape, v, [v, m, n], [room(w_ogate), dma((4,))], flops=3_000_000_000
    )(rows, w_ogate, head_gain)
    hidden = pltpu.VMEM((HALF, HEADS * DV), BF)
    sent, wout = call(
        sent_kernel,
        (shape((HALF, width), BF), shape(w_out.shape, BF)),
        (n, v),
        [v, v, n, v, v, m],
        [hidden, dma((2,))],
        flops=1_000_000_000,
    )(query, ogate, state, numer, stats, w_out)
    got = lax.ppermute(sent, "tp", [(0, 1), (1, 0)])
    kept = call(kept_kernel, shape((HALF, width), F32), n, [v, v, n, v, v, v], [hidden], flops=1_000_000_000)(
        query, ogate, state, numer, stats, wout
    )
    return (kept + got.astype(F32)).astype(BF)


def solution(mesh):
    split = Mesh(mesh.devices.reshape(4, 4, 4, mesh.shape["tp"]), ("sp_0", "sp_1", "sp_2", "tp"))
    placed = (
        P(SP_TP, None),
        P(),
        P(None, "tp"),
        P(None, "tp"),
        P(None, "tp"),
        P(None, "tp"),
        P(),
        P(),
        P(),
        P(),
        P(None, SP, "tp"),
        P(),
        P("tp", None),
    )
    return jax.shard_map(
        body, mesh=split, in_specs=placed, out_specs=P(SP_TP, None), check_vma=False
    )
```

```python
import jax
import jax.numpy as jnp
import numpy as np
from jax import lax
from jax.experimental import pallas as pl
from jax.experimental.pallas import tpu as pltpu
from jax.sharding import Mesh
from jax.sharding import PartitionSpec as P


SPAN = 128
SP = ("sp_0", "sp_1", "sp_2")
SP_TP = ("sp_0", "sp_1", "sp_2", "tp")
EPS = 1e-06
EMPTY = -1e30
TAIL = 16
HEADS = 4
DQK = 128
DV = 256
WIDTH = DV + 128
BLOCKS = 3
ROWS = BLOCKS * SPAN
HALF = ROWS // 2
HIGHEST = lax.Precision.HIGHEST
BF = jnp.bfloat16
F32 = jnp.float32
MIB = 1 << 20


def call(kernel, outs, out_spaces, spaces, scratch=(), flops=0, limit=8):
    def spec(space):
        return pl.BlockSpec(memory_space=pltpu.VMEM if space is None else space)

    def placed(like, space):
        return like if space is None else space(like.shape, like.dtype)

    several = isinstance(outs, tuple)
    run = pl.pallas_call(
        kernel,
        out_shape=tuple(map(placed, outs, out_spaces)) if several else placed(outs, out_spaces),
        in_specs=[spec(space) for space in spaces],
        out_specs=tuple(map(spec, out_spaces)) if several else spec(out_spaces),
        scratch_shapes=list(scratch),
        cost_estimate=pl.CostEstimate(flops=flops, transcendentals=0, bytes_accessed=1 << 20),
        compiler_params=pltpu.CompilerParams(vmem_limit_bytes=limit * MIB),
    )

    def kept(x, space):
        return x if space is None else pltpu.with_memory_space_constraint(x, space)

    return lambda *args: run(*map(kept, args, spaces))


def started(pairs, sems):
    copies = [pltpu.make_async_copy(src, dst, sems.at[n]) for n, (src, dst) in enumerate(pairs)]
    for copy in copies:
        copy.start()
    return copies


def by_rows(src, dst, parts):
    rows = src.shape[0] // parts
    return [(src.at[pl.ds(c * rows, rows)], dst.at[pl.ds(c * rows, rows)]) for c in range(parts)]


def wait_all(copies):
    for copy in copies:
        copy.wait()


def thirds(x):
    hi = x.astype(BF).astype(F32)
    rest = x - hi
    mid = rest.astype(BF).astype(F32)
    return hi, mid, (rest - mid).astype(BF).astype(F32)


def lane_of(shape):
    return lax.broadcasted_iota(jnp.int32, shape, len(shape) - 1)


def mixed_rows(pre_ref, taps, lanes, first, rows):
    acc = None
    for j in range(4):
        term = taps[j : j + 1, lanes] * pre_ref[pl.ds(first + TAIL - 3 + j, rows), lanes]
        acc = term if acc is None else acc + term
    return acc * (1.0 / (1.0 + jnp.exp(-acc)))


def row_scale(x):
    return lax.rsqrt(jnp.mean(x * x, axis=-1, keepdims=True) + EPS)


def normalized(x, gain):
    x = x.astype(F32)
    return (x * row_scale(x) * gain).astype(BF)


def fetch_kernel(own_hbm, gain_hbm, wk_hbm, wv_hbm, rows_ref, wk_ref, wv_ref, own_ref, gain_ref, sems):
    copies = started(
        [(own_hbm, own_ref), (gain_hbm, gain_ref)] + by_rows(wk_hbm, wk_ref, 4) + by_rows(wv_hbm, wv_ref, 8), sems
    )
    copies[0].wait()
    parts = [slice(at, at + 48) for at in range(0, HALF, 48)]
    scales = [row_scale(own_ref[part, :].astype(F32)) for part in parts]
    copies[1].wait()
    gain = gain_ref[...]
    for part, scale in zip(parts, scales):
        rows_ref[part, :] = (own_ref[part, :].astype(F32) * scale * gain).astype(BF)
    wait_all(copies[2:])


def summary_kernel(own_ref, oth_ref, one_ref, two_ref, gain_ref, wk_ref, wv_ref, wi_ref, wf_ref, taps_ref, offs_ref,
                   key_out, value_out, logs_out, piece_ref, rows_out,
                   rows_ref, pre_ref, key_ref, value_ref, logs_ref, wg_ref, sems):
    outs = [
        pltpu.make_async_copy(src, dst, sems.at[n])
        for n, (src, dst) in enumerate(
            [(logs_ref, logs_out), (key_ref, key_out), (value_ref, value_out), (rows_ref, rows_out)]
        )
    ]
    tp = lax.axis_index("tp")
    gain = gain_ref[...]
    rows_ref[0:TAIL, :] = normalized(one_ref[...] + two_ref[...], gain)
    mine = pl.multiple_of(TAIL + tp * HALF, 16)
    rows_ref[pl.ds(mine, HALF), :] = own_ref[...]
    for part in range(HALF // 48):
        to = pl.multiple_of(TAIL + (1 - tp) * HALF + part * 48, 16)
        rows_ref[pl.ds(to, 48), :] = normalized(oth_ref[part * 48 : part * 48 + 48, :], gain)
    outs[3].start()
    all_heads = wi_ref.shape[0]
    wg_ref[...] = jnp.zeros_like(wg_ref)
    wg_ref[0:all_heads, :] = wi_ref[...]
    wg_ref[all_heads : 2 * all_heads, :] = wf_ref[...]
    own = pl.ds(TAIL, ROWS)
    gates = lax.dot_general(rows_ref[own, :], wg_ref[...], (((1,), (1,)), ((), ())), preferred_element_type=F32)
    gates = jnp.where(tp == 0, gates, pltpu.roll(gates, 128 - HEADS, 1))
    pre_ref[...] = jnp.dot(rows_ref[...], wk_ref[...], preferred_element_type=F32).astype(BF).astype(F32)

    lane = lane_of((SPAN, 128))
    tri = (lax.broadcasted_iota(jnp.int32, (SPAN, SPAN), 0) >= lax.broadcasted_iota(jnp.int32, (SPAN, SPAN), 1)).astype(F32)
    gate, inside, totals = [], [], []
    for b in range(BLOCKS):
        offs = jnp.zeros((1, 128), F32)
        for h in range(HEADS):
            for row, at in ((0, h), (1, 2 * HEADS + h)):
                offs = jnp.where(lane_of((1, 128)) == at, offs_ref[b, row : row + 1, h : h + 1], offs)
        g = gates[b * SPAN : (b + 1) * SPAN] + offs
        soft = jnp.minimum(g, 0.0) - jnp.log1p(jnp.exp(-jnp.abs(g)))
        total = jnp.dot(tri, soft, precision=HIGHEST, preferred_element_type=F32)
        logs_ref[b * SPAN : (b + 1) * SPAN, :] = jnp.where(lane < HEADS, g, pltpu.roll(total, 128 - HEADS, 1))
        total = pltpu.roll(total, 128 - 2 * HEADS, 1)
        gate.append(g)
        inside.append(total)
        totals.append(total[SPAN - 1 : SPAN, :])
    outs[0].start()
    write, level = [], None
    later = jnp.zeros_like(totals[0])
    for b in reversed(range(BLOCKS)):
        w = (totals[b] - inside[b]) + later + gate[b]
        later = later + totals[b]
        write.insert(0, w)
        top = jnp.max(w, axis=0, keepdims=True)
        level = top if level is None else jnp.maximum(level, top)
    weight = [jnp.exp(w - level) for w in write]
    numbers = thirds(later) + thirds(level)

    taps = taps_ref[:, pl.ds(pl.multiple_of(tp * (HEADS * DQK), 128), HEADS * DQK)].astype(F32)
    for h in range(HEADS):
        lanes = slice(h * DQK, (h + 1) * DQK)
        for b in range(BLOCKS):
            rows = slice(b * SPAN, (b + 1) * SPAN)
            key_ref[rows, lanes] = (mixed_rows(pre_ref, taps, lanes, b * SPAN, SPAN) * DQK**-0.5).astype(BF)
    outs[1].start()
    value_ref[...] = jnp.dot(rows_ref[own, :], wv_ref[...], preferred_element_type=F32).astype(BF)
    outs[2].start()
    ones = jnp.ones((ROWS, 128), BF)
    dims = (((0,), (0,)), ((), ()))
    for h in range(HEADS):
        lanes = slice(h * DQK, (h + 1) * DQK)
        weighted = jnp.concatenate(
            [
                (key_ref[b * SPAN : (b + 1) * SPAN, lanes].astype(F32) * weight[b][:, h : h + 1]).astype(BF)
                for b in range(BLOCKS)
            ],
            axis=0,
        )
        memory = lax.dot_general(weighted, value_ref[:, h * DV : (h + 1) * DV], dims, preferred_element_type=F32)
        extra = lax.dot_general(weighted, ones, dims, preferred_element_type=F32)
        for n, number in enumerate(numbers):
            extra = jnp.where(lane == n + 1, number[:, h : h + 1], extra)
        out = slice(h * DQK, (h + 1) * DQK)
        piece_ref[out, :DV] = memory.astype(BF)
        piece_ref[out, DV:] = extra.astype(BF)
    for copy in outs:
        copy.wait()


def prefix_kernel(piece_ref, place_ref, wout_hbm, out_ref, wout_ref, sems):
    copies = started(by_rows(wout_hbm.at[pl.ds(0, wout_ref.shape[0])], wout_ref, 4), sems)
    count = piece_ref.shape[0] // 8
    tall = piece_ref.shape[0]

    def iota(shape, dim):
        return lax.broadcasted_iota(jnp.int32, shape, dim)

    def ones_where(test):
        return jnp.where(test, 1.0, 0.0).astype(BF)

    first = ones_where(iota((count, tall), 1) == 8 * iota((count, tall), 0))
    down = iota((tall, count), 0) - 8 * iota((tall, count), 1)
    spread = ones_where((down >= 0) & (down < 8))
    over = iota((count, tall), 1) - 8 * iota((count, tall), 0)
    spread_over = ones_where((over >= 0) & (over < 8))
    extra = jnp.dot(first, piece_ref[:, DV:], preferred_element_type=F32)
    lane = lane_of((count, 128))

    def number(at):
        return jnp.sum(jnp.where((lane >= at) & (lane < at + 3), extra, 0.0), axis=1, keepdims=True)

    forget, level = number(1), number(4)
    down, over = place_ref[0], place_ref[1]
    steps = jnp.where(down > over, forget, jnp.where(down == over, level, 0.0))
    earlier = over < down
    logs = jnp.dot(jnp.where(earlier, 1.0, 0.0), steps, precision=HIGHEST, preferred_element_type=F32)
    logs = jnp.where(earlier, logs, EMPTY)
    top = jnp.max(logs, axis=1, keepdims=True)
    weight = jnp.where(earlier, jnp.exp(logs - top), 0.0).astype(BF)
    weight = jnp.dot(weight, spread_over, preferred_element_type=F32).astype(BF)
    weight = jnp.dot(spread, weight, preferred_element_type=F32)
    same = (iota((tall, tall), 0) & 7) == (iota((tall, tall), 1) & 7)
    weight = jnp.where(same, weight, 0.0).astype(BF)
    marks = jnp.zeros((count, 128), F32)
    for n, mark in enumerate(thirds(top)):
        marks = jnp.where(lane == n + 1, mark, marks)
    marks = jnp.dot(spread, marks.astype(BF), preferred_element_type=F32)
    state = jnp.dot(weight, piece_ref[...], preferred_element_type=F32)
    lane = lane_of((tall, 128))
    out_ref[:, :DV] = state[:, :DV].astype(BF)
    out_ref[:, DV:] = jnp.where((lane >= 1) & (lane < 4), marks, state[:, DV:]).astype(BF)
    wait_all(copies)


def local_kernel(rows_hbm, wq_hbm, key_hbm, value_hbm, logs_hbm, wo_hbm, taps_ref, gain_ref,
                 query_ref, numer_ref, stats_ref, ogate_ref,
                 rows_ref, wq_ref, pre_ref, key_ref, value_ref, logs_ref, wo_ref, sems):
    copies = started(
        by_rows(rows_hbm, rows_ref, 5)
        + by_rows(wq_hbm, wq_ref, 4)
        + [(logs_hbm, logs_ref), (key_hbm, key_ref), (value_hbm, value_ref)]
        + by_rows(wo_hbm, wo_ref, 8),
        sems,
    )
    tp = lax.axis_index("tp")
    taps = taps_ref[:, pl.ds(pl.multiple_of(tp * (HEADS * DQK), 128), HEADS * DQK)].astype(F32)
    wait_all(copies[:9])
    pre_ref[...] = jnp.dot(rows_ref[...], wq_ref[...], preferred_element_type=F32).astype(BF).astype(F32)
    for h in range(HEADS):
        lanes = slice(h * DQK, (h + 1) * DQK)
        for b in range(BLOCKS):
            rows = slice(b * SPAN, (b + 1) * SPAN)
            query_ref[rows, lanes] = mixed_rows(pre_ref, taps, lanes, b * SPAN, SPAN).astype(BF)
    wait_all(copies[9:12])
    lane = lane_of((SPAN, 128))
    cols = [logs_ref[b * SPAN : (b + 1) * SPAN, :] for b in range(BLOCKS)]
    flat = [c.T for c in cols]
    ends = [c[SPAN - 1 : SPAN, :] for c in cols]
    causal = lax.broadcasted_iota(jnp.int32, (SPAN, SPAN), 0) >= lax.broadcasted_iota(jnp.int32, (SPAN, SPAN), 1)
    stats = []
    before = jnp.zeros_like(ends[0])
    for b in range(BLOCKS):
        carried = pltpu.roll(cols[b] + before, HEADS, 1)
        before = before + ends[b]
        stats.append(jnp.where((lane >= 2 * HEADS) & (lane < 3 * HEADS), carried, 0.0))
    nt = (((1,), (1,)), ((), ()))
    for h in range(HEADS):
        head = slice(h * DQK, (h + 1) * DQK)
        wide = slice(h * DV, (h + 1) * DV)
        for t in range(BLOCKS):
            rows = slice(t * SPAN, (t + 1) * SPAN)
            seen = (t + 1) * SPAN
            now = cols[t][:, HEADS + h : HEADS + h + 1]
            logs = []
            for s in range(t + 1):
                gate = flat[s][h : h + 1, :]
                past = flat[s][HEADS + h : HEADS + h + 1, :]
                if s == t:
                    logs.append(jnp.where(causal, (now - past) + gate, EMPTY))
                else:
                    rest = ends[s][:, HEADS + h : HEADS + h + 1] - past
                    for c in range(s + 1, t):
                        rest = rest + ends[c][:, HEADS + h : HEADS + h + 1]
                    logs.append(now + (rest + gate))
            top = None
            for x in logs:
                peak = jnp.max(x, axis=1, keepdims=True)
                top = peak if top is None else jnp.maximum(top, peak)
            weight = jnp.concatenate([jnp.exp(x - top) for x in logs], axis=1)
            scores = (
                lax.dot_general(query_ref[rows, head], key_ref[:seen, head], nt, preferred_element_type=F32) * weight
            )
            denom = jnp.sum(scores, axis=1, keepdims=True)
            numer = jnp.dot(scores.astype(BF), value_ref[:seen, wide], preferred_element_type=F32)
            numer_ref[rows, wide] = numer.astype(BF)
            stats[t] = jnp.where(lane == h, denom, jnp.where(lane == HEADS + h, top, stats[t]))
    for t in range(BLOCKS):
        stats_ref[t * SPAN : (t + 1) * SPAN, :] = stats[t]
    wait_all(copies[12:])
    gain = gain_ref[:, pl.ds(pl.multiple_of(tp * (HEADS * DV), 128), HEADS * DV)]
    for c in range(2):
        cols = slice(c * HEADS * DV // 2, (c + 1) * HEADS * DV // 2)
        pre = jnp.dot(rows_ref[pl.ds(TAIL, ROWS), :], wo_ref[:, cols], preferred_element_type=F32).astype(BF).astype(F32)
        ogate_ref[:, cols] = (gain[:, cols] / (1.0 + jnp.exp(-pre))).astype(BF)


def hidden_rows(first, query_ref, ogate_ref, state_ref, numer_ref, stats_ref, hidden_ref):
    rows = pl.ds(pl.multiple_of(first, 16), HALF)
    lane = lane_of((HALF, 128))
    stats = stats_ref[rows, :]
    place = lane_of((DQK, 128))
    norms, level = [], jnp.zeros((1, 128), F32)
    for h in range(HEADS):
        extra = state_ref[h * DQK : (h + 1) * DQK, DV:].astype(F32)
        norms.append(jnp.where(place == h, extra[:, 0:1], 0.0).astype(BF))
        mark = extra[0:1, 1:2] + extra[0:1, 2:3] + extra[0:1, 3:4]
        level = jnp.where(lane_of((1, 128)) == h, mark, level)
    norms = jnp.concatenate(norms, axis=0)
    query = query_ref[rows, :]
    read_norm = jnp.dot(query, norms, preferred_element_type=F32)
    top = pltpu.roll(stats, 128 - HEADS, 1)
    carried = pltpu.roll(stats, 128 - 2 * HEADS, 1) + level
    peak = jnp.maximum(carried, top)
    one = jnp.exp(carried - peak)
    two = jnp.exp(top - peak)
    denom = one * read_norm + two * stats
    denom = jnp.maximum(jnp.abs(denom), jnp.exp(-peak))
    one = one / denom
    two = two / denom
    for h in range(HEADS):
        wide = slice(h * DV, (h + 1) * DV)
        read = jnp.dot(
            query[:, h * DQK : (h + 1) * DQK], state_ref[h * DQK : (h + 1) * DQK, :DV], preferred_element_type=F32
        )
        cell = one[:, h : h + 1] * read + two[:, h : h + 1] * numer_ref[rows, wide].astype(F32)
        scale = lax.rsqrt(jnp.mean(cell * cell, axis=-1, keepdims=True) + EPS)
        hidden_ref[:, wide] = (cell * scale * ogate_ref[rows, wide].astype(F32)).astype(BF)


def sent_kernel(query_ref, ogate_ref, state_ref, numer_ref, stats_ref, upper_ref, wout_hbm, out_ref, lower_ref, hidden_ref, sems):
    deep = upper_ref.shape[0]
    copies = started(by_rows(wout_hbm.at[pl.ds(deep, deep)], lower_ref, 4), sems)
    first = (1 - lax.axis_index("tp")) * HALF
    hidden_rows(first, query_ref, ogate_ref, state_ref, numer_ref, stats_ref, hidden_ref)
    part = jnp.dot(hidden_ref[:, :deep], upper_ref[...], preferred_element_type=F32)
    wait_all(copies)
    out_ref[...] = (part + jnp.dot(hidden_ref[:, deep:], lower_ref[...], preferred_element_type=F32)).astype(BF)


def kept_kernel(query_ref, ogate_ref, state_ref, numer_ref, stats_ref, upper_ref, lower_ref, out_ref, hidden_ref):
    deep = upper_ref.shape[0]
    first = lax.axis_index("tp") * HALF
    hidden_rows(first, query_ref, ogate_ref, state_ref, numer_ref, stats_ref, hidden_ref)
    part = jnp.dot(hidden_ref[:, :deep], upper_ref[...], preferred_element_type=F32)
    out_ref[...] = part + jnp.dot(hidden_ref[:, deep:], lower_ref[...], preferred_element_type=F32)


def far_first(stretches):
    at = np.arange(stretches)
    hops = sum(np.minimum(c, 4 - c) for c in (at // 16, at // 4 % 4, at % 4))
    return np.lexsort((at, -hops))


def body(
    tokens, norm_gain, w_query, w_key, w_value, w_ogate, w_igate, w_fgate, conv_query, conv_key, gate_offset, head_gain, w_out
):
    width = tokens.shape[1]
    stretches = lax.axis_size(SP)
    shape = jax.ShapeDtypeStruct
    other = lax.ppermute(tokens, "tp", [(0, 1), (1, 0)])
    last = tokens[HALF - TAIL :]
    to_second = lax.ppermute(last, SP_TP, [(2 * i + 1, 2 * i + 3) for i in range(stretches - 1)])
    to_first = lax.ppermute(last, SP_TP, [(2 * i + 1, 2 * i + 2) for i in range(stretches - 1)])
    gain = norm_gain.reshape(1, -1)
    head_gain = head_gain.reshape(1, -1)
    order = far_first(stretches)
    groups = [[2 * int(i) + t for i in order] for t in range(2)]
    place = np.stack([np.broadcast_to(order[:, None], (stretches, stretches)), np.broadcast_to(order, (stretches, stretches))])
    place = jnp.asarray(place.astype(np.int32))
    v, m, n = pltpu.VMEM, pltpu.HBM, None
    dma = pltpu.SemaphoreType.DMA
    key_shape, value_shape = shape((ROWS, HEADS * DQK), BF), shape((ROWS, HEADS * DV), BF)
    logs_shape = shape((ROWS, 128), F32)
    rows_shape, pre_shape = shape((TAIL + ROWS, width), BF), shape((TAIL + ROWS, HEADS * DQK), F32)

    def room(like):
        return pltpu.VMEM(like.shape, like.dtype)

    own, wk, wv = call(
        fetch_kernel,
        (shape(tokens.shape, BF), shape(w_key.shape, BF), shape(w_value.shape, BF)),
        (v, v, v),
        [m, m, m, m],
        [room(tokens), room(gain), dma((14,))],
        flops=1_000_000_000,
    )(tokens, gain, w_key, w_value)
    key, value, logs, pieces, rows = call(
        summary_kernel,
        (key_shape, value_shape, logs_shape, shape((HEADS * DQK, WIDTH), BF), rows_shape),
        (m, m, m, n, m),
        [v, n, n, n, n, v, v, n, n, n, n],
        [room(rows_shape), room(pre_shape), room(key_shape), room(value_shape), room(logs_shape), pltpu.VMEM((128, width), BF), dma((4,))],
        flops=3_000_000_000,
        limit=12,
    )(own, other, to_first, to_second, gain, wk, wv, w_igate.T, w_fgate.T, conv_key, gate_offset.transpose(1, 0, 2))
    pieces = lax.all_to_all(pieces.reshape(stretches, 8, WIDTH), SP_TP, 0, 0, axis_index_groups=groups, tiled=True)
    query, numer, stats, ogate = call(
        local_kernel,
        (key_shape, value_shape, logs_shape, value_shape),
        (v, v, v, v),
        [m, m, m, m, m, m, n, n],
        [room(rows_shape), room(w_query), room(pre_shape), room(key_shape), room(value_shape), room(logs_shape), room(w_ogate), dma((20,))],
        flops=6_000_000_000,
        limit=16,
    )(rows, w_query, key, value, logs, w_ogate, conv_query, head_gain)
    pieces, query, numer, stats, ogate = lax.optimization_barrier((pieces, query, numer, stats, ogate))
    piece_shape = shape((stretches * 8, WIDTH), BF)
    half_shape = shape((w_out.shape[0] // 2, width), BF)
    state, upper = call(
        prefix_kernel, (piece_shape, half_shape), (n, v), [n, n, m], [dma((4,))], flops=100_000_000
    )(pieces.reshape(piece_shape.shape), place, w_out)
    state = lax.all_to_all(state.reshape(stretches, 8, WIDTH), SP_TP, 0, 0, axis_index_groups=groups, tiled=True)
    state = state.reshape(HEADS * DQK, WIDTH)
    hidden = pltpu.VMEM((HALF, HEADS * DV), BF)
    sent, lower = call(
        sent_kernel,
        (shape((HALF, width), BF), half_shape),
        (n, v),
        [v, v, n, v, v, v, m],
        [hidden, dma((4,))],
        flops=1_000_000_000,
    )(query, ogate, state, numer, stats, upper, w_out)
    got = lax.ppermute(sent, "tp", [(0, 1), (1, 0)])
    kept = call(kept_kernel, shape((HALF, width), F32), n, [v, v, n, v, v, v, v], [hidden], flops=1_000_000_000)(
        query, ogate, state, numer, stats, upper, lower
    )
    return (kept + got.astype(F32)).astype(BF)


def solution(mesh):
    split = Mesh(mesh.devices.reshape(4, 4, 4, mesh.shape["tp"]), ("sp_0", "sp_1", "sp_2", "tp"))
    placed = (
        P(SP_TP, None),
        P(),
        P(None, "tp"),
        P(None, "tp"),
        P(None, "tp"),
        P(None, "tp"),
        P(),
        P(),
        P(),
        P(),
        P(None, SP, "tp"),
        P(),
        P("tp", None),
    )
    return jax.shard_map(body, mesh=split, in_specs=placed, out_specs=P(SP_TP, None), check_vma=False)
```

```python
import jax
import jax.numpy as jnp
import numpy as np
from jax import lax
from jax.experimental import pallas as pl
from jax.experimental.pallas import tpu as pltpu
from jax.sharding import Mesh
from jax.sharding import PartitionSpec as P


SPAN = 128
SP = ("sp_0", "sp_1", "sp_2")
SP_TP = ("sp_0", "sp_1", "sp_2", "tp")
EPS = 1e-06
EMPTY = -1e30
TAIL = 16
HEADS = 4
DQK = 128
DV = 256
WIDTH = DV + 128
BLOCKS = 3
ROWS = BLOCKS * SPAN
HALF = ROWS // 2
HIGHEST = lax.Precision.HIGHEST
BF = jnp.bfloat16
F32 = jnp.float32
MIB = 1 << 20


def call(kernel, outs, out_spaces, spaces, scratch=(), flops=0, limit=8):
    def spec(space):
        return pl.BlockSpec(memory_space=pltpu.VMEM if space is None else space)

    def placed(like, space):
        return like if space is None else space(like.shape, like.dtype)

    several = isinstance(outs, tuple)
    run = pl.pallas_call(
        kernel,
        out_shape=tuple(map(placed, outs, out_spaces)) if several else placed(outs, out_spaces),
        in_specs=[spec(space) for space in spaces],
        out_specs=tuple(map(spec, out_spaces)) if several else spec(out_spaces),
        scratch_shapes=list(scratch),
        cost_estimate=pl.CostEstimate(flops=flops, transcendentals=0, bytes_accessed=1 << 20),
        compiler_params=pltpu.CompilerParams(vmem_limit_bytes=limit * MIB),
    )

    def kept(x, space):
        return x if space is None else pltpu.with_memory_space_constraint(x, space)

    return lambda *args: run(*map(kept, args, spaces))


def started(pairs, sems):
    copies = [pltpu.make_async_copy(src, dst, sems.at[n]) for n, (src, dst) in enumerate(pairs)]
    for copy in copies:
        copy.start()
    return copies


def by_rows(src, dst, parts):
    rows = src.shape[0] // parts
    return [(src.at[pl.ds(c * rows, rows)], dst.at[pl.ds(c * rows, rows)]) for c in range(parts)]


def wait_all(copies):
    for copy in copies:
        copy.wait()


def thirds(x):
    hi = x.astype(BF).astype(F32)
    rest = x - hi
    mid = rest.astype(BF).astype(F32)
    return hi, mid, (rest - mid).astype(BF).astype(F32)


def lane_of(shape):
    return lax.broadcasted_iota(jnp.int32, shape, len(shape) - 1)


def mixed_rows(pre_ref, taps, lanes, first, rows):
    acc = None
    for j in range(4):
        term = taps[j : j + 1, lanes] * pre_ref[pl.ds(first + TAIL - 3 + j, rows), lanes]
        acc = term if acc is None else acc + term
    return acc * (1.0 / (1.0 + jnp.exp(-acc)))


def row_scale(x):
    return lax.rsqrt(jnp.mean(x * x, axis=-1, keepdims=True) + EPS)


def normalized(x, gain):
    x = x.astype(F32)
    return (x * row_scale(x) * gain).astype(BF)


def fetch_kernel(own_hbm, gain_hbm, wk_hbm, wv_hbm, rows_ref, wk_ref, wv_ref, own_ref, gain_ref, sems):
    copies = started(
        [(own_hbm, own_ref), (gain_hbm, gain_ref)] + by_rows(wk_hbm, wk_ref, 4) + by_rows(wv_hbm, wv_ref, 8), sems
    )
    copies[0].wait()
    parts = [slice(at, at + 48) for at in range(0, HALF, 48)]
    scales = [row_scale(own_ref[part, :].astype(F32)) for part in parts]
    copies[1].wait()
    gain = gain_ref[...]
    for part, scale in zip(parts, scales):
        rows_ref[part, :] = (own_ref[part, :].astype(F32) * scale * gain).astype(BF)
    wait_all(copies[2:])


def summary_kernel(own_ref, oth_ref, one_ref, two_ref, gain_ref, wk_ref, wv_ref, wi_ref, wf_ref, taps_ref, offs_ref,
                   key_out, value_out, logs_out, piece_ref, rows_out,
                   rows_ref, pre_ref, key_ref, value_ref, logs_ref, wg_ref, sems):
    outs = [
        pltpu.make_async_copy(src, dst, sems.at[n])
        for n, (src, dst) in enumerate(
            [(logs_ref, logs_out), (key_ref, key_out), (value_ref, value_out), (rows_ref, rows_out)]
        )
    ]
    tp = lax.axis_index("tp")
    gain = gain_ref[...]
    rows_ref[0:TAIL, :] = normalized(one_ref[...] + two_ref[...], gain)
    mine = pl.multiple_of(TAIL + tp * HALF, 16)
    rows_ref[pl.ds(mine, HALF), :] = own_ref[...]
    for part in range(HALF // 48):
        to = pl.multiple_of(TAIL + (1 - tp) * HALF + part * 48, 16)
        rows_ref[pl.ds(to, 48), :] = normalized(oth_ref[part * 48 : part * 48 + 48, :], gain)
    outs[3].start()
    all_heads = wi_ref.shape[0]
    wg_ref[...] = jnp.zeros_like(wg_ref)
    wg_ref[0:all_heads, :] = wi_ref[...]
    wg_ref[all_heads : 2 * all_heads, :] = wf_ref[...]
    own = pl.ds(TAIL, ROWS)
    gates = lax.dot_general(rows_ref[own, :], wg_ref[...], (((1,), (1,)), ((), ())), preferred_element_type=F32)
    gates = jnp.where(tp == 0, gates, pltpu.roll(gates, 128 - HEADS, 1))
    pre_ref[...] = jnp.dot(rows_ref[...], wk_ref[...], preferred_element_type=F32).astype(BF).astype(F32)

    lane = lane_of((SPAN, 128))
    tri = (lax.broadcasted_iota(jnp.int32, (SPAN, SPAN), 0) >= lax.broadcasted_iota(jnp.int32, (SPAN, SPAN), 1)).astype(F32)
    gate, inside, totals = [], [], []
    for b in range(BLOCKS):
        offs = jnp.zeros((1, 128), F32)
        for h in range(HEADS):
            for row, at in ((0, h), (1, 2 * HEADS + h)):
                offs = jnp.where(lane_of((1, 128)) == at, offs_ref[b, row : row + 1, h : h + 1], offs)
        g = gates[b * SPAN : (b + 1) * SPAN] + offs
        soft = jnp.minimum(g, 0.0) - jnp.log1p(jnp.exp(-jnp.abs(g)))
        total = jnp.dot(tri, soft, precision=HIGHEST, preferred_element_type=F32)
        logs_ref[b * SPAN : (b + 1) * SPAN, :] = jnp.where(lane < HEADS, g, pltpu.roll(total, 128 - HEADS, 1))
        total = pltpu.roll(total, 128 - 2 * HEADS, 1)
        gate.append(g)
        inside.append(total)
        totals.append(total[SPAN - 1 : SPAN, :])
    outs[0].start()
    write, level = [], None
    later = jnp.zeros_like(totals[0])
    for b in reversed(range(BLOCKS)):
        w = (totals[b] - inside[b]) + later + gate[b]
        later = later + totals[b]
        write.insert(0, w)
        top = jnp.max(w, axis=0, keepdims=True)
        level = top if level is None else jnp.maximum(level, top)
    weight = [jnp.exp(w - level) for w in write]
    numbers = thirds(later) + thirds(level)

    taps = taps_ref[:, pl.ds(pl.multiple_of(tp * (HEADS * DQK), 128), HEADS * DQK)].astype(F32)
    for h in range(HEADS):
        lanes = slice(h * DQK, (h + 1) * DQK)
        for b in range(BLOCKS):
            rows = slice(b * SPAN, (b + 1) * SPAN)
            key_ref[rows, lanes] = (mixed_rows(pre_ref, taps, lanes, b * SPAN, SPAN) * DQK**-0.5).astype(BF)
    outs[1].start()
    value_ref[...] = jnp.dot(rows_ref[own, :], wv_ref[...], preferred_element_type=F32).astype(BF)
    outs[2].start()
    ones = jnp.ones((ROWS, 128), BF)
    dims = (((0,), (0,)), ((), ()))
    for h in range(HEADS):
        lanes = slice(h * DQK, (h + 1) * DQK)
        weighted = jnp.concatenate(
            [
                (key_ref[b * SPAN : (b + 1) * SPAN, lanes].astype(F32) * weight[b][:, h : h + 1]).astype(BF)
                for b in range(BLOCKS)
            ],
            axis=0,
        )
        memory = lax.dot_general(weighted, value_ref[:, h * DV : (h + 1) * DV], dims, preferred_element_type=F32)
        extra = lax.dot_general(weighted, ones, dims, preferred_element_type=F32)
        for n, number in enumerate(numbers):
            extra = jnp.where(lane == n + 1, number[:, h : h + 1], extra)
        out = slice(h * DQK, (h + 1) * DQK)
        piece_ref[out, :DV] = memory.astype(BF)
        piece_ref[out, DV:] = extra.astype(BF)
    for copy in outs:
        copy.wait()


def prefix_kernel(piece_ref, place_ref, out_ref):
    count = piece_ref.shape[0] // 8
    tall = piece_ref.shape[0]

    def iota(shape, dim):
        return lax.broadcasted_iota(jnp.int32, shape, dim)

    def ones_where(test):
        return jnp.where(test, 1.0, 0.0).astype(BF)

    first = ones_where(iota((count, tall), 1) == 8 * iota((count, tall), 0))
    down = iota((tall, count), 0) - 8 * iota((tall, count), 1)
    spread = ones_where((down >= 0) & (down < 8))
    over = iota((count, tall), 1) - 8 * iota((count, tall), 0)
    spread_over = ones_where((over >= 0) & (over < 8))
    extra = jnp.dot(first, piece_ref[:, DV:], preferred_element_type=F32)
    lane = lane_of((count, 128))

    def number(at):
        return jnp.sum(jnp.where((lane >= at) & (lane < at + 3), extra, 0.0), axis=1, keepdims=True)

    forget, level = number(1), number(4)
    down, over = place_ref[0], place_ref[1]
    steps = jnp.where(down > over, forget, jnp.where(down == over, level, 0.0))
    earlier = over < down
    logs = jnp.dot(jnp.where(earlier, 1.0, 0.0), steps, precision=HIGHEST, preferred_element_type=F32)
    logs = jnp.where(earlier, logs, EMPTY)
    top = jnp.max(logs, axis=1, keepdims=True)
    weight = jnp.where(earlier, jnp.exp(logs - top), 0.0).astype(BF)
    weight = jnp.dot(weight, spread_over, preferred_element_type=F32).astype(BF)
    weight = jnp.dot(spread, weight, preferred_element_type=F32)
    same = (iota((tall, tall), 0) & 7) == (iota((tall, tall), 1) & 7)
    weight = jnp.where(same, weight, 0.0).astype(BF)
    marks = jnp.zeros((count, 128), F32)
    for n, mark in enumerate(thirds(top)):
        marks = jnp.where(lane == n + 1, mark, marks)
    marks = jnp.dot(spread, marks.astype(BF), preferred_element_type=F32)
    state = jnp.dot(weight, piece_ref[...], preferred_element_type=F32)
    lane = lane_of((tall, 128))
    out_ref[:, :DV] = state[:, :DV].astype(BF)
    out_ref[:, DV:] = jnp.where((lane >= 1) & (lane < 4), marks, state[:, DV:]).astype(BF)


def local_kernel(rows_hbm, wq_hbm, key_hbm, value_hbm, logs_hbm, wo_hbm, taps_ref, gain_ref,
                 query_ref, numer_ref, stats_ref, ogate_ref,
                 rows_ref, wq_ref, pre_ref, key_ref, value_ref, logs_ref, wo_ref, sems):
    copies = started(
        by_rows(rows_hbm, rows_ref, 5)
        + by_rows(wq_hbm, wq_ref, 4)
        + [(logs_hbm, logs_ref), (key_hbm, key_ref), (value_hbm, value_ref)]
        + by_rows(wo_hbm, wo_ref, 8),
        sems,
    )
    tp = lax.axis_index("tp")
    taps = taps_ref[:, pl.ds(pl.multiple_of(tp * (HEADS * DQK), 128), HEADS * DQK)].astype(F32)
    wait_all(copies[:9])
    pre_ref[...] = jnp.dot(rows_ref[...], wq_ref[...], preferred_element_type=F32).astype(BF).astype(F32)
    for h in range(HEADS):
        lanes = slice(h * DQK, (h + 1) * DQK)
        for b in range(BLOCKS):
            rows = slice(b * SPAN, (b + 1) * SPAN)
            query_ref[rows, lanes] = mixed_rows(pre_ref, taps, lanes, b * SPAN, SPAN).astype(BF)
    wait_all(copies[9:12])
    lane = lane_of((SPAN, 128))
    cols = [logs_ref[b * SPAN : (b + 1) * SPAN, :] for b in range(BLOCKS)]
    flat = [c.T for c in cols]
    ends = [c[SPAN - 1 : SPAN, :] for c in cols]
    causal = lax.broadcasted_iota(jnp.int32, (SPAN, SPAN), 0) >= lax.broadcasted_iota(jnp.int32, (SPAN, SPAN), 1)
    stats = []
    before = jnp.zeros_like(ends[0])
    for b in range(BLOCKS):
        carried = pltpu.roll(cols[b] + before, HEADS, 1)
        before = before + ends[b]
        stats.append(jnp.where((lane >= 2 * HEADS) & (lane < 3 * HEADS), carried, 0.0))
    nt = (((1,), (1,)), ((), ()))
    for h in range(HEADS):
        head = slice(h * DQK, (h + 1) * DQK)
        wide = slice(h * DV, (h + 1) * DV)
        for t in range(BLOCKS):
            rows = slice(t * SPAN, (t + 1) * SPAN)
            seen = (t + 1) * SPAN
            now = cols[t][:, HEADS + h : HEADS + h + 1]
            logs = []
            for s in range(t + 1):
                gate = flat[s][h : h + 1, :]
                past = flat[s][HEADS + h : HEADS + h + 1, :]
                if s == t:
                    logs.append(jnp.where(causal, (now - past) + gate, EMPTY))
                else:
                    rest = ends[s][:, HEADS + h : HEADS + h + 1] - past
                    for c in range(s + 1, t):
                        rest = rest + ends[c][:, HEADS + h : HEADS + h + 1]
                    logs.append(now + (rest + gate))
            top = None
            for x in logs:
                peak = jnp.max(x, axis=1, keepdims=True)
                top = peak if top is None else jnp.maximum(top, peak)
            weight = jnp.concatenate([jnp.exp(x - top) for x in logs], axis=1)
            scores = (
                lax.dot_general(query_ref[rows, head], key_ref[:seen, head], nt, preferred_element_type=F32) * weight
            )
            denom = jnp.sum(scores, axis=1, keepdims=True)
            numer = jnp.dot(scores.astype(BF), value_ref[:seen, wide], preferred_element_type=F32)
            numer_ref[rows, wide] = numer.astype(BF)
            stats[t] = jnp.where(lane == h, denom, jnp.where(lane == HEADS + h, top, stats[t]))
    for t in range(BLOCKS):
        stats_ref[t * SPAN : (t + 1) * SPAN, :] = stats[t]
    wait_all(copies[12:])
    gain = gain_ref[:, pl.ds(pl.multiple_of(tp * (HEADS * DV), 128), HEADS * DV)]
    for c in range(2):
        cols = slice(c * HEADS * DV // 2, (c + 1) * HEADS * DV // 2)
        pre = jnp.dot(rows_ref[pl.ds(TAIL, ROWS), :], wo_ref[:, cols], preferred_element_type=F32).astype(BF).astype(F32)
        ogate_ref[:, cols] = (gain[:, cols] / (1.0 + jnp.exp(-pre))).astype(BF)


def hidden_rows(first, query_ref, ogate_ref, state_ref, numer_ref, stats_ref, hidden_ref):
    rows = pl.ds(pl.multiple_of(first, 16), HALF)
    lane = lane_of((HALF, 128))
    stats = stats_ref[rows, :]
    place = lane_of((DQK, 128))
    norms, level = [], jnp.zeros((1, 128), F32)
    for h in range(HEADS):
        extra = state_ref[h * DQK : (h + 1) * DQK, DV:].astype(F32)
        norms.append(jnp.where(place == h, extra[:, 0:1], 0.0).astype(BF))
        mark = extra[0:1, 1:2] + extra[0:1, 2:3] + extra[0:1, 3:4]
        level = jnp.where(lane_of((1, 128)) == h, mark, level)
    norms = jnp.concatenate(norms, axis=0)
    query = query_ref[rows, :]
    read_norm = jnp.dot(query, norms, preferred_element_type=F32)
    top = pltpu.roll(stats, 128 - HEADS, 1)
    carried = pltpu.roll(stats, 128 - 2 * HEADS, 1) + level
    peak = jnp.maximum(carried, top)
    one = jnp.exp(carried - peak)
    two = jnp.exp(top - peak)
    denom = one * read_norm + two * stats
    denom = jnp.maximum(jnp.abs(denom), jnp.exp(-peak))
    one = one / denom
    two = two / denom
    for h in range(HEADS):
        wide = slice(h * DV, (h + 1) * DV)
        read = jnp.dot(
            query[:, h * DQK : (h + 1) * DQK], state_ref[h * DQK : (h + 1) * DQK, :DV], preferred_element_type=F32
        )
        cell = one[:, h : h + 1] * read + two[:, h : h + 1] * numer_ref[rows, wide].astype(F32)
        scale = lax.rsqrt(jnp.mean(cell * cell, axis=-1, keepdims=True) + EPS)
        hidden_ref[:, wide] = (cell * scale * ogate_ref[rows, wide].astype(F32)).astype(BF)


def sent_kernel(query_ref, ogate_ref, state_ref, numer_ref, stats_ref, wout_hbm, out_ref, wout_ref, hidden_ref, sems):
    deep = HEADS * DV // 2
    copies = started(by_rows(wout_hbm, wout_ref, 8), sems)
    first = (1 - lax.axis_index("tp")) * HALF
    hidden_rows(first, query_ref, ogate_ref, state_ref, numer_ref, stats_ref, hidden_ref)
    wait_all(copies[:4])
    part = jnp.dot(hidden_ref[:, :deep], wout_ref[:deep, :], preferred_element_type=F32)
    wait_all(copies[4:])
    out_ref[...] = (part + jnp.dot(hidden_ref[:, deep:], wout_ref[deep:, :], preferred_element_type=F32)).astype(BF)


def kept_kernel(query_ref, ogate_ref, state_ref, numer_ref, stats_ref, wout_ref, out_ref, hidden_ref):
    first = lax.axis_index("tp") * HALF
    hidden_rows(first, query_ref, ogate_ref, state_ref, numer_ref, stats_ref, hidden_ref)
    out_ref[...] = jnp.dot(hidden_ref[...], wout_ref[...], preferred_element_type=F32)


def far_first(stretches):
    at = np.arange(stretches)
    hops = sum(np.minimum(c, 4 - c) for c in (at // 16, at // 4 % 4, at % 4))
    return np.lexsort((at, -hops))


def body(
    tokens, norm_gain, w_query, w_key, w_value, w_ogate, w_igate, w_fgate, conv_query, conv_key, gate_offset, head_gain, w_out
):
    width = tokens.shape[1]
    stretches = lax.axis_size(SP)
    shape = jax.ShapeDtypeStruct
    other = lax.ppermute(tokens, "tp", [(0, 1), (1, 0)])
    last = tokens[HALF - TAIL :]
    to_second = lax.ppermute(last, SP_TP, [(2 * i + 1, 2 * i + 3) for i in range(stretches - 1)])
    to_first = lax.ppermute(last, SP_TP, [(2 * i + 1, 2 * i + 2) for i in range(stretches - 1)])
    gain = norm_gain.reshape(1, -1)
    head_gain = head_gain.reshape(1, -1)
    order = far_first(stretches)
    groups = [[2 * int(i) + t for i in order] for t in range(2)]
    place = np.stack([np.broadcast_to(order[:, None], (stretches, stretches)), np.broadcast_to(order, (stretches, stretches))])
    place = jnp.asarray(place.astype(np.int32))
    v, m, n = pltpu.VMEM, pltpu.HBM, None
    dma = pltpu.SemaphoreType.DMA
    key_shape, value_shape = shape((ROWS, HEADS * DQK), BF), shape((ROWS, HEADS * DV), BF)
    logs_shape = shape((ROWS, 128), F32)
    rows_shape, pre_shape = shape((TAIL + ROWS, width), BF), shape((TAIL + ROWS, HEADS * DQK), F32)

    def room(like):
        return pltpu.VMEM(like.shape, like.dtype)

    own, wk, wv = call(
        fetch_kernel,
        (shape(tokens.shape, BF), shape(w_key.shape, BF), shape(w_value.shape, BF)),
        (v, v, v),
        [m, m, m, m],
        [room(tokens), room(gain), dma((14,))],
        flops=1_000_000_000,
    )(tokens, gain, w_key, w_value)
    key, value, logs, pieces, rows = call(
        summary_kernel,
        (key_shape, value_shape, logs_shape, shape((HEADS * DQK, WIDTH), BF), rows_shape),
        (m, m, m, n, m),
        [v, n, n, n, n, v, v, n, n, n, n],
        [room(rows_shape), room(pre_shape), room(key_shape), room(value_shape), room(logs_shape), pltpu.VMEM((128, width), BF), dma((4,))],
        flops=3_000_000_000,
        limit=12,
    )(own, other, to_first, to_second, gain, wk, wv, w_igate.T, w_fgate.T, conv_key, gate_offset.transpose(1, 0, 2))
    pieces = lax.all_to_all(pieces.reshape(stretches, 8, WIDTH), SP_TP, 0, 0, axis_index_groups=groups, tiled=True)
    piece_shape = shape((stretches * 8, WIDTH), BF)
    state = call(prefix_kernel, piece_shape, n, [n, n], flops=100_000_000)(pieces.reshape(piece_shape.shape), place)
    state, rows = lax.optimization_barrier((state, rows))
    state = lax.all_to_all(state.reshape(stretches, 8, WIDTH), SP_TP, 0, 0, axis_index_groups=groups, tiled=True)
    state = state.reshape(HEADS * DQK, WIDTH)
    query, numer, stats, ogate = call(
        local_kernel,
        (key_shape, value_shape, logs_shape, value_shape),
        (v, v, v, v),
        [m, m, m, m, m, m, n, n],
        [room(rows_shape), room(w_query), room(pre_shape), room(key_shape), room(value_shape), room(logs_shape), room(w_ogate), dma((20,))],
        flops=6_000_000_000,
        limit=16,
    )(rows, w_query, key, value, logs, w_ogate, conv_query, head_gain)
    hidden = pltpu.VMEM((HALF, HEADS * DV), BF)
    sent, wout = call(
        sent_kernel,
        (shape((HALF, width), BF), shape(w_out.shape, BF)),
        (n, v),
        [v, v, n, v, v, m],
        [hidden, dma((8,))],
        flops=1_000_000_000,
    )(query, ogate, state, numer, stats, w_out)
    got = lax.ppermute(sent, "tp", [(0, 1), (1, 0)])
    kept = call(kept_kernel, shape((HALF, width), F32), n, [v, v, n, v, v, v], [hidden], flops=1_000_000_000)(
        query, ogate, state, numer, stats, wout
    )
    return (kept + got.astype(F32)).astype(BF)


def solution(mesh):
    split = Mesh(mesh.devices.reshape(4, 4, 4, mesh.shape["tp"]), ("sp_0", "sp_1", "sp_2", "tp"))
    placed = (
        P(SP_TP, None),
        P(),
        P(None, "tp"),
        P(None, "tp"),
        P(None, "tp"),
        P(None, "tp"),
        P(),
        P(),
        P(),
        P(),
        P(None, SP, "tp"),
        P(),
        P("tp", None),
    )
    return jax.shard_map(body, mesh=split, in_specs=placed, out_specs=P(SP_TP, None), check_vma=False)
```

```python
import jax
import jax.numpy as jnp
import numpy as np
from jax import lax
from jax.experimental import pallas as pl
from jax.experimental.pallas import tpu as pltpu
from jax.sharding import Mesh
from jax.sharding import PartitionSpec as P


SPAN = 128
SP = ("sp_0", "sp_1", "sp_2")
SP_TP = ("sp_0", "sp_1", "sp_2", "tp")
EPS = 1e-06
EMPTY = -1e30
TAIL = 16
HEADS = 4
DQK = 128
DV = 256
WIDTH = DV + 128
BLOCKS = 3
ROWS = BLOCKS * SPAN
HALF = ROWS // 2
HIGHEST = lax.Precision.HIGHEST
BF = jnp.bfloat16
F32 = jnp.float32
MIB = 1 << 20


def call(kernel, outs, out_spaces, spaces, scratch=(), flops=0, limit=8):
    def spec(space):
        return pl.BlockSpec(memory_space=pltpu.VMEM if space is None else space)

    def placed(like, space):
        return like if space is None else space(like.shape, like.dtype)

    several = isinstance(outs, tuple)
    run = pl.pallas_call(
        kernel,
        out_shape=tuple(map(placed, outs, out_spaces)) if several else placed(outs, out_spaces),
        in_specs=[spec(space) for space in spaces],
        out_specs=tuple(map(spec, out_spaces)) if several else spec(out_spaces),
        scratch_shapes=list(scratch),
        cost_estimate=pl.CostEstimate(flops=flops, transcendentals=0, bytes_accessed=1 << 20),
        compiler_params=pltpu.CompilerParams(vmem_limit_bytes=limit * MIB),
    )

    def kept(x, space):
        return x if space is None else pltpu.with_memory_space_constraint(x, space)

    return lambda *args: run(*map(kept, args, spaces))


def started(pairs, sems):
    copies = [pltpu.make_async_copy(src, dst, sems.at[n]) for n, (src, dst) in enumerate(pairs)]
    for copy in copies:
        copy.start()
    return copies


def by_rows(src, dst, parts):
    rows = src.shape[0] // parts
    return [(src.at[pl.ds(c * rows, rows)], dst.at[pl.ds(c * rows, rows)]) for c in range(parts)]


def wait_all(copies):
    for copy in copies:
        copy.wait()


def thirds(x):
    hi = x.astype(BF).astype(F32)
    rest = x - hi
    mid = rest.astype(BF).astype(F32)
    return hi, mid, (rest - mid).astype(BF).astype(F32)


def lane_of(shape):
    return lax.broadcasted_iota(jnp.int32, shape, len(shape) - 1)


def mixed_rows(pre_ref, taps, lanes, first, rows):
    acc = None
    for j in range(4):
        term = taps[j : j + 1, lanes] * pre_ref[pl.ds(first + TAIL - 3 + j, rows), lanes]
        acc = term if acc is None else acc + term
    return acc * (1.0 / (1.0 + jnp.exp(-acc)))


def row_scale(x):
    return lax.rsqrt(jnp.mean(x * x, axis=-1, keepdims=True) + EPS)


def normalized(x, gain):
    x = x.astype(F32)
    return (x * row_scale(x) * gain).astype(BF)


def fetch_kernel(own_hbm, gain_hbm, wk_hbm, rows_ref, wk_ref, own_ref, gain_ref, sems):
    copies = started([(own_hbm, own_ref), (gain_hbm, gain_ref)] + by_rows(wk_hbm, wk_ref, 4), sems)
    copies[0].wait()
    parts = [slice(at, at + 48) for at in range(0, HALF, 48)]
    scales = [row_scale(own_ref[part, :].astype(F32)) for part in parts]
    copies[1].wait()
    gain = gain_ref[...]
    for part, scale in zip(parts, scales):
        rows_ref[part, :] = (own_ref[part, :].astype(F32) * scale * gain).astype(BF)
    wait_all(copies[2:])


def summary_kernel(own_ref, oth_ref, one_ref, two_ref, gain_ref, wk_ref, wv_hbm, wi_ref, wf_ref, taps_ref, offs_ref,
                   key_out, value_out, logs_out, piece_ref, rows_out,
                   rows_ref, pre_ref, key_ref, value_ref, logs_ref, wg_ref, wv_ref, sems, in_sems):
    copies = started(by_rows(wv_hbm, wv_ref, 8), in_sems)
    outs = [
        pltpu.make_async_copy(src, dst, sems.at[n])
        for n, (src, dst) in enumerate(
            [(logs_ref, logs_out), (key_ref, key_out), (value_ref, value_out), (rows_ref, rows_out)]
        )
    ]
    tp = lax.axis_index("tp")
    gain = gain_ref[...]
    rows_ref[0:TAIL, :] = normalized(one_ref[...] + two_ref[...], gain)
    mine = pl.multiple_of(TAIL + tp * HALF, 16)
    rows_ref[pl.ds(mine, HALF), :] = own_ref[...]
    for part in range(HALF // 48):
        to = pl.multiple_of(TAIL + (1 - tp) * HALF + part * 48, 16)
        rows_ref[pl.ds(to, 48), :] = normalized(oth_ref[part * 48 : part * 48 + 48, :], gain)
    outs[3].start()
    all_heads = wi_ref.shape[0]
    wg_ref[...] = jnp.zeros_like(wg_ref)
    wg_ref[0:all_heads, :] = wi_ref[...]
    wg_ref[all_heads : 2 * all_heads, :] = wf_ref[...]
    own = pl.ds(TAIL, ROWS)
    gates = lax.dot_general(rows_ref[own, :], wg_ref[...], (((1,), (1,)), ((), ())), preferred_element_type=F32)
    gates = jnp.where(tp == 0, gates, pltpu.roll(gates, 128 - HEADS, 1))
    pre_ref[...] = jnp.dot(rows_ref[...], wk_ref[...], preferred_element_type=F32).astype(BF).astype(F32)
    wait_all(copies)

    lane = lane_of((SPAN, 128))
    tri = (lax.broadcasted_iota(jnp.int32, (SPAN, SPAN), 0) >= lax.broadcasted_iota(jnp.int32, (SPAN, SPAN), 1)).astype(F32)
    gate, inside, totals = [], [], []
    for b in range(BLOCKS):
        offs = jnp.zeros((1, 128), F32)
        for h in range(HEADS):
            for row, at in ((0, h), (1, 2 * HEADS + h)):
                offs = jnp.where(lane_of((1, 128)) == at, offs_ref[b, row : row + 1, h : h + 1], offs)
        g = gates[b * SPAN : (b + 1) * SPAN] + offs
        soft = jnp.minimum(g, 0.0) - jnp.log1p(jnp.exp(-jnp.abs(g)))
        total = jnp.dot(tri, soft, precision=HIGHEST, preferred_element_type=F32)
        logs_ref[b * SPAN : (b + 1) * SPAN, :] = jnp.where(lane < HEADS, g, pltpu.roll(total, 128 - HEADS, 1))
        total = pltpu.roll(total, 128 - 2 * HEADS, 1)
        gate.append(g)
        inside.append(total)
        totals.append(total[SPAN - 1 : SPAN, :])
    outs[0].start()
    write, level = [], None
    later = jnp.zeros_like(totals[0])
    for b in reversed(range(BLOCKS)):
        w = (totals[b] - inside[b]) + later + gate[b]
        later = later + totals[b]
        write.insert(0, w)
        top = jnp.max(w, axis=0, keepdims=True)
        level = top if level is None else jnp.maximum(level, top)
    weight = [jnp.exp(w - level) for w in write]
    numbers = thirds(later) + thirds(level)

    taps = taps_ref[:, pl.ds(pl.multiple_of(tp * (HEADS * DQK), 128), HEADS * DQK)].astype(F32)
    for h in range(HEADS):
        lanes = slice(h * DQK, (h + 1) * DQK)
        for b in range(BLOCKS):
            rows = slice(b * SPAN, (b + 1) * SPAN)
            key_ref[rows, lanes] = (mixed_rows(pre_ref, taps, lanes, b * SPAN, SPAN) * DQK**-0.5).astype(BF)
    outs[1].start()
    value_ref[...] = jnp.dot(rows_ref[own, :], wv_ref[...], preferred_element_type=F32).astype(BF)
    outs[2].start()
    ones = jnp.ones((ROWS, 128), BF)
    dims = (((0,), (0,)), ((), ()))
    for h in range(HEADS):
        lanes = slice(h * DQK, (h + 1) * DQK)
        weighted = jnp.concatenate(
            [
                (key_ref[b * SPAN : (b + 1) * SPAN, lanes].astype(F32) * weight[b][:, h : h + 1]).astype(BF)
                for b in range(BLOCKS)
            ],
            axis=0,
        )
        memory = lax.dot_general(weighted, value_ref[:, h * DV : (h + 1) * DV], dims, preferred_element_type=F32)
        extra = lax.dot_general(weighted, ones, dims, preferred_element_type=F32)
        for n, number in enumerate(numbers):
            extra = jnp.where(lane == n + 1, number[:, h : h + 1], extra)
        out = slice(h * DQK, (h + 1) * DQK)
        piece_ref[out, :DV] = memory.astype(BF)
        piece_ref[out, DV:] = extra.astype(BF)
    for copy in outs:
        copy.wait()


def prefix_kernel(piece_ref, place_ref, wout_hbm, out_ref, wout_ref, sems):
    copies = started(by_rows(wout_hbm.at[pl.ds(0, wout_ref.shape[0])], wout_ref, 4), sems)
    count = piece_ref.shape[0] // 8
    tall = piece_ref.shape[0]

    def iota(shape, dim):
        return lax.broadcasted_iota(jnp.int32, shape, dim)

    def ones_where(test):
        return jnp.where(test, 1.0, 0.0).astype(BF)

    first = ones_where(iota((count, tall), 1) == 8 * iota((count, tall), 0))
    down = iota((tall, count), 0) - 8 * iota((tall, count), 1)
    spread = ones_where((down >= 0) & (down < 8))
    over = iota((count, tall), 1) - 8 * iota((count, tall), 0)
    spread_over = ones_where((over >= 0) & (over < 8))
    extra = jnp.dot(first, piece_ref[:, DV:], preferred_element_type=F32)
    lane = lane_of((count, 128))

    def number(at):
        return jnp.sum(jnp.where((lane >= at) & (lane < at + 3), extra, 0.0), axis=1, keepdims=True)

    forget, level = number(1), number(4)
    down, over = place_ref[0], place_ref[1]
    steps = jnp.where(down > over, forget, jnp.where(down == over, level, 0.0))
    earlier = over < down
    logs = jnp.dot(jnp.where(earlier, 1.0, 0.0), steps, precision=HIGHEST, preferred_element_type=F32)
    logs = jnp.where(earlier, logs, EMPTY)
    top = jnp.max(logs, axis=1, keepdims=True)
    weight = jnp.where(earlier, jnp.exp(logs - top), 0.0).astype(BF)
    weight = jnp.dot(weight, spread_over, preferred_element_type=F32).astype(BF)
    weight = jnp.dot(spread, weight, preferred_element_type=F32)
    same = (iota((tall, tall), 0) & 7) == (iota((tall, tall), 1) & 7)
    weight = jnp.where(same, weight, 0.0).astype(BF)
    marks = jnp.zeros((count, 128), F32)
    for n, mark in enumerate(thirds(top)):
        marks = jnp.where(lane == n + 1, mark, marks)
    marks = jnp.dot(spread, marks.astype(BF), preferred_element_type=F32)
    state = jnp.dot(weight, piece_ref[...], preferred_element_type=F32)
    lane = lane_of((tall, 128))
    out_ref[:, :DV] = state[:, :DV].astype(BF)
    out_ref[:, DV:] = jnp.where((lane >= 1) & (lane < 4), marks, state[:, DV:]).astype(BF)
    wait_all(copies)


def local_kernel(rows_hbm, wq_hbm, key_hbm, value_hbm, logs_hbm, wo_hbm, taps_ref, gain_ref,
                 query_ref, numer_ref, stats_ref, ogate_ref,
                 rows_ref, wq_ref, pre_ref, key_ref, value_ref, logs_ref, wo_ref, sems):
    copies = started(
        by_rows(rows_hbm, rows_ref, 5)
        + by_rows(wq_hbm, wq_ref, 4)
        + [(logs_hbm, logs_ref), (key_hbm, key_ref), (value_hbm, value_ref)]
        + by_rows(wo_hbm, wo_ref, 8),
        sems,
    )
    tp = lax.axis_index("tp")
    taps = taps_ref[:, pl.ds(pl.multiple_of(tp * (HEADS * DQK), 128), HEADS * DQK)].astype(F32)
    wait_all(copies[:9])
    pre_ref[...] = jnp.dot(rows_ref[...], wq_ref[...], preferred_element_type=F32).astype(BF).astype(F32)
    for h in range(HEADS):
        lanes = slice(h * DQK, (h + 1) * DQK)
        for b in range(BLOCKS):
            rows = slice(b * SPAN, (b + 1) * SPAN)
            query_ref[rows, lanes] = mixed_rows(pre_ref, taps, lanes, b * SPAN, SPAN).astype(BF)
    wait_all(copies[9:12])
    lane = lane_of((SPAN, 128))
    cols = [logs_ref[b * SPAN : (b + 1) * SPAN, :] for b in range(BLOCKS)]
    flat = [c.T for c in cols]
    ends = [c[SPAN - 1 : SPAN, :] for c in cols]
    causal = lax.broadcasted_iota(jnp.int32, (SPAN, SPAN), 0) >= lax.broadcasted_iota(jnp.int32, (SPAN, SPAN), 1)
    stats = []
    before = jnp.zeros_like(ends[0])
    for b in range(BLOCKS):
        carried = pltpu.roll(cols[b] + before, HEADS, 1)
        before = before + ends[b]
        stats.append(jnp.where((lane >= 2 * HEADS) & (lane < 3 * HEADS), carried, 0.0))
    nt = (((1,), (1,)), ((), ()))
    for h in range(HEADS):
        head = slice(h * DQK, (h + 1) * DQK)
        wide = slice(h * DV, (h + 1) * DV)
        for t in range(BLOCKS):
            rows = slice(t * SPAN, (t + 1) * SPAN)
            seen = (t + 1) * SPAN
            now = cols[t][:, HEADS + h : HEADS + h + 1]
            logs = []
            for s in range(t + 1):
                gate = flat[s][h : h + 1, :]
                past = flat[s][HEADS + h : HEADS + h + 1, :]
                if s == t:
                    logs.append(jnp.where(causal, (now - past) + gate, EMPTY))
                else:
                    rest = ends[s][:, HEADS + h : HEADS + h + 1] - past
                    for c in range(s + 1, t):
                        rest = rest + ends[c][:, HEADS + h : HEADS + h + 1]
                    logs.append(now + (rest + gate))
            top = None
            for x in logs:
                peak = jnp.max(x, axis=1, keepdims=True)
                top = peak if top is None else jnp.maximum(top, peak)
            weight = jnp.concatenate([jnp.exp(x - top) for x in logs], axis=1)
            scores = (
                lax.dot_general(query_ref[rows, head], key_ref[:seen, head], nt, preferred_element_type=F32) * weight
            )
            denom = jnp.sum(scores, axis=1, keepdims=True)
            numer = jnp.dot(scores.astype(BF), value_ref[:seen, wide], preferred_element_type=F32)
            numer_ref[rows, wide] = numer.astype(BF)
            stats[t] = jnp.where(lane == h, denom, jnp.where(lane == HEADS + h, top, stats[t]))
    for t in range(BLOCKS):
        stats_ref[t * SPAN : (t + 1) * SPAN, :] = stats[t]
    wait_all(copies[12:])
    gain = gain_ref[:, pl.ds(pl.multiple_of(tp * (HEADS * DV), 128), HEADS * DV)]
    for c in range(2):
        cols = slice(c * HEADS * DV // 2, (c + 1) * HEADS * DV // 2)
        pre = jnp.dot(rows_ref[pl.ds(TAIL, ROWS), :], wo_ref[:, cols], preferred_element_type=F32).astype(BF).astype(F32)
        ogate_ref[:, cols] = (gain[:, cols] / (1.0 + jnp.exp(-pre))).astype(BF)


def hidden_rows(first, query_ref, ogate_ref, state_ref, numer_ref, stats_ref, hidden_ref):
    rows = pl.ds(pl.multiple_of(first, 16), HALF)
    lane = lane_of((HALF, 128))
    stats = stats_ref[rows, :]
    place = lane_of((DQK, 128))
    norms, level = [], jnp.zeros((1, 128), F32)
    for h in range(HEADS):
        extra = state_ref[h * DQK : (h + 1) * DQK, DV:].astype(F32)
        norms.append(jnp.where(place == h, extra[:, 0:1], 0.0).astype(BF))
        mark = extra[0:1, 1:2] + extra[0:1, 2:3] + extra[0:1, 3:4]
        level = jnp.where(lane_of((1, 128)) == h, mark, level)
    norms = jnp.concatenate(norms, axis=0)
    query = query_ref[rows, :]
    read_norm = jnp.dot(query, norms, preferred_element_type=F32)
    top = pltpu.roll(stats, 128 - HEADS, 1)
    carried = pltpu.roll(stats, 128 - 2 * HEADS, 1) + level
    peak = jnp.maximum(carried, top)
    one = jnp.exp(carried - peak)
    two = jnp.exp(top - peak)
    denom = one * read_norm + two * stats
    denom = jnp.maximum(jnp.abs(denom), jnp.exp(-peak))
    one = one / denom
    two = two / denom
    for h in range(HEADS):
        wide = slice(h * DV, (h + 1) * DV)
        read = jnp.dot(
            query[:, h * DQK : (h + 1) * DQK], state_ref[h * DQK : (h + 1) * DQK, :DV], preferred_element_type=F32
        )
        cell = one[:, h : h + 1] * read + two[:, h : h + 1] * numer_ref[rows, wide].astype(F32)
        scale = lax.rsqrt(jnp.mean(cell * cell, axis=-1, keepdims=True) + EPS)
        hidden_ref[:, wide] = (cell * scale * ogate_ref[rows, wide].astype(F32)).astype(BF)


def sent_kernel(query_ref, ogate_ref, state_ref, numer_ref, stats_ref, upper_ref, wout_hbm, out_ref, lower_ref, hidden_ref, sems):
    deep = upper_ref.shape[0]
    copies = started(by_rows(wout_hbm.at[pl.ds(deep, deep)], lower_ref, 4), sems)
    first = (1 - lax.axis_index("tp")) * HALF
    hidden_rows(first, query_ref, ogate_ref, state_ref, numer_ref, stats_ref, hidden_ref)
    part = jnp.dot(hidden_ref[:, :deep], upper_ref[...], preferred_element_type=F32)
    wait_all(copies)
    out_ref[...] = (part + jnp.dot(hidden_ref[:, deep:], lower_ref[...], preferred_element_type=F32)).astype(BF)


def kept_kernel(query_ref, ogate_ref, state_ref, numer_ref, stats_ref, upper_ref, lower_ref, out_ref, hidden_ref):
    deep = upper_ref.shape[0]
    first = lax.axis_index("tp") * HALF
    hidden_rows(first, query_ref, ogate_ref, state_ref, numer_ref, stats_ref, hidden_ref)
    part = jnp.dot(hidden_ref[:, :deep], upper_ref[...], preferred_element_type=F32)
    out_ref[...] = part + jnp.dot(hidden_ref[:, deep:], lower_ref[...], preferred_element_type=F32)


def far_first(stretches):
    at = np.arange(stretches)
    hops = sum(np.minimum(c, 4 - c) for c in (at // 16, at // 4 % 4, at % 4))
    return np.lexsort((at, -hops))


def body(
    tokens, norm_gain, w_query, w_key, w_value, w_ogate, w_igate, w_fgate, conv_query, conv_key, gate_offset, head_gain, w_out
):
    width = tokens.shape[1]
    stretches = lax.axis_size(SP)
    shape = jax.ShapeDtypeStruct
    other = lax.ppermute(tokens, "tp", [(0, 1), (1, 0)])
    last = tokens[HALF - TAIL :]
    to_second = lax.ppermute(last, SP_TP, [(2 * i + 1, 2 * i + 3) for i in range(stretches - 1)])
    to_first = lax.ppermute(last, SP_TP, [(2 * i + 1, 2 * i + 2) for i in range(stretches - 1)])
    gain = norm_gain.reshape(1, -1)
    head_gain = head_gain.reshape(1, -1)
    order = far_first(stretches)
    groups = [[2 * int(i) + t for i in order] for t in range(2)]
    place = np.stack([np.broadcast_to(order[:, None], (stretches, stretches)), np.broadcast_to(order, (stretches, stretches))])
    place = jnp.asarray(place.astype(np.int32))
    v, m, n = pltpu.VMEM, pltpu.HBM, None
    dma = pltpu.SemaphoreType.DMA
    key_shape, value_shape = shape((ROWS, HEADS * DQK), BF), shape((ROWS, HEADS * DV), BF)
    logs_shape = shape((ROWS, 128), F32)
    rows_shape, pre_shape = shape((TAIL + ROWS, width), BF), shape((TAIL + ROWS, HEADS * DQK), F32)

    def room(like):
        return pltpu.VMEM(like.shape, like.dtype)

    own, wk = call(
        fetch_kernel,
        (shape(tokens.shape, BF), shape(w_key.shape, BF)),
        (v, v),
        [m, m, m],
        [room(tokens), room(gain), dma((6,))],
        flops=1_000_000_000,
    )(tokens, gain, w_key)
    key, value, logs, pieces, rows = call(
        summary_kernel,
        (key_shape, value_shape, logs_shape, shape((HEADS * DQK, WIDTH), BF), rows_shape),
        (m, m, m, n, m),
        [v, n, n, n, n, v, m, n, n, n, n],
        [room(rows_shape), room(pre_shape), room(key_shape), room(value_shape), room(logs_shape), pltpu.VMEM((128, width), BF), room(w_value), dma((4,)), dma((8,))],
        flops=3_000_000_000,
        limit=16,
    )(own, other, to_first, to_second, gain, wk, w_value, w_igate.T, w_fgate.T, conv_key, gate_offset.transpose(1, 0, 2))
    pieces = lax.all_to_all(pieces.reshape(stretches, 8, WIDTH), SP_TP, 0, 0, axis_index_groups=groups, tiled=True)
    query, numer, stats, ogate = call(
        local_kernel,
        (key_shape, value_shape, logs_shape, value_shape),
        (v, v, v, v),
        [m, m, m, m, m, m, n, n],
        [room(rows_shape), room(w_query), room(pre_shape), room(key_shape), room(value_shape), room(logs_shape), room(w_ogate), dma((20,))],
        flops=6_000_000_000,
        limit=16,
    )(rows, w_query, key, value, logs, w_ogate, conv_query, head_gain)
    pieces, query, numer, stats, ogate = lax.optimization_barrier((pieces, query, numer, stats, ogate))
    piece_shape = shape((stretches * 8, WIDTH), BF)
    half_shape = shape((w_out.shape[0] // 2, width), BF)
    state, upper = call(
        prefix_kernel, (piece_shape, half_shape), (n, v), [n, n, m], [dma((4,))], flops=100_000_000
    )(pieces.reshape(piece_shape.shape), place, w_out)
    state = lax.all_to_all(state.reshape(stretches, 8, WIDTH), SP_TP, 0, 0, axis_index_groups=groups, tiled=True)
    state = state.reshape(HEADS * DQK, WIDTH)
    hidden = pltpu.VMEM((HALF, HEADS * DV), BF)
    sent, lower = call(
        sent_kernel,
        (shape((HALF, width), BF), half_shape),
        (n, v),
        [v, v, n, v, v, v, m],
        [hidden, dma((4,))],
        flops=1_000_000_000,
    )(query, ogate, state, numer, stats, upper, w_out)
    got = lax.ppermute(sent, "tp", [(0, 1), (1, 0)])
    kept = call(kept_kernel, shape((HALF, width), F32), n, [v, v, n, v, v, v, v], [hidden], flops=1_000_000_000)(
        query, ogate, state, numer, stats, upper, lower
    )
    return (kept + got.astype(F32)).astype(BF)


def solution(mesh):
    split = Mesh(mesh.devices.reshape(4, 4, 4, mesh.shape["tp"]), ("sp_0", "sp_1", "sp_2", "tp"))
    placed = (
        P(SP_TP, None),
        P(),
        P(None, "tp"),
        P(None, "tp"),
        P(None, "tp"),
        P(None, "tp"),
        P(),
        P(),
        P(),
        P(),
        P(None, SP, "tp"),
        P(),
        P("tp", None),
    )
    return jax.shard_map(body, mesh=split, in_specs=placed, out_specs=P(SP_TP, None), check_vma=False)
```

```python
import jax
import jax.numpy as jnp
import numpy as np
from jax import lax
from jax.experimental import pallas as pl
from jax.experimental.pallas import tpu as pltpu
from jax.sharding import Mesh
from jax.sharding import PartitionSpec as P


SPAN = 128
SP = ("sp_0", "sp_1", "sp_2")
SP_TP = ("sp_0", "sp_1", "sp_2", "tp")
EPS = 1e-06
EMPTY = -1e30
TAIL = 16
HEADS = 4
DQK = 128
DV = 256
WIDTH = DV + 128
BLOCKS = 3
ROWS = BLOCKS * SPAN
HALF = ROWS // 2
HIGHEST = lax.Precision.HIGHEST
BF = jnp.bfloat16
F32 = jnp.float32
MIB = 1 << 20


def call(kernel, outs, out_spaces, spaces, scratch=(), flops=0, limit=8, aliases=None):
    def spec(space):
        return pl.BlockSpec(memory_space=pltpu.VMEM if space is None else space)

    def placed(like, space):
        return like if space is None else space(like.shape, like.dtype)

    several = isinstance(outs, tuple)
    run = pl.pallas_call(
        kernel,
        out_shape=tuple(map(placed, outs, out_spaces)) if several else placed(outs, out_spaces),
        in_specs=[spec(space) for space in spaces],
        out_specs=tuple(map(spec, out_spaces)) if several else spec(out_spaces),
        scratch_shapes=list(scratch),
        input_output_aliases=aliases or {},
        cost_estimate=pl.CostEstimate(flops=flops, transcendentals=0, bytes_accessed=1 << 20),
        compiler_params=pltpu.CompilerParams(vmem_limit_bytes=limit * MIB),
    )

    def kept(x, space):
        return x if space is None else pltpu.with_memory_space_constraint(x, space)

    return lambda *args: run(*map(kept, args, spaces))


def started(pairs, sems):
    copies = [pltpu.make_async_copy(src, dst, sems.at[n]) for n, (src, dst) in enumerate(pairs)]
    for copy in copies:
        copy.start()
    return copies


def by_rows(src, dst, parts):
    rows = src.shape[0] // parts
    return [(src.at[pl.ds(c * rows, rows)], dst.at[pl.ds(c * rows, rows)]) for c in range(parts)]


def wait_all(copies):
    for copy in copies:
        copy.wait()


def thirds(x):
    hi = x.astype(BF).astype(F32)
    rest = x - hi
    mid = rest.astype(BF).astype(F32)
    return hi, mid, (rest - mid).astype(BF).astype(F32)


def lane_of(shape):
    return lax.broadcasted_iota(jnp.int32, shape, len(shape) - 1)


def mixed_rows(pre_ref, taps, lanes, first, rows):
    acc = None
    for j in range(4):
        term = taps[j : j + 1, lanes] * pre_ref[pl.ds(first + TAIL - 3 + j, rows), lanes]
        acc = term if acc is None else acc + term
    return acc * (1.0 / (1.0 + jnp.exp(-acc)))


def row_scale(x):
    return lax.rsqrt(jnp.mean(x * x, axis=-1, keepdims=True) + EPS)


def normalized(x, gain):
    x = x.astype(F32)
    return (x * row_scale(x) * gain).astype(BF)


def fetch_kernel(own_hbm, gain_hbm, wk_hbm, wv_hbm, wi_hbm, wf_hbm,
                 rows_ref, wk_ref, wv_ref, wg_ref, gates_ref, own_ref, gain_ref, wi_ref, wf_ref, flat_ref, sems):
    copies = started(
        [(own_hbm, own_ref), (gain_hbm, gain_ref), (wi_hbm, wi_ref), (wf_hbm, wf_ref)]
        + by_rows(wk_hbm, wk_ref, 4)
        + by_rows(wv_hbm, wv_ref, 8),
        sems,
    )
    copies[0].wait()
    parts = [slice(at, at + 48) for at in range(0, HALF, 48)]
    scales = [row_scale(own_ref[part, :].astype(F32)) for part in parts]
    copies[1].wait()
    gain = gain_ref[...]
    for part, scale in zip(parts, scales):
        rows_ref[part, :] = (own_ref[part, :].astype(F32) * scale * gain).astype(BF)
    wait_all(copies[2:4])
    all_heads = wi_ref.shape[0]
    flat_ref[...] = jnp.zeros_like(flat_ref)
    flat_ref[0:all_heads, :] = wi_ref[...].astype(F32)
    flat_ref[all_heads : 2 * all_heads, :] = wf_ref[...].astype(F32)
    for at in range(0, wg_ref.shape[0], 128):
        wg_ref[at : at + 128, :] = flat_ref[:, at : at + 128].T.astype(BF)
    gates_ref[...] = jnp.dot(rows_ref[...], wg_ref[...], preferred_element_type=F32)
    wait_all(copies[4:])


def summary_kernel(own_ref, oth_ref, one_ref, two_ref, gain_ref, wk_ref, wv_ref, wg_ref, gates_ref, taps_ref, offs_ref,
                   key_ref, value_ref, logs_ref, piece_ref, rows_ref, pre_ref, both_ref):
    tp = lax.axis_index("tp")
    gain = gain_ref[...]
    rows_ref[0:TAIL, :] = normalized(one_ref[...] + two_ref[...], gain)
    mine = pl.multiple_of(TAIL + tp * HALF, 16)
    rows_ref[pl.ds(mine, HALF), :] = own_ref[...]
    for part in range(HALF // 48):
        to = pl.multiple_of(TAIL + (1 - tp) * HALF + part * 48, 16)
        rows_ref[pl.ds(to, 48), :] = normalized(oth_ref[part * 48 : part * 48 + 48, :], gain)
    own = pl.ds(TAIL, ROWS)
    theirs = pl.multiple_of((1 - tp) * HALF, 8)
    both_ref[pl.ds(pl.multiple_of(tp * HALF, 8), HALF), :] = gates_ref[...]
    both_ref[pl.ds(theirs, HALF), :] = jnp.dot(
        rows_ref[pl.ds(pl.multiple_of(TAIL + (1 - tp) * HALF, 16), HALF), :], wg_ref[...], preferred_element_type=F32
    )
    gates = both_ref[...]
    gates = jnp.where(tp == 0, gates, pltpu.roll(gates, 128 - HEADS, 1))
    pre_ref[...] = jnp.dot(rows_ref[...], wk_ref[...], preferred_element_type=F32).astype(BF).astype(F32)

    lane = lane_of((SPAN, 128))
    tri = (lax.broadcasted_iota(jnp.int32, (SPAN, SPAN), 0) >= lax.broadcasted_iota(jnp.int32, (SPAN, SPAN), 1)).astype(F32)
    gate, inside, totals = [], [], []
    for b in range(BLOCKS):
        offs = jnp.zeros((1, 128), F32)
        for h in range(HEADS):
            for row, at in ((0, h), (1, 2 * HEADS + h)):
                offs = jnp.where(lane_of((1, 128)) == at, offs_ref[b, row : row + 1, h : h + 1], offs)
        g = gates[b * SPAN : (b + 1) * SPAN] + offs
        soft = jnp.minimum(g, 0.0) - jnp.log1p(jnp.exp(-jnp.abs(g)))
        total = jnp.dot(tri, soft, precision=HIGHEST, preferred_element_type=F32)
        logs_ref[b * SPAN : (b + 1) * SPAN, :] = jnp.where(lane < HEADS, g, pltpu.roll(total, 128 - HEADS, 1))
        total = pltpu.roll(total, 128 - 2 * HEADS, 1)
        gate.append(g)
        inside.append(total)
        totals.append(total[SPAN - 1 : SPAN, :])
    write, level = [], None
    later = jnp.zeros_like(totals[0])
    for b in reversed(range(BLOCKS)):
        w = (totals[b] - inside[b]) + later + gate[b]
        later = later + totals[b]
        write.insert(0, w)
        top = jnp.max(w, axis=0, keepdims=True)
        level = top if level is None else jnp.maximum(level, top)
    weight = [jnp.exp(w - level) for w in write]
    numbers = thirds(later) + thirds(level)

    taps = taps_ref[:, pl.ds(pl.multiple_of(tp * (HEADS * DQK), 128), HEADS * DQK)].astype(F32)
    for h in range(HEADS):
        lanes = slice(h * DQK, (h + 1) * DQK)
        for b in range(BLOCKS):
            rows = slice(b * SPAN, (b + 1) * SPAN)
            key_ref[rows, lanes] = (mixed_rows(pre_ref, taps, lanes, b * SPAN, SPAN) * DQK**-0.5).astype(BF)
    value_ref[...] = jnp.dot(rows_ref[own, :], wv_ref[...], preferred_element_type=F32).astype(BF)
    ones = jnp.ones((ROWS, 128), BF)
    dims = (((0,), (0,)), ((), ()))
    for h in range(HEADS):
        lanes = slice(h * DQK, (h + 1) * DQK)
        weighted = jnp.concatenate(
            [
                (key_ref[b * SPAN : (b + 1) * SPAN, lanes].astype(F32) * weight[b][:, h : h + 1]).astype(BF)
                for b in range(BLOCKS)
            ],
            axis=0,
        )
        memory = lax.dot_general(weighted, value_ref[:, h * DV : (h + 1) * DV], dims, preferred_element_type=F32)
        extra = lax.dot_general(weighted, ones, dims, preferred_element_type=F32)
        for n, number in enumerate(numbers):
            extra = jnp.where(lane == n + 1, number[:, h : h + 1], extra)
        out = slice(h * DQK, (h + 1) * DQK)
        piece_ref[out, :DV] = memory.astype(BF)
        piece_ref[out, DV:] = extra.astype(BF)


def prefix_kernel(piece_ref, place_ref, wout_hbm, out_ref, wout_ref, sems):
    copies = started(by_rows(wout_hbm.at[pl.ds(0, wout_ref.shape[0])], wout_ref, 4), sems)
    count = piece_ref.shape[0] // 8
    tall = piece_ref.shape[0]

    def iota(shape, dim):
        return lax.broadcasted_iota(jnp.int32, shape, dim)

    def ones_where(test):
        return jnp.where(test, 1.0, 0.0).astype(BF)

    first = ones_where(iota((count, tall), 1) == 8 * iota((count, tall), 0))
    down = iota((tall, count), 0) - 8 * iota((tall, count), 1)
    spread = ones_where((down >= 0) & (down < 8))
    over = iota((count, tall), 1) - 8 * iota((count, tall), 0)
    spread_over = ones_where((over >= 0) & (over < 8))
    extra = jnp.dot(first, piece_ref[:, DV:], preferred_element_type=F32)
    lane = lane_of((count, 128))

    def number(at):
        return jnp.sum(jnp.where((lane >= at) & (lane < at + 3), extra, 0.0), axis=1, keepdims=True)

    forget, level = number(1), number(4)
    down, over = place_ref[0], place_ref[1]
    steps = jnp.where(down > over, forget, jnp.where(down == over, level, 0.0))
    earlier = over < down
    logs = jnp.dot(jnp.where(earlier, 1.0, 0.0), steps, precision=HIGHEST, preferred_element_type=F32)
    logs = jnp.where(earlier, logs, EMPTY)
    top = jnp.max(logs, axis=1, keepdims=True)
    weight = jnp.where(earlier, jnp.exp(logs - top), 0.0).astype(BF)
    weight = jnp.dot(weight, spread_over, preferred_element_type=F32).astype(BF)
    weight = jnp.dot(spread, weight, preferred_element_type=F32)
    same = (iota((tall, tall), 0) & 7) == (iota((tall, tall), 1) & 7)
    weight = jnp.where(same, weight, 0.0).astype(BF)
    marks = jnp.zeros((count, 128), F32)
    for n, mark in enumerate(thirds(top)):
        marks = jnp.where(lane == n + 1, mark, marks)
    marks = jnp.dot(spread, marks.astype(BF), preferred_element_type=F32)
    state = jnp.dot(weight, piece_ref[...], preferred_element_type=F32)
    lane = lane_of((tall, 128))
    out_ref[:, :DV] = state[:, :DV].astype(BF)
    out_ref[:, DV:] = jnp.where((lane >= 1) & (lane < 4), marks, state[:, DV:]).astype(BF)
    wait_all(copies)


def local_kernel(rows_ref, wq_hbm, key_ref, value_ref, logs_ref, wo_hbm, taps_ref, gain_ref,
                 query_out, wide_out, stats_ref, query_ref, numer_ref, ogate_ref, wq_ref, pre_ref, wo_ref, sems):
    copies = started(by_rows(wq_hbm, wq_ref, 4) + by_rows(wo_hbm, wo_ref, 8), sems)
    tp = lax.axis_index("tp")
    taps = taps_ref[:, pl.ds(pl.multiple_of(tp * (HEADS * DQK), 128), HEADS * DQK)].astype(F32)
    wait_all(copies[:4])
    pre_ref[...] = jnp.dot(rows_ref[...], wq_ref[...], preferred_element_type=F32).astype(BF).astype(F32)
    for h in range(HEADS):
        lanes = slice(h * DQK, (h + 1) * DQK)
        for b in range(BLOCKS):
            rows = slice(b * SPAN, (b + 1) * SPAN)
            query_ref[rows, lanes] = mixed_rows(pre_ref, taps, lanes, b * SPAN, SPAN).astype(BF)
    lane = lane_of((SPAN, 128))
    cols = [logs_ref[b * SPAN : (b + 1) * SPAN, :] for b in range(BLOCKS)]
    flat = [c.T for c in cols]
    ends = [c[SPAN - 1 : SPAN, :] for c in cols]
    causal = lax.broadcasted_iota(jnp.int32, (SPAN, SPAN), 0) >= lax.broadcasted_iota(jnp.int32, (SPAN, SPAN), 1)
    stats = []
    before = jnp.zeros_like(ends[0])
    for b in range(BLOCKS):
        carried = pltpu.roll(cols[b] + before, HEADS, 1)
        before = before + ends[b]
        stats.append(jnp.where((lane >= 2 * HEADS) & (lane < 3 * HEADS), carried, 0.0))
    nt = (((1,), (1,)), ((), ()))
    for h in range(HEADS):
        head = slice(h * DQK, (h + 1) * DQK)
        wide = slice(h * DV, (h + 1) * DV)
        for t in range(BLOCKS):
            rows = slice(t * SPAN, (t + 1) * SPAN)
            seen = (t + 1) * SPAN
            now = cols[t][:, HEADS + h : HEADS + h + 1]
            logs = []
            for s in range(t + 1):
                gate = flat[s][h : h + 1, :]
                past = flat[s][HEADS + h : HEADS + h + 1, :]
                if s == t:
                    logs.append(jnp.where(causal, (now - past) + gate, EMPTY))
                else:
                    rest = ends[s][:, HEADS + h : HEADS + h + 1] - past
                    for c in range(s + 1, t):
                        rest = rest + ends[c][:, HEADS + h : HEADS + h + 1]
                    logs.append(now + (rest + gate))
            top = None
            for x in logs:
                peak = jnp.max(x, axis=1, keepdims=True)
                top = peak if top is None else jnp.maximum(top, peak)
            weight = jnp.concatenate([jnp.exp(x - top) for x in logs], axis=1)
            scores = (
                lax.dot_general(query_ref[rows, head], key_ref[:seen, head], nt, preferred_element_type=F32) * weight
            )
            denom = jnp.sum(scores, axis=1, keepdims=True)
            numer = jnp.dot(scores.astype(BF), value_ref[:seen, wide], preferred_element_type=F32)
            numer_ref[rows, wide] = numer.astype(BF)
            stats[t] = jnp.where(lane == h, denom, jnp.where(lane == HEADS + h, top, stats[t]))
    for t in range(BLOCKS):
        stats_ref[t * SPAN : (t + 1) * SPAN, :] = stats[t]
    wait_all(copies[4:])
    gain = gain_ref[:, pl.ds(pl.multiple_of(tp * (HEADS * DV), 128), HEADS * DV)]
    for c in range(2):
        cols = slice(c * HEADS * DV // 2, (c + 1) * HEADS * DV // 2)
        pre = jnp.dot(rows_ref[pl.ds(TAIL, ROWS), :], wo_ref[:, cols], preferred_element_type=F32).astype(BF).astype(F32)
        ogate_ref[:, cols] = (gain[:, cols] / (1.0 + jnp.exp(-pre))).astype(BF)
    query_out[...] = query_ref[...]
    wide_out[0:ROWS, : HEADS * DV] = numer_ref[...]
    wide_out[0:ROWS, HEADS * DV :] = ogate_ref[...]


def hidden_rows(first, query_ref, wide_ref, state_ref, stats_ref, hidden_ref):
    rows = pl.ds(pl.multiple_of(first, 16), HALF)
    lane = lane_of((HALF, 128))
    stats = stats_ref[rows, :]
    place = lane_of((DQK, 128))
    norms, level = [], jnp.zeros((1, 128), F32)
    for h in range(HEADS):
        extra = state_ref[h * DQK : (h + 1) * DQK, DV:].astype(F32)
        norms.append(jnp.where(place == h, extra[:, 0:1], 0.0).astype(BF))
        mark = extra[0:1, 1:2] + extra[0:1, 2:3] + extra[0:1, 3:4]
        level = jnp.where(lane_of((1, 128)) == h, mark, level)
    norms = jnp.concatenate(norms, axis=0)
    query = query_ref[rows, :]
    read_norm = jnp.dot(query, norms, preferred_element_type=F32)
    top = pltpu.roll(stats, 128 - HEADS, 1)
    carried = pltpu.roll(stats, 128 - 2 * HEADS, 1) + level
    peak = jnp.maximum(carried, top)
    one = jnp.exp(carried - peak)
    two = jnp.exp(top - peak)
    denom = one * read_norm + two * stats
    denom = jnp.maximum(jnp.abs(denom), jnp.exp(-peak))
    one = one / denom
    two = two / denom
    for h in range(HEADS):
        wide = slice(h * DV, (h + 1) * DV)
        read = jnp.dot(
            query[:, h * DQK : (h + 1) * DQK], state_ref[h * DQK : (h + 1) * DQK, :DV], preferred_element_type=F32
        )
        cell = one[:, h : h + 1] * read + two[:, h : h + 1] * wide_ref[rows, wide].astype(F32)
        scale = lax.rsqrt(jnp.mean(cell * cell, axis=-1, keepdims=True) + EPS)
        hidden_ref[:, wide] = (cell * scale * wide_ref[rows, HEADS * DV + h * DV : HEADS * DV + (h + 1) * DV].astype(F32)).astype(BF)


def sent_kernel(query_ref, wide_ref, state_ref, stats_ref, upper_ref, wout_hbm, out_ref, lower_ref, hidden_ref, sems):
    deep = upper_ref.shape[0]
    copies = started(by_rows(wout_hbm.at[pl.ds(deep, deep)], lower_ref, 4), sems)
    first = (1 - lax.axis_index("tp")) * HALF
    hidden_rows(first, query_ref, wide_ref, state_ref, stats_ref, hidden_ref)
    part = jnp.dot(hidden_ref[:, :deep], upper_ref[...], preferred_element_type=F32)
    wait_all(copies)
    out_ref[...] = (part + jnp.dot(hidden_ref[:, deep:], lower_ref[...], preferred_element_type=F32)).astype(BF)


def kept_kernel(query_ref, wide_ref, state_ref, stats_ref, upper_ref, lower_ref, out_ref, hidden_ref):
    deep = upper_ref.shape[0]
    first = lax.axis_index("tp") * HALF
    hidden_rows(first, query_ref, wide_ref, state_ref, stats_ref, hidden_ref)
    part = jnp.dot(hidden_ref[:, :deep], upper_ref[...], preferred_element_type=F32)
    out_ref[...] = part + jnp.dot(hidden_ref[:, deep:], lower_ref[...], preferred_element_type=F32)


def far_first(stretches):
    at = np.arange(stretches)
    hops = sum(np.minimum(c, 4 - c) for c in (at // 16, at // 4 % 4, at % 4))
    return np.lexsort((at, -hops))


def body(
    tokens, norm_gain, w_query, w_key, w_value, w_ogate, w_igate, w_fgate, conv_query, conv_key, gate_offset, head_gain, w_out
):
    width = tokens.shape[1]
    stretches = lax.axis_size(SP)
    shape = jax.ShapeDtypeStruct
    other = lax.ppermute(tokens, "tp", [(0, 1), (1, 0)])
    last = tokens[HALF - TAIL :]
    to_second = lax.ppermute(last, SP_TP, [(2 * i + 1, 2 * i + 3) for i in range(stretches - 1)])
    to_first = lax.ppermute(last, SP_TP, [(2 * i + 1, 2 * i + 2) for i in range(stretches - 1)])
    gain = norm_gain.reshape(1, -1)
    head_gain = head_gain.reshape(1, -1)
    order = far_first(stretches)
    groups = [[2 * int(i) + t for i in order] for t in range(2)]
    place = np.stack([np.broadcast_to(order[:, None], (stretches, stretches)), np.broadcast_to(order, (stretches, stretches))])
    place = jnp.asarray(place.astype(np.int32))
    v, m, n = pltpu.VMEM, pltpu.HBM, None
    dma = pltpu.SemaphoreType.DMA
    key_shape, value_shape = shape((ROWS, HEADS * DQK), BF), shape((ROWS, HEADS * DV), BF)
    logs_shape = shape((ROWS, 128), F32)
    rows_shape, pre_shape = shape((TAIL + ROWS, width), BF), shape((TAIL + ROWS, HEADS * DQK), F32)

    def room(like):
        return pltpu.VMEM(like.shape, like.dtype)

    gates_shape = shape((width, 128), BF), shape((HALF, 128), F32)
    own, wk, wv, wg, gates = call(
        fetch_kernel,
        (shape(tokens.shape, BF), shape(w_key.shape, BF), shape(w_value.shape, BF), *gates_shape),
        (v, v, v, v, v),
        [m, m, m, m, m, m],
        [room(tokens), room(gain), *[pltpu.VMEM((w_igate.shape[1], width), BF)] * 2, pltpu.VMEM((128, width), F32), dma((16,))],
        flops=1_000_000_000,
    )(tokens, gain, w_key, w_value, w_igate.T, w_fgate.T)
    key, value, logs, pieces, rows = call(
        summary_kernel,
        (key_shape, value_shape, logs_shape, shape((HEADS * DQK, WIDTH), BF), rows_shape),
        (v, v, v, n, v),
        [v, n, n, n, n, v, v, v, v, n, n],
        [room(pre_shape), room(logs_shape)],
        flops=3_000_000_000,
    )(own, other, to_first, to_second, gain, wk, wv, wg, gates, conv_key, gate_offset.transpose(1, 0, 2))
    pieces = lax.all_to_all(pieces.reshape(stretches, 8, WIDTH), SP_TP, 0, 0, axis_index_groups=groups, tiled=True)
    query, wide, stats = call(
        local_kernel,
        (key_shape, rows_shape, logs_shape),
        (v, v, v),
        [v, m, v, v, v, m, n, n],
        [room(key_shape), room(value_shape), room(value_shape), room(w_query), room(pre_shape), room(w_ogate), dma((12,))],
        flops=6_000_000_000,
        limit=16,
        aliases={2: 0, 0: 1, 4: 2},
    )(rows, w_query, key, value, logs, w_ogate, conv_query, head_gain)
    pieces, query, wide, stats = lax.optimization_barrier((pieces, query, wide, stats))
    piece_shape = shape((stretches * 8, WIDTH), BF)
    half_shape = shape((w_out.shape[0] // 2, width), BF)
    state, upper = call(
        prefix_kernel, (piece_shape, half_shape), (n, v), [n, n, m], [dma((4,))], flops=100_000_000
    )(pieces.reshape(piece_shape.shape), place, w_out)
    state = lax.all_to_all(state.reshape(stretches, 8, WIDTH), SP_TP, 0, 0, axis_index_groups=groups, tiled=True)
    state = state.reshape(HEADS * DQK, WIDTH)
    hidden = pltpu.VMEM((HALF, HEADS * DV), BF)
    sent, lower = call(
        sent_kernel,
        (shape((HALF, width), BF), half_shape),
        (n, v),
        [v, v, n, v, v, m],
        [hidden, dma((4,))],
        flops=1_000_000_000,
    )(query, wide, state, stats, upper, w_out)
    got = lax.ppermute(sent, "tp", [(0, 1), (1, 0)])
    kept = call(kept_kernel, shape((HALF, width), F32), n, [v, v, n, v, v, v], [hidden], flops=1_000_000_000)(
        query, wide, state, stats, upper, lower
    )
    return (kept + got.astype(F32)).astype(BF)


def solution(mesh):
    split = Mesh(mesh.devices.reshape(4, 4, 4, mesh.shape["tp"]), ("sp_0", "sp_1", "sp_2", "tp"))
    placed = (
        P(SP_TP, None),
        P(),
        P(None, "tp"),
        P(None, "tp"),
        P(None, "tp"),
        P(None, "tp"),
        P(),
        P(),
        P(),
        P(),
        P(None, SP, "tp"),
        P(),
        P("tp", None),
    )
    return jax.shard_map(body, mesh=split, in_specs=placed, out_specs=P(SP_TP, None), check_vma=False)
```

```python
import jax
import jax.numpy as jnp
import numpy as np
from jax import lax
from jax.experimental import pallas as pl
from jax.experimental.pallas import tpu as pltpu
from jax.sharding import Mesh
from jax.sharding import PartitionSpec as P


SPAN = 128
SP = ("sp_0", "sp_1", "sp_2")
SP_TP = ("sp_0", "sp_1", "sp_2", "tp")
EPS = 1e-06
EMPTY = -1e30
TAIL = 16
HEADS = 4
DQK = 128
DV = 256
WIDTH = DV + 128
BLOCKS = 3
ROWS = BLOCKS * SPAN
HALF = ROWS // 2
HIGHEST = lax.Precision.HIGHEST
BF = jnp.bfloat16
F32 = jnp.float32
MIB = 1 << 20


def call(kernel, outs, out_spaces, spaces, scratch=(), flops=0, limit=8, aliases=None):
    def spec(space):
        return pl.BlockSpec(memory_space=pltpu.VMEM if space is None else space)

    def placed(like, space):
        return like if space is None else space(like.shape, like.dtype)

    several = isinstance(outs, tuple)
    run = pl.pallas_call(
        kernel,
        out_shape=tuple(map(placed, outs, out_spaces)) if several else placed(outs, out_spaces),
        in_specs=[spec(space) for space in spaces],
        out_specs=tuple(map(spec, out_spaces)) if several else spec(out_spaces),
        scratch_shapes=list(scratch),
        input_output_aliases=aliases or {},
        cost_estimate=pl.CostEstimate(flops=flops, transcendentals=0, bytes_accessed=1 << 20),
        compiler_params=pltpu.CompilerParams(vmem_limit_bytes=limit * MIB),
    )

    def kept(x, space):
        return x if space is None else pltpu.with_memory_space_constraint(x, space)

    return lambda *args: run(*map(kept, args, spaces))


def started(pairs, sems):
    copies = [pltpu.make_async_copy(src, dst, sems.at[n]) for n, (src, dst) in enumerate(pairs)]
    for copy in copies:
        copy.start()
    return copies


def by_rows(src, dst, parts):
    rows = src.shape[0] // parts
    return [(src.at[pl.ds(c * rows, rows)], dst.at[pl.ds(c * rows, rows)]) for c in range(parts)]


def wait_all(copies):
    for copy in copies:
        copy.wait()


def thirds(x):
    hi = x.astype(BF).astype(F32)
    rest = x - hi
    mid = rest.astype(BF).astype(F32)
    return hi, mid, (rest - mid).astype(BF).astype(F32)


def lane_of(shape):
    return lax.broadcasted_iota(jnp.int32, shape, len(shape) - 1)


def mixed_rows(pre_ref, taps, lanes, first, rows):
    acc = None
    for j in range(4):
        term = taps[j : j + 1, lanes] * pre_ref[pl.ds(first + TAIL - 3 + j, rows), lanes]
        acc = term if acc is None else acc + term
    return acc * (1.0 / (1.0 + jnp.exp(-acc)))


def row_scale(x):
    return lax.rsqrt(jnp.mean(x * x, axis=-1, keepdims=True) + EPS)


def normalized(x, gain):
    x = x.astype(F32)
    return (x * row_scale(x) * gain).astype(BF)


def fetch_kernel(own_hbm, gain_hbm, wk_hbm, wv_hbm, wi_hbm, wf_hbm,
                 rows_ref, wk_ref, wv_ref, wg_ref, gates_ref, own_ref, gain_ref, wi_ref, wf_ref, flat_ref, sems):
    copies = started(
        [(own_hbm, own_ref), (gain_hbm, gain_ref), (wi_hbm, wi_ref), (wf_hbm, wf_ref)]
        + by_rows(wk_hbm, wk_ref, 4)
        + by_rows(wv_hbm, wv_ref, 8),
        sems,
    )
    copies[0].wait()
    parts = [slice(at, at + 48) for at in range(0, HALF, 48)]
    scales = [row_scale(own_ref[part, :].astype(F32)) for part in parts]
    copies[1].wait()
    gain = gain_ref[...]
    for part, scale in zip(parts, scales):
        rows_ref[part, :] = (own_ref[part, :].astype(F32) * scale * gain).astype(BF)
    wait_all(copies[2:4])
    all_heads = wi_ref.shape[0]
    flat_ref[...] = jnp.zeros_like(flat_ref)
    flat_ref[0:all_heads, :] = wi_ref[...].astype(F32)
    flat_ref[all_heads : 2 * all_heads, :] = wf_ref[...].astype(F32)
    for at in range(0, wg_ref.shape[0], 128):
        wg_ref[at : at + 128, :] = flat_ref[:, at : at + 128].T.astype(BF)
    gates_ref[...] = jnp.dot(rows_ref[...], wg_ref[...], preferred_element_type=F32)
    wait_all(copies[4:])


def summary_kernel(own_ref, oth_ref, one_ref, two_ref, gain_ref, wk_ref, wv_ref, wg_ref, gates_ref, taps_ref, offs_ref,
                   key_ref, value_ref, logs_ref, piece_ref, rows_ref, pre_ref, both_ref):
    tp = lax.axis_index("tp")
    gain = gain_ref[...]
    rows_ref[0:TAIL, :] = normalized(one_ref[...] + two_ref[...], gain)
    mine = pl.multiple_of(TAIL + tp * HALF, 16)
    rows_ref[pl.ds(mine, HALF), :] = own_ref[...]
    for part in range(HALF // 48):
        to = pl.multiple_of(TAIL + (1 - tp) * HALF + part * 48, 16)
        rows_ref[pl.ds(to, 48), :] = normalized(oth_ref[part * 48 : part * 48 + 48, :], gain)
    own = pl.ds(TAIL, ROWS)
    theirs = pl.multiple_of((1 - tp) * HALF, 8)
    both_ref[pl.ds(pl.multiple_of(tp * HALF, 8), HALF), :] = gates_ref[...]
    both_ref[pl.ds(theirs, HALF), :] = jnp.dot(
        rows_ref[pl.ds(pl.multiple_of(TAIL + (1 - tp) * HALF, 16), HALF), :], wg_ref[...], preferred_element_type=F32
    )
    gates = both_ref[...]
    gates = jnp.where(tp == 0, gates, pltpu.roll(gates, 128 - HEADS, 1))
    pre_ref[...] = jnp.dot(rows_ref[...], wk_ref[...], preferred_element_type=F32).astype(BF).astype(F32)

    lane = lane_of((SPAN, 128))
    tri = (lax.broadcasted_iota(jnp.int32, (SPAN, SPAN), 0) >= lax.broadcasted_iota(jnp.int32, (SPAN, SPAN), 1)).astype(F32)
    gate, inside, totals = [], [], []
    for b in range(BLOCKS):
        offs = jnp.zeros((1, 128), F32)
        for h in range(HEADS):
            for row, at in ((0, h), (1, 2 * HEADS + h)):
                offs = jnp.where(lane_of((1, 128)) == at, offs_ref[b, row : row + 1, h : h + 1], offs)
        g = gates[b * SPAN : (b + 1) * SPAN] + offs
        soft = jnp.minimum(g, 0.0) - jnp.log1p(jnp.exp(-jnp.abs(g)))
        total = jnp.dot(tri, soft, precision=HIGHEST, preferred_element_type=F32)
        logs_ref[b * SPAN : (b + 1) * SPAN, :] = jnp.where(lane < HEADS, g, pltpu.roll(total, 128 - HEADS, 1))
        total = pltpu.roll(total, 128 - 2 * HEADS, 1)
        gate.append(g)
        inside.append(total)
        totals.append(total[SPAN - 1 : SPAN, :])
    write, level = [], None
    later = jnp.zeros_like(totals[0])
    for b in reversed(range(BLOCKS)):
        w = (totals[b] - inside[b]) + later + gate[b]
        later = later + totals[b]
        write.insert(0, w)
        top = jnp.max(w, axis=0, keepdims=True)
        level = top if level is None else jnp.maximum(level, top)
    weight = [jnp.exp(w - level) for w in write]
    numbers = thirds(later) + thirds(level)

    taps = taps_ref[:, pl.ds(pl.multiple_of(tp * (HEADS * DQK), 128), HEADS * DQK)].astype(F32)
    for h in range(HEADS):
        lanes = slice(h * DQK, (h + 1) * DQK)
        for b in range(BLOCKS):
            rows = slice(b * SPAN, (b + 1) * SPAN)
            key_ref[rows, lanes] = (mixed_rows(pre_ref, taps, lanes, b * SPAN, SPAN) * DQK**-0.5).astype(BF)
    value_ref[...] = jnp.dot(rows_ref[own, :], wv_ref[...], preferred_element_type=F32).astype(BF)
    ones = jnp.ones((ROWS, 128), BF)
    dims = (((0,), (0,)), ((), ()))
    for h in range(HEADS):
        lanes = slice(h * DQK, (h + 1) * DQK)
        weighted = jnp.concatenate(
            [
                (key_ref[b * SPAN : (b + 1) * SPAN, lanes].astype(F32) * weight[b][:, h : h + 1]).astype(BF)
                for b in range(BLOCKS)
            ],
            axis=0,
        )
        memory = lax.dot_general(weighted, value_ref[:, h * DV : (h + 1) * DV], dims, preferred_element_type=F32)
        extra = lax.dot_general(weighted, ones, dims, preferred_element_type=F32)
        for n, number in enumerate(numbers):
            extra = jnp.where(lane == n + 1, number[:, h : h + 1], extra)
        out = slice(h * DQK, (h + 1) * DQK)
        piece_ref[out, :DV] = memory.astype(BF)
        piece_ref[out, DV:] = extra.astype(BF)


def prefix_kernel(piece_ref, place_ref, out_ref):
    count = piece_ref.shape[0] // 8
    tall = piece_ref.shape[0]

    def iota(shape, dim):
        return lax.broadcasted_iota(jnp.int32, shape, dim)

    def ones_where(test):
        return jnp.where(test, 1.0, 0.0).astype(BF)

    first = ones_where(iota((count, tall), 1) == 8 * iota((count, tall), 0))
    down = iota((tall, count), 0) - 8 * iota((tall, count), 1)
    spread = ones_where((down >= 0) & (down < 8))
    over = iota((count, tall), 1) - 8 * iota((count, tall), 0)
    spread_over = ones_where((over >= 0) & (over < 8))
    extra = jnp.dot(first, piece_ref[:, DV:], preferred_element_type=F32)
    lane = lane_of((count, 128))

    def number(at):
        return jnp.sum(jnp.where((lane >= at) & (lane < at + 3), extra, 0.0), axis=1, keepdims=True)

    forget, level = number(1), number(4)
    down, over = place_ref[0], place_ref[1]
    steps = jnp.where(down > over, forget, jnp.where(down == over, level, 0.0))
    earlier = over < down
    logs = jnp.dot(jnp.where(earlier, 1.0, 0.0), steps, precision=HIGHEST, preferred_element_type=F32)
    logs = jnp.where(earlier, logs, EMPTY)
    top = jnp.max(logs, axis=1, keepdims=True)
    weight = jnp.where(earlier, jnp.exp(logs - top), 0.0).astype(BF)
    weight = jnp.dot(weight, spread_over, preferred_element_type=F32).astype(BF)
    weight = jnp.dot(spread, weight, preferred_element_type=F32)
    same = (iota((tall, tall), 0) & 7) == (iota((tall, tall), 1) & 7)
    weight = jnp.where(same, weight, 0.0).astype(BF)
    marks = jnp.zeros((count, 128), F32)
    for n, mark in enumerate(thirds(top)):
        marks = jnp.where(lane == n + 1, mark, marks)
    marks = jnp.dot(spread, marks.astype(BF), preferred_element_type=F32)
    state = jnp.dot(weight, piece_ref[...], preferred_element_type=F32)
    lane = lane_of((tall, 128))
    out_ref[:, :DV] = state[:, :DV].astype(BF)
    out_ref[:, DV:] = jnp.where((lane >= 1) & (lane < 4), marks, state[:, DV:]).astype(BF)


def local_kernel(rows_ref, wq_hbm, key_ref, value_ref, logs_ref, taps_ref,
                 query_out, numer_out, stats_ref, query_ref, numer_ref, wq_ref, pre_ref, sems):
    copies = started(by_rows(wq_hbm, wq_ref, 4), sems)
    tp = lax.axis_index("tp")
    taps = taps_ref[:, pl.ds(pl.multiple_of(tp * (HEADS * DQK), 128), HEADS * DQK)].astype(F32)
    wait_all(copies)
    pre_ref[...] = jnp.dot(rows_ref[...], wq_ref[...], preferred_element_type=F32).astype(BF).astype(F32)
    for h in range(HEADS):
        lanes = slice(h * DQK, (h + 1) * DQK)
        for b in range(BLOCKS):
            rows = slice(b * SPAN, (b + 1) * SPAN)
            query_ref[rows, lanes] = mixed_rows(pre_ref, taps, lanes, b * SPAN, SPAN).astype(BF)
    lane = lane_of((SPAN, 128))
    cols = [logs_ref[b * SPAN : (b + 1) * SPAN, :] for b in range(BLOCKS)]
    flat = [c.T for c in cols]
    ends = [c[SPAN - 1 : SPAN, :] for c in cols]
    causal = lax.broadcasted_iota(jnp.int32, (SPAN, SPAN), 0) >= lax.broadcasted_iota(jnp.int32, (SPAN, SPAN), 1)
    stats = []
    before = jnp.zeros_like(ends[0])
    for b in range(BLOCKS):
        carried = pltpu.roll(cols[b] + before, HEADS, 1)
        before = before + ends[b]
        stats.append(jnp.where((lane >= 2 * HEADS) & (lane < 3 * HEADS), carried, 0.0))
    nt = (((1,), (1,)), ((), ()))
    for h in range(HEADS):
        head = slice(h * DQK, (h + 1) * DQK)
        wide = slice(h * DV, (h + 1) * DV)
        for t in range(BLOCKS):
            rows = slice(t * SPAN, (t + 1) * SPAN)
            seen = (t + 1) * SPAN
            now = cols[t][:, HEADS + h : HEADS + h + 1]
            logs = []
            for s in range(t + 1):
                gate = flat[s][h : h + 1, :]
                past = flat[s][HEADS + h : HEADS + h + 1, :]
                if s == t:
                    logs.append(jnp.where(causal, (now - past) + gate, EMPTY))
                else:
                    rest = ends[s][:, HEADS + h : HEADS + h + 1] - past
                    for c in range(s + 1, t):
                        rest = rest + ends[c][:, HEADS + h : HEADS + h + 1]
                    logs.append(now + (rest + gate))
            top = None
            for x in logs:
                peak = jnp.max(x, axis=1, keepdims=True)
                top = peak if top is None else jnp.maximum(top, peak)
            weight = jnp.concatenate([jnp.exp(x - top) for x in logs], axis=1)
            scores = (
                lax.dot_general(query_ref[rows, head], key_ref[:seen, head], nt, preferred_element_type=F32) * weight
            )
            denom = jnp.sum(scores, axis=1, keepdims=True)
            numer = jnp.dot(scores.astype(BF), value_ref[:seen, wide], preferred_element_type=F32)
            numer_ref[rows, wide] = numer.astype(BF)
            stats[t] = jnp.where(lane == h, denom, jnp.where(lane == HEADS + h, top, stats[t]))
    for t in range(BLOCKS):
        stats_ref[t * SPAN : (t + 1) * SPAN, :] = stats[t]
    query_out[...] = query_ref[...]
    numer_out[...] = numer_ref[...]


def gate_kernel(rows_ref, wo_hbm, gain_ref, wide_out, wo_ref, ogate_ref, sems):
    wide = HEADS * DV // 2
    pairs = []
    for c in range(2):
        cols = pl.ds(c * wide, wide)
        pairs += by_rows(wo_hbm.at[:, cols], wo_ref.at[:, cols], 4)
    copies = started(pairs, sems)
    tp = lax.axis_index("tp")
    gain = gain_ref[:, pl.ds(pl.multiple_of(tp * (HEADS * DV), 128), HEADS * DV)]
    for c in range(2):
        wait_all(copies[4 * c : 4 * c + 4])
        cols = slice(c * wide, (c + 1) * wide)
        pre = jnp.dot(rows_ref[pl.ds(TAIL, ROWS), :], wo_ref[:, cols], preferred_element_type=F32).astype(BF).astype(F32)
        ogate_ref[:, cols] = (gain[:, cols] / (1.0 + jnp.exp(-pre))).astype(BF)
    wide_out[0:ROWS, : HEADS * DV] = ogate_ref[...]


def hidden_rows(first, query_ref, wide_ref, state_ref, numer_ref, stats_ref, hidden_ref):
    rows = pl.ds(pl.multiple_of(first, 16), HALF)
    lane = lane_of((HALF, 128))
    stats = stats_ref[rows, :]
    place = lane_of((DQK, 128))
    norms, level = [], jnp.zeros((1, 128), F32)
    for h in range(HEADS):
        extra = state_ref[h * DQK : (h + 1) * DQK, DV:].astype(F32)
        norms.append(jnp.where(place == h, extra[:, 0:1], 0.0).astype(BF))
        mark = extra[0:1, 1:2] + extra[0:1, 2:3] + extra[0:1, 3:4]
        level = jnp.where(lane_of((1, 128)) == h, mark, level)
    norms = jnp.concatenate(norms, axis=0)
    query = query_ref[rows, :]
    read_norm = jnp.dot(query, norms, preferred_element_type=F32)
    top = pltpu.roll(stats, 128 - HEADS, 1)
    carried = pltpu.roll(stats, 128 - 2 * HEADS, 1) + level
    peak = jnp.maximum(carried, top)
    one = jnp.exp(carried - peak)
    two = jnp.exp(top - peak)
    denom = one * read_norm + two * stats
    denom = jnp.maximum(jnp.abs(denom), jnp.exp(-peak))
    one = one / denom
    two = two / denom
    for h in range(HEADS):
        wide = slice(h * DV, (h + 1) * DV)
        read = jnp.dot(
            query[:, h * DQK : (h + 1) * DQK], state_ref[h * DQK : (h + 1) * DQK, :DV], preferred_element_type=F32
        )
        cell = one[:, h : h + 1] * read + two[:, h : h + 1] * numer_ref[rows, wide].astype(F32)
        scale = lax.rsqrt(jnp.mean(cell * cell, axis=-1, keepdims=True) + EPS)
        hidden_ref[:, wide] = (cell * scale * wide_ref[rows, wide].astype(F32)).astype(BF)


def sent_kernel(query_ref, wide_ref, state_ref, numer_ref, stats_ref, wout_hbm, out_ref, wout_ref, hidden_ref, sems):
    deep = HEADS * DV // 2
    copies = started(by_rows(wout_hbm, wout_ref, 8), sems)
    first = (1 - lax.axis_index("tp")) * HALF
    hidden_rows(first, query_ref, wide_ref, state_ref, numer_ref, stats_ref, hidden_ref)
    wait_all(copies[:4])
    part = jnp.dot(hidden_ref[:, :deep], wout_ref[:deep, :], preferred_element_type=F32)
    wait_all(copies[4:])
    out_ref[...] = (part + jnp.dot(hidden_ref[:, deep:], wout_ref[deep:, :], preferred_element_type=F32)).astype(BF)


def kept_kernel(query_ref, wide_ref, state_ref, numer_ref, stats_ref, wout_ref, out_ref, hidden_ref):
    first = lax.axis_index("tp") * HALF
    hidden_rows(first, query_ref, wide_ref, state_ref, numer_ref, stats_ref, hidden_ref)
    out_ref[...] = jnp.dot(hidden_ref[...], wout_ref[...], preferred_element_type=F32)


def far_first(stretches):
    at = np.arange(stretches)
    hops = sum(np.minimum(c, 4 - c) for c in (at // 16, at // 4 % 4, at % 4))
    return np.lexsort((at, -hops))


def body(
    tokens, norm_gain, w_query, w_key, w_value, w_ogate, w_igate, w_fgate, conv_query, conv_key, gate_offset, head_gain, w_out
):
    width = tokens.shape[1]
    stretches = lax.axis_size(SP)
    shape = jax.ShapeDtypeStruct
    other = lax.ppermute(tokens, "tp", [(0, 1), (1, 0)])
    last = tokens[HALF - TAIL :]
    to_second = lax.ppermute(last, SP_TP, [(2 * i + 1, 2 * i + 3) for i in range(stretches - 1)])
    to_first = lax.ppermute(last, SP_TP, [(2 * i + 1, 2 * i + 2) for i in range(stretches - 1)])
    gain = norm_gain.reshape(1, -1)
    head_gain = head_gain.reshape(1, -1)
    order = far_first(stretches)
    groups = [[2 * int(i) + t for i in order] for t in range(2)]
    place = np.stack([np.broadcast_to(order[:, None], (stretches, stretches)), np.broadcast_to(order, (stretches, stretches))])
    place = jnp.asarray(place.astype(np.int32))
    v, m, n = pltpu.VMEM, pltpu.HBM, None
    dma = pltpu.SemaphoreType.DMA
    key_shape, value_shape = shape((ROWS, HEADS * DQK), BF), shape((ROWS, HEADS * DV), BF)
    logs_shape = shape((ROWS, 128), F32)
    rows_shape, pre_shape = shape((TAIL + ROWS, width), BF), shape((TAIL + ROWS, HEADS * DQK), F32)

    def room(like):
        return pltpu.VMEM(like.shape, like.dtype)

    gates_shape = shape((width, 128), BF), shape((HALF, 128), F32)
    own, wk, wv, wg, gates = call(
        fetch_kernel,
        (shape(tokens.shape, BF), shape(w_key.shape, BF), shape(w_value.shape, BF), *gates_shape),
        (v, v, v, v, v),
        [m, m, m, m, m, m],
        [room(tokens), room(gain), *[pltpu.VMEM((w_igate.shape[1], width), BF)] * 2, pltpu.VMEM((128, width), F32), dma((16,))],
        flops=1_000_000_000,
    )(tokens, gain, w_key, w_value, w_igate.T, w_fgate.T)
    key, value, logs, pieces, rows = call(
        summary_kernel,
        (key_shape, value_shape, logs_shape, shape((HEADS * DQK, WIDTH), BF), rows_shape),
        (v, v, v, n, v),
        [v, n, n, n, n, v, v, v, v, n, n],
        [room(pre_shape), room(logs_shape)],
        flops=3_000_000_000,
    )(own, other, to_first, to_second, gain, wk, wv, wg, gates, conv_key, gate_offset.transpose(1, 0, 2))
    pieces = lax.all_to_all(pieces.reshape(stretches, 8, WIDTH), SP_TP, 0, 0, axis_index_groups=groups, tiled=True)
    query, numer, stats = call(
        local_kernel,
        (key_shape, value_shape, logs_shape),
        (v, v, v),
        [v, m, v, v, v, n],
        [room(key_shape), room(value_shape), room(w_query), room(pre_shape), dma((4,))],
        flops=4_000_000_000,
        limit=10,
        aliases={2: 0, 3: 1, 4: 2},
    )(rows, w_query, key, value, logs, conv_query)
    pieces, query, numer, stats = lax.optimization_barrier((pieces, query, numer, stats))
    piece_shape = shape((stretches * 8, WIDTH), BF)
    state = call(prefix_kernel, piece_shape, n, [n, n], flops=100_000_000)(pieces.reshape(piece_shape.shape), place)
    state, rows = lax.optimization_barrier((state, rows))
    state = lax.all_to_all(state.reshape(stretches, 8, WIDTH), SP_TP, 0, 0, axis_index_groups=groups, tiled=True)
    state = state.reshape(HEADS * DQK, WIDTH)
    wide = call(
        gate_kernel,
        rows_shape,
        v,
        [v, m, n],
        [room(w_ogate), room(value_shape), dma((8,))],
        flops=4_000_000_000,
        limit=10,
        aliases={0: 0},
    )(rows, w_ogate, head_gain)
    hidden = pltpu.VMEM((HALF, HEADS * DV), BF)
    sent, wout = call(
        sent_kernel,
        (shape((HALF, width), BF), shape(w_out.shape, BF)),
        (n, v),
        [v, v, n, v, v, m],
        [hidden, dma((8,))],
        flops=1_000_000_000,
    )(query, wide, state, numer, stats, w_out)
    got = lax.ppermute(sent, "tp", [(0, 1), (1, 0)])
    kept = call(kept_kernel, shape((HALF, width), F32), n, [v, v, n, v, v, v], [hidden], flops=1_000_000_000)(
        query, wide, state, numer, stats, wout
    )
    return (kept + got.astype(F32)).astype(BF)


def solution(mesh):
    split = Mesh(mesh.devices.reshape(4, 4, 4, mesh.shape["tp"]), ("sp_0", "sp_1", "sp_2", "tp"))
    placed = (
        P(SP_TP, None),
        P(),
        P(None, "tp"),
        P(None, "tp"),
        P(None, "tp"),
        P(None, "tp"),
        P(),
        P(),
        P(),
        P(),
        P(None, SP, "tp"),
        P(),
        P("tp", None),
    )
    return jax.shard_map(body, mesh=split, in_specs=placed, out_specs=P(SP_TP, None), check_vma=False)
```

```python
import jax
import jax.numpy as jnp
import numpy as np
from jax import lax
from jax.experimental import pallas as pl
from jax.experimental.pallas import tpu as pltpu
from jax.sharding import Mesh
from jax.sharding import PartitionSpec as P


SPAN = 128
SP = ("sp_0", "sp_1", "sp_2")
SP_TP = ("sp_0", "sp_1", "sp_2", "tp")
EPS = 1e-06
EMPTY = -1e30
TAIL = 16
HEADS = 4
DQK = 128
DV = 256
WIDTH = DV + 128
BLOCKS = 3
ROWS = BLOCKS * SPAN
HALF = ROWS // 2
HIGHEST = lax.Precision.HIGHEST
BF = jnp.bfloat16
F32 = jnp.float32
MIB = 1 << 20


def call(kernel, outs, out_spaces, spaces, scratch=(), flops=0, limit=8, aliases=None):
    def spec(space):
        return pl.BlockSpec(memory_space=pltpu.VMEM if space is None else space)

    def placed(like, space):
        return like if space is None else space(like.shape, like.dtype)

    several = isinstance(outs, tuple)
    run = pl.pallas_call(
        kernel,
        out_shape=tuple(map(placed, outs, out_spaces)) if several else placed(outs, out_spaces),
        in_specs=[spec(space) for space in spaces],
        out_specs=tuple(map(spec, out_spaces)) if several else spec(out_spaces),
        scratch_shapes=list(scratch),
        input_output_aliases=aliases or {},
        cost_estimate=pl.CostEstimate(flops=flops, transcendentals=0, bytes_accessed=1 << 20),
        compiler_params=pltpu.CompilerParams(vmem_limit_bytes=limit * MIB),
    )

    def kept(x, space):
        return x if space is None else pltpu.with_memory_space_constraint(x, space)

    return lambda *args: run(*map(kept, args, spaces))


def started(pairs, sems):
    copies = [pltpu.make_async_copy(src, dst, sems.at[n]) for n, (src, dst) in enumerate(pairs)]
    for copy in copies:
        copy.start()
    return copies


def by_rows(src, dst, parts):
    rows = src.shape[0] // parts
    return [(src.at[pl.ds(c * rows, rows)], dst.at[pl.ds(c * rows, rows)]) for c in range(parts)]


def wait_all(copies):
    for copy in copies:
        copy.wait()


def thirds(x):
    hi = x.astype(BF).astype(F32)
    rest = x - hi
    mid = rest.astype(BF).astype(F32)
    return hi, mid, (rest - mid).astype(BF).astype(F32)


def lane_of(shape):
    return lax.broadcasted_iota(jnp.int32, shape, len(shape) - 1)


def mixed_rows(pre_ref, taps, lanes, first, rows):
    acc = None
    for j in range(4):
        term = taps[j : j + 1, lanes] * pre_ref[pl.ds(first + TAIL - 3 + j, rows), lanes]
        acc = term if acc is None else acc + term
    return acc * (1.0 / (1.0 + jnp.exp(-acc)))


def row_scale(x):
    return lax.rsqrt(jnp.mean(x * x, axis=-1, keepdims=True) + EPS)


def normalized(x, gain):
    x = x.astype(F32)
    return (x * row_scale(x) * gain).astype(BF)


def last_kernel(own_hbm, out_ref, sems):
    wait_all(started([(own_hbm.at[pl.ds(HALF - TAIL, TAIL)], out_ref)], sems))


def fetch_kernel(own_hbm, gain_hbm, wi_hbm, wf_hbm,
                 rows_ref, wg_ref, gates_ref, own_ref, gain_ref, wi_ref, wf_ref, flat_ref, sems):
    copies = started(
        [(own_hbm, own_ref), (gain_hbm, gain_ref), (wi_hbm, wi_ref), (wf_hbm, wf_ref)],
        sems,
    )
    copies[0].wait()
    parts = [slice(at, at + 48) for at in range(0, HALF, 48)]
    scales = [row_scale(own_ref[part, :].astype(F32)) for part in parts]
    copies[1].wait()
    gain = gain_ref[...]
    for part, scale in zip(parts, scales):
        rows_ref[part, :] = (own_ref[part, :].astype(F32) * scale * gain).astype(BF)
    wait_all(copies[2:4])
    all_heads = wi_ref.shape[0]
    flat_ref[...] = jnp.zeros_like(flat_ref)
    flat_ref[0:all_heads, :] = wi_ref[...].astype(F32)
    flat_ref[all_heads : 2 * all_heads, :] = wf_ref[...].astype(F32)
    for at in range(0, wg_ref.shape[0], 128):
        wg_ref[at : at + 128, :] = flat_ref[:, at : at + 128].T.astype(BF)
    gates_ref[...] = jnp.dot(rows_ref[...], wg_ref[...], preferred_element_type=F32)


def summary_kernel(own_ref, oth_ref, one_ref, two_ref, gain_ref, wk_ref, wv_ref, wg_ref, gates_ref, taps_ref, offs_ref,
                   key_ref, value_ref, logs_ref, piece_out, rows_ref, pre_ref, both_ref, piece_ref, sems):
    tp = lax.axis_index("tp")
    gain = gain_ref[...]
    rows_ref[0:TAIL, :] = normalized(one_ref[...] + two_ref[...], gain)
    mine = pl.multiple_of(TAIL + tp * HALF, 16)
    rows_ref[pl.ds(mine, HALF), :] = own_ref[...]
    for part in range(HALF // 48):
        to = pl.multiple_of(TAIL + (1 - tp) * HALF + part * 48, 16)
        rows_ref[pl.ds(to, 48), :] = normalized(oth_ref[part * 48 : part * 48 + 48, :], gain)
    own = pl.ds(TAIL, ROWS)
    theirs = pl.multiple_of((1 - tp) * HALF, 8)
    both_ref[pl.ds(pl.multiple_of(tp * HALF, 8), HALF), :] = gates_ref[...]
    both_ref[pl.ds(theirs, HALF), :] = jnp.dot(
        rows_ref[pl.ds(pl.multiple_of(TAIL + (1 - tp) * HALF, 16), HALF), :], wg_ref[...], preferred_element_type=F32
    )
    gates = both_ref[...]
    gates = jnp.where(tp == 0, gates, pltpu.roll(gates, 128 - HEADS, 1))
    pre_ref[...] = jnp.dot(rows_ref[...], wk_ref[...], preferred_element_type=F32).astype(BF).astype(F32)

    lane = lane_of((SPAN, 128))
    tri = (lax.broadcasted_iota(jnp.int32, (SPAN, SPAN), 0) >= lax.broadcasted_iota(jnp.int32, (SPAN, SPAN), 1)).astype(F32)
    gate, inside, totals = [], [], []
    for b in range(BLOCKS):
        offs = jnp.zeros((1, 128), F32)
        for h in range(HEADS):
            for row, at in ((0, h), (1, 2 * HEADS + h)):
                offs = jnp.where(lane_of((1, 128)) == at, offs_ref[b, row : row + 1, h : h + 1], offs)
        g = gates[b * SPAN : (b + 1) * SPAN] + offs
        soft = jnp.minimum(g, 0.0) - jnp.log1p(jnp.exp(-jnp.abs(g)))
        total = jnp.dot(tri, soft, precision=HIGHEST, preferred_element_type=F32)
        logs_ref[b * SPAN : (b + 1) * SPAN, :] = jnp.where(lane < HEADS, g, pltpu.roll(total, 128 - HEADS, 1))
        total = pltpu.roll(total, 128 - 2 * HEADS, 1)
        gate.append(g)
        inside.append(total)
        totals.append(total[SPAN - 1 : SPAN, :])
    write, level = [], None
    later = jnp.zeros_like(totals[0])
    for b in reversed(range(BLOCKS)):
        w = (totals[b] - inside[b]) + later + gate[b]
        later = later + totals[b]
        write.insert(0, w)
        top = jnp.max(w, axis=0, keepdims=True)
        level = top if level is None else jnp.maximum(level, top)
    weight = [jnp.exp(w - level) for w in write]
    numbers = thirds(later) + thirds(level)

    taps = taps_ref[:, pl.ds(pl.multiple_of(tp * (HEADS * DQK), 128), HEADS * DQK)].astype(F32)
    for h in range(HEADS):
        lanes = slice(h * DQK, (h + 1) * DQK)
        for b in range(BLOCKS):
            rows = slice(b * SPAN, (b + 1) * SPAN)
            key_ref[rows, lanes] = (mixed_rows(pre_ref, taps, lanes, b * SPAN, SPAN) * DQK**-0.5).astype(BF)
    value_ref[...] = jnp.dot(rows_ref[own, :], wv_ref[...], preferred_element_type=F32).astype(BF)
    ones = jnp.ones((ROWS, 128), BF)
    copies = []
    dims = (((0,), (0,)), ((), ()))
    for h in range(HEADS):
        lanes = slice(h * DQK, (h + 1) * DQK)
        weighted = jnp.concatenate(
            [
                (key_ref[b * SPAN : (b + 1) * SPAN, lanes].astype(F32) * weight[b][:, h : h + 1]).astype(BF)
                for b in range(BLOCKS)
            ],
            axis=0,
        )
        memory = lax.dot_general(weighted, value_ref[:, h * DV : (h + 1) * DV], dims, preferred_element_type=F32)
        extra = lax.dot_general(weighted, ones, dims, preferred_element_type=F32)
        for n, number in enumerate(numbers):
            extra = jnp.where(lane == n + 1, number[:, h : h + 1], extra)
        out = slice(h * DQK, (h + 1) * DQK)
        piece_ref[out, :DV] = memory.astype(BF)
        piece_ref[out, DV:] = extra.astype(BF)
        copy = pltpu.make_async_copy(piece_ref.at[pl.ds(h * DQK, DQK)], piece_out.at[pl.ds(h * DQK, DQK)], sems.at[h])
        copy.start()
        copies.append(copy)
    wait_all(copies)


def prefix_kernel(piece_ref, place_ref, out_hbm, out_ref, sems):
    count = piece_ref.shape[0] // 8
    tall = piece_ref.shape[0]

    def iota(shape, dim):
        return lax.broadcasted_iota(jnp.int32, shape, dim)

    def ones_where(test):
        return jnp.where(test, 1.0, 0.0).astype(BF)

    first = ones_where(iota((count, tall), 1) == 8 * iota((count, tall), 0))
    down = iota((tall, count), 0) - 8 * iota((tall, count), 1)
    spread = ones_where((down >= 0) & (down < 8))
    over = iota((count, tall), 1) - 8 * iota((count, tall), 0)
    spread_over = ones_where((over >= 0) & (over < 8))
    extra = jnp.dot(first, piece_ref[:, DV:], preferred_element_type=F32)
    lane = lane_of((count, 128))

    def number(at):
        return jnp.sum(jnp.where((lane >= at) & (lane < at + 3), extra, 0.0), axis=1, keepdims=True)

    forget, level = number(1), number(4)
    down, over = place_ref[0], place_ref[1]
    steps = jnp.where(down > over, forget, jnp.where(down == over, level, 0.0))
    earlier = over < down
    logs = jnp.dot(jnp.where(earlier, 1.0, 0.0), steps, precision=HIGHEST, preferred_element_type=F32)
    logs = jnp.where(earlier, logs, EMPTY)
    top = jnp.max(logs, axis=1, keepdims=True)
    weight = jnp.where(earlier, jnp.exp(logs - top), 0.0).astype(BF)
    weight = jnp.dot(weight, spread_over, preferred_element_type=F32).astype(BF)
    weight = jnp.dot(spread, weight, preferred_element_type=F32)
    same = (iota((tall, tall), 0) & 7) == (iota((tall, tall), 1) & 7)
    weight = jnp.where(same, weight, 0.0).astype(BF)
    marks = jnp.zeros((count, 128), F32)
    for n, mark in enumerate(thirds(top)):
        marks = jnp.where(lane == n + 1, mark, marks)
    marks = jnp.dot(spread, marks.astype(BF), preferred_element_type=F32)
    part = tall // 4
    lane = lane_of((part, 128))
    copies = []
    for c in range(4):
        rows = slice(c * part, (c + 1) * part)
        state = jnp.dot(weight[rows], piece_ref[...], preferred_element_type=F32)
        out_ref[rows, :DV] = state[:, :DV].astype(BF)
        out_ref[rows, DV:] = jnp.where((lane >= 1) & (lane < 4), marks[rows], state[:, DV:]).astype(BF)
        copy = pltpu.make_async_copy(out_ref.at[pl.ds(c * part, part)], out_hbm.at[pl.ds(c * part, part)], sems.at[c])
        copy.start()
        copies.append(copy)
    wait_all(copies)


def local_kernel(rows_ref, wq_hbm, key_ref, value_ref, logs_ref, taps_ref,
                 query_out, numer_out, stats_ref, query_ref, numer_ref, wq_ref, pre_ref, sems):
    copies = started(by_rows(wq_hbm, wq_ref, 4), sems)
    tp = lax.axis_index("tp")
    taps = taps_ref[:, pl.ds(pl.multiple_of(tp * (HEADS * DQK), 128), HEADS * DQK)].astype(F32)
    wait_all(copies)
    pre_ref[...] = jnp.dot(rows_ref[...], wq_ref[...], preferred_element_type=F32).astype(BF).astype(F32)
    for h in range(HEADS):
        lanes = slice(h * DQK, (h + 1) * DQK)
        for b in range(BLOCKS):
            rows = slice(b * SPAN, (b + 1) * SPAN)
            query_ref[rows, lanes] = mixed_rows(pre_ref, taps, lanes, b * SPAN, SPAN).astype(BF)
    lane = lane_of((SPAN, 128))
    cols = [logs_ref[b * SPAN : (b + 1) * SPAN, :] for b in range(BLOCKS)]
    flat = [c.T for c in cols]
    ends = [c[SPAN - 1 : SPAN, :] for c in cols]
    causal = lax.broadcasted_iota(jnp.int32, (SPAN, SPAN), 0) >= lax.broadcasted_iota(jnp.int32, (SPAN, SPAN), 1)
    stats = []
    before = jnp.zeros_like(ends[0])
    for b in range(BLOCKS):
        carried = pltpu.roll(cols[b] + before, HEADS, 1)
        before = before + ends[b]
        stats.append(jnp.where((lane >= 2 * HEADS) & (lane < 3 * HEADS), carried, 0.0))
    nt = (((1,), (1,)), ((), ()))
    for h in range(HEADS):
        head = slice(h * DQK, (h + 1) * DQK)
        wide = slice(h * DV, (h + 1) * DV)
        for t in range(BLOCKS):
            rows = slice(t * SPAN, (t + 1) * SPAN)
            seen = (t + 1) * SPAN
            now = cols[t][:, HEADS + h : HEADS + h + 1]
            logs = []
            for s in range(t + 1):
                gate = flat[s][h : h + 1, :]
                past = flat[s][HEADS + h : HEADS + h + 1, :]
                if s == t:
                    logs.append(jnp.where(causal, (now - past) + gate, EMPTY))
                else:
                    rest = ends[s][:, HEADS + h : HEADS + h + 1] - past
                    for c in range(s + 1, t):
                        rest = rest + ends[c][:, HEADS + h : HEADS + h + 1]
                    logs.append(now + (rest + gate))
            top = None
            for x in logs:
                peak = jnp.max(x, axis=1, keepdims=True)
                top = peak if top is None else jnp.maximum(top, peak)
            weight = jnp.concatenate([jnp.exp(x - top) for x in logs], axis=1)
            scores = (
                lax.dot_general(query_ref[rows, head], key_ref[:seen, head], nt, preferred_element_type=F32) * weight
            )
            denom = jnp.sum(scores, axis=1, keepdims=True)
            numer = jnp.dot(scores.astype(BF), value_ref[:seen, wide], preferred_element_type=F32)
            numer_ref[rows, wide] = numer.astype(BF)
            stats[t] = jnp.where(lane == h, denom, jnp.where(lane == HEADS + h, top, stats[t]))
    for t in range(BLOCKS):
        stats_ref[t * SPAN : (t + 1) * SPAN, :] = stats[t]
    query_out[...] = query_ref[...]
    numer_out[...] = numer_ref[...]


def gate_kernel(rows_ref, wo_hbm, gain_ref, wide_out, wo_ref, ogate_ref, sems):
    wide = HEADS * DV // 2
    pairs = []
    for c in range(2):
        cols = pl.ds(c * wide, wide)
        pairs += by_rows(wo_hbm.at[:, cols], wo_ref.at[:, cols], 4)
    copies = started(pairs, sems)
    tp = lax.axis_index("tp")
    gain = gain_ref[:, pl.ds(pl.multiple_of(tp * (HEADS * DV), 128), HEADS * DV)]
    for c in range(2):
        wait_all(copies[4 * c : 4 * c + 4])
        cols = slice(c * wide, (c + 1) * wide)
        pre = jnp.dot(rows_ref[pl.ds(TAIL, ROWS), :], wo_ref[:, cols], preferred_element_type=F32).astype(BF).astype(F32)
        ogate_ref[:, cols] = (gain[:, cols] / (1.0 + jnp.exp(-pre))).astype(BF)
    wide_out[0:ROWS, : HEADS * DV] = ogate_ref[...]


def hidden_rows(first, query_ref, wide_ref, state_ref, numer_ref, stats_ref, hidden_ref):
    rows = pl.ds(pl.multiple_of(first, 16), HALF)
    lane = lane_of((HALF, 128))
    stats = stats_ref[rows, :]
    place = lane_of((DQK, 128))
    norms, level = [], jnp.zeros((1, 128), F32)
    for h in range(HEADS):
        extra = state_ref[h * DQK : (h + 1) * DQK, DV:].astype(F32)
        norms.append(jnp.where(place == h, extra[:, 0:1], 0.0).astype(BF))
        mark = extra[0:1, 1:2] + extra[0:1, 2:3] + extra[0:1, 3:4]
        level = jnp.where(lane_of((1, 128)) == h, mark, level)
    norms = jnp.concatenate(norms, axis=0)
    query = query_ref[rows, :]
    read_norm = jnp.dot(query, norms, preferred_element_type=F32)
    top = pltpu.roll(stats, 128 - HEADS, 1)
    carried = pltpu.roll(stats, 128 - 2 * HEADS, 1) + level
    peak = jnp.maximum(carried, top)
    one = jnp.exp(carried - peak)
    two = jnp.exp(top - peak)
    denom = one * read_norm + two * stats
    denom = jnp.maximum(jnp.abs(denom), jnp.exp(-peak))
    one = one / denom
    two = two / denom
    for h in range(HEADS):
        wide = slice(h * DV, (h + 1) * DV)
        read = jnp.dot(
            query[:, h * DQK : (h + 1) * DQK], state_ref[h * DQK : (h + 1) * DQK, :DV], preferred_element_type=F32
        )
        cell = one[:, h : h + 1] * read + two[:, h : h + 1] * numer_ref[rows, wide].astype(F32)
        scale = lax.rsqrt(jnp.mean(cell * cell, axis=-1, keepdims=True) + EPS)
        hidden_ref[:, wide] = (cell * scale * wide_ref[rows, wide].astype(F32)).astype(BF)


def sent_kernel(query_ref, wide_ref, state_ref, numer_ref, stats_ref, wout_hbm, out_ref, wout_ref, hidden_ref, sems):
    deep = HEADS * DV // 2
    copies = started(by_rows(wout_hbm, wout_ref, 8), sems)
    first = (1 - lax.axis_index("tp")) * HALF
    hidden_rows(first, query_ref, wide_ref, state_ref, numer_ref, stats_ref, hidden_ref)
    wait_all(copies[:4])
    part = jnp.dot(hidden_ref[:, :deep], wout_ref[:deep, :], preferred_element_type=F32)
    wait_all(copies[4:])
    out_ref[...] = (part + jnp.dot(hidden_ref[:, deep:], wout_ref[deep:, :], preferred_element_type=F32)).astype(BF)


def kept_kernel(query_ref, wide_ref, state_ref, numer_ref, stats_ref, wout_ref, out_ref, hidden_ref):
    first = lax.axis_index("tp") * HALF
    hidden_rows(first, query_ref, wide_ref, state_ref, numer_ref, stats_ref, hidden_ref)
    out_ref[...] = jnp.dot(hidden_ref[...], wout_ref[...], preferred_element_type=F32)


def far_first(stretches):
    at = np.arange(stretches)
    hops = sum(np.minimum(c, 4 - c) for c in (at // 16, at // 4 % 4, at % 4))
    return np.lexsort((at, -hops))


def body(
    tokens, norm_gain, w_query, w_key, w_value, w_ogate, w_igate, w_fgate, conv_query, conv_key, gate_offset, head_gain, w_out
):
    width = tokens.shape[1]
    stretches = lax.axis_size(SP)
    shape = jax.ShapeDtypeStruct
    other = lax.ppermute(tokens, "tp", [(0, 1), (1, 0)])
    last = call(
        last_kernel,
        jax.ShapeDtypeStruct((TAIL, width), BF),
        None,
        [pltpu.HBM],
        [pltpu.SemaphoreType.DMA((1,))],
        flops=100_000_000_000,
    )(tokens)
    to_second = lax.ppermute(last, SP_TP, [(2 * i + 1, 2 * i + 3) for i in range(stretches - 1)])
    to_first = lax.ppermute(last, SP_TP, [(2 * i + 1, 2 * i + 2) for i in range(stretches - 1)])
    gain = norm_gain.reshape(1, -1)
    head_gain = head_gain.reshape(1, -1)
    order = far_first(stretches)
    groups = [[2 * int(i) + t for i in order] for t in range(2)]
    place = np.stack([np.broadcast_to(order[:, None], (stretches, stretches)), np.broadcast_to(order, (stretches, stretches))])
    place = jnp.asarray(place.astype(np.int32))
    v, m, n = pltpu.VMEM, pltpu.HBM, None
    dma = pltpu.SemaphoreType.DMA
    key_shape, value_shape = shape((ROWS, HEADS * DQK), BF), shape((ROWS, HEADS * DV), BF)
    logs_shape = shape((ROWS, 128), F32)
    rows_shape, pre_shape = shape((TAIL + ROWS, width), BF), shape((TAIL + ROWS, HEADS * DQK), F32)

    def room(like):
        return pltpu.VMEM(like.shape, like.dtype)

    gates_shape = shape((width, 128), BF), shape((HALF, 128), F32)
    own, wg, gates = call(
        fetch_kernel,
        (shape(tokens.shape, BF), *gates_shape),
        (v, v, v),
        [m, m, m, m],
        [room(tokens), room(gain), *[pltpu.VMEM((w_igate.shape[1], width), BF)] * 2, pltpu.VMEM((128, width), F32), dma((4,))],
        flops=1000000000,
    )(tokens, gain, w_igate.T, w_fgate.T)
    key, value, logs, pieces, rows = call(
        summary_kernel,
        (key_shape, value_shape, logs_shape, shape((HEADS * DQK, WIDTH), BF), rows_shape),
        (v, v, v, m, v),
        [v, n, n, n, n, n, n, v, v, n, n],
        [room(pre_shape), room(logs_shape), pltpu.VMEM((HEADS * DQK, WIDTH), BF), dma((HEADS,))],
        flops=3_000_000_000,
    )(own, other, to_first, to_second, gain, w_key, w_value, wg, gates, conv_key, gate_offset.transpose(1, 0, 2))
    pieces = lax.all_to_all(pieces.reshape(stretches, 8, WIDTH), SP_TP, 0, 0, axis_index_groups=groups, tiled=True)
    query, numer, stats = call(
        local_kernel,
        (key_shape, value_shape, logs_shape),
        (v, v, v),
        [v, m, v, v, v, n],
        [room(key_shape), room(value_shape), room(w_query), room(pre_shape), dma((4,))],
        flops=4_000_000_000,
        limit=10,
        aliases={2: 0, 3: 1, 4: 2},
    )(rows, w_query, key, value, logs, conv_query)
    pieces, query, numer, stats = lax.optimization_barrier((pieces, query, numer, stats))
    piece_shape = shape((stretches * 8, WIDTH), BF)
    state = call(prefix_kernel, piece_shape, m, [n, n], [room(piece_shape), dma((4,))], flops=100_000_000)(pieces.reshape(piece_shape.shape), place)
    state, rows = lax.optimization_barrier((state, rows))
    state = lax.all_to_all(state.reshape(stretches, 8, WIDTH), SP_TP, 0, 0, axis_index_groups=groups, tiled=True)
    state = state.reshape(HEADS * DQK, WIDTH)
    wide = call(
        gate_kernel,
        rows_shape,
        v,
        [v, m, n],
        [room(w_ogate), room(value_shape), dma((8,))],
        flops=4_000_000_000,
        limit=10,
        aliases={0: 0},
    )(rows, w_ogate, head_gain)
    hidden = pltpu.VMEM((HALF, HEADS * DV), BF)
    sent, wout = call(
        sent_kernel,
        (shape((HALF, width), BF), shape(w_out.shape, BF)),
        (n, v),
        [v, v, n, v, v, m],
        [hidden, dma((8,))],
        flops=1_000_000_000,
    )(query, wide, state, numer, stats, w_out)
    got = lax.ppermute(sent, "tp", [(0, 1), (1, 0)])
    kept = call(kept_kernel, shape((HALF, width), F32), n, [v, v, n, v, v, v], [hidden], flops=1_000_000_000)(
        query, wide, state, numer, stats, wout
    )
    return (kept + got.astype(F32)).astype(BF)


def solution(mesh):
    split = Mesh(mesh.devices.reshape(4, 4, 4, mesh.shape["tp"]), ("sp_0", "sp_1", "sp_2", "tp"))
    placed = (
        P(SP_TP, None),
        P(),
        P(None, "tp"),
        P(None, "tp"),
        P(None, "tp"),
        P(None, "tp"),
        P(),
        P(),
        P(),
        P(),
        P(None, SP, "tp"),
        P(),
        P("tp", None),
    )
    return jax.shard_map(body, mesh=split, in_specs=placed, out_specs=P(SP_TP, None), check_vma=False)
```

```python
import jax
import jax.numpy as jnp
import numpy as np
from jax import lax
from jax.experimental import pallas as pl
from jax.experimental.pallas import tpu as pltpu
from jax.sharding import Mesh
from jax.sharding import PartitionSpec as P


SPAN = 128
SP = ("sp_0", "sp_1", "sp_2")
SP_TP = ("sp_0", "sp_1", "sp_2", "tp")
EPS = 1e-06
EMPTY = -1e30
TAIL = 16
HEADS = 4
DQK = 128
DV = 256
WIDTH = DV + 128
BLOCKS = 3
ROWS = BLOCKS * SPAN
HALF = ROWS // 2
HIGHEST = lax.Precision.HIGHEST
BF = jnp.bfloat16
F32 = jnp.float32
MIB = 1 << 20


def call(kernel, outs, out_spaces, spaces, scratch=(), flops=0, limit=8, aliases=None):
    def spec(space):
        return pl.BlockSpec(memory_space=pltpu.VMEM if space is None else space)

    def placed(like, space):
        return like if space is None else space(like.shape, like.dtype)

    several = isinstance(outs, tuple)
    run = pl.pallas_call(
        kernel,
        out_shape=tuple(map(placed, outs, out_spaces)) if several else placed(outs, out_spaces),
        in_specs=[spec(space) for space in spaces],
        out_specs=tuple(map(spec, out_spaces)) if several else spec(out_spaces),
        scratch_shapes=list(scratch),
        input_output_aliases=aliases or {},
        cost_estimate=pl.CostEstimate(flops=flops, transcendentals=0, bytes_accessed=1 << 20),
        compiler_params=pltpu.CompilerParams(vmem_limit_bytes=limit * MIB),
    )

    def kept(x, space):
        return x if space is None else pltpu.with_memory_space_constraint(x, space)

    return lambda *args: run(*map(kept, args, spaces))


def started(pairs, sems):
    copies = [pltpu.make_async_copy(src, dst, sems.at[n]) for n, (src, dst) in enumerate(pairs)]
    for copy in copies:
        copy.start()
    return copies


def by_rows(src, dst, parts):
    rows = src.shape[0] // parts
    return [(src.at[pl.ds(c * rows, rows)], dst.at[pl.ds(c * rows, rows)]) for c in range(parts)]


def wait_all(copies):
    for copy in copies:
        copy.wait()


def thirds(x):
    hi = x.astype(BF).astype(F32)
    rest = x - hi
    mid = rest.astype(BF).astype(F32)
    return hi, mid, (rest - mid).astype(BF).astype(F32)


def lane_of(shape):
    return lax.broadcasted_iota(jnp.int32, shape, len(shape) - 1)


def mixed_rows(pre_ref, taps, lanes, first, rows):
    acc = None
    for j in range(4):
        term = taps[j : j + 1, lanes] * pre_ref[pl.ds(first + TAIL - 3 + j, rows), lanes]
        acc = term if acc is None else acc + term
    return acc * (1.0 / (1.0 + jnp.exp(-acc)))


def row_scale(x):
    return lax.rsqrt(jnp.mean(x * x, axis=-1, keepdims=True) + EPS)


def normalized(x, gain):
    x = x.astype(F32)
    return (x * row_scale(x) * gain).astype(BF)


def fetch_kernel(own_hbm, gain_hbm, wi_hbm, wf_hbm,
                 rows_ref, wg_ref, gates_ref, own_ref, gain_ref, wi_ref, wf_ref, flat_ref, sems):
    copies = started([(own_hbm, own_ref), (gain_hbm, gain_ref), (wi_hbm, wi_ref), (wf_hbm, wf_ref)], sems)
    copies[0].wait()
    parts = [slice(at, at + 48) for at in range(0, HALF, 48)]
    scales = [row_scale(own_ref[part, :].astype(F32)) for part in parts]
    copies[1].wait()
    gain = gain_ref[...]
    for part, scale in zip(parts, scales):
        rows_ref[part, :] = (own_ref[part, :].astype(F32) * scale * gain).astype(BF)
    wait_all(copies[2:4])
    all_heads = wi_ref.shape[0]
    flat_ref[...] = jnp.zeros_like(flat_ref)
    flat_ref[0:all_heads, :] = wi_ref[...].astype(F32)
    flat_ref[all_heads : 2 * all_heads, :] = wf_ref[...].astype(F32)
    for at in range(0, wg_ref.shape[0], 128):
        wg_ref[at : at + 128, :] = flat_ref[:, at : at + 128].T.astype(BF)
    gates_ref[...] = jnp.dot(rows_ref[...], wg_ref[...], preferred_element_type=F32)


def spread_kernel(own_ref, oth_ref, gain_ref, rows_ref, tail_ref):
    tp = lax.axis_index("tp")
    gain = gain_ref[...]
    rows_ref[0:TAIL, :] = jnp.zeros((TAIL, rows_ref.shape[1]), BF)
    rows_ref[pl.ds(pl.multiple_of(TAIL + tp * HALF, 16), HALF), :] = own_ref[...]
    for part in range(HALF // 48):
        to = pl.multiple_of(TAIL + (1 - tp) * HALF + part * 48, 16)
        rows_ref[pl.ds(to, 48), :] = normalized(oth_ref[part * 48 : part * 48 + 48, :], gain)
    tail_ref[...] = rows_ref[ROWS : ROWS + TAIL, :]


def project_kernel(rows_ref, wk_ref, wv_ref, wg_ref, gates_ref, pre_ref, value_ref, both_ref):
    tp = lax.axis_index("tp")
    own = pl.ds(TAIL, ROWS)
    both_ref[pl.ds(pl.multiple_of(tp * HALF, 8), HALF), :] = gates_ref[...]
    both_ref[pl.ds(pl.multiple_of((1 - tp) * HALF, 8), HALF), :] = jnp.dot(
        rows_ref[pl.ds(pl.multiple_of(TAIL + (1 - tp) * HALF, 16), HALF), :], wg_ref[...], preferred_element_type=F32
    )
    pre_ref[...] = jnp.dot(rows_ref[own, :], wk_ref[...], preferred_element_type=F32).astype(BF).astype(F32)
    value_ref[...] = jnp.dot(rows_ref[own, :], wv_ref[...], preferred_element_type=F32).astype(BF)


def summary_kernel(rows_ref, tail_ref, wk_ref, own_pre_ref, value_ref, both_ref, taps_ref, offs_ref,
                   rows_out, key_ref, logs_ref, piece_out, pre_ref, piece_ref, sems):
    tp = lax.axis_index("tp")
    rows_out[0:TAIL, :] = tail_ref[...]
    pre_ref[0:TAIL, :] = jnp.dot(tail_ref[...], wk_ref[...], preferred_element_type=F32).astype(BF).astype(F32)
    pre_ref[TAIL : TAIL + ROWS, :] = own_pre_ref[...]
    gates = both_ref[...]
    gates = jnp.where(tp == 0, gates, pltpu.roll(gates, 128 - HEADS, 1))
    lane = lane_of((SPAN, 128))
    tri = (lax.broadcasted_iota(jnp.int32, (SPAN, SPAN), 0) >= lax.broadcasted_iota(jnp.int32, (SPAN, SPAN), 1)).astype(F32)
    gate, inside, totals = [], [], []
    for b in range(BLOCKS):
        offs = jnp.zeros((1, 128), F32)
        for h in range(HEADS):
            for row, at in ((0, h), (1, 2 * HEADS + h)):
                offs = jnp.where(lane_of((1, 128)) == at, offs_ref[b, row : row + 1, h : h + 1], offs)
        g = gates[b * SPAN : (b + 1) * SPAN] + offs
        soft = jnp.minimum(g, 0.0) - jnp.log1p(jnp.exp(-jnp.abs(g)))
        total = jnp.dot(tri, soft, precision=HIGHEST, preferred_element_type=F32)
        logs_ref[b * SPAN : (b + 1) * SPAN, :] = jnp.where(lane < HEADS, g, pltpu.roll(total, 128 - HEADS, 1))
        total = pltpu.roll(total, 128 - 2 * HEADS, 1)
        gate.append(g)
        inside.append(total)
        totals.append(total[SPAN - 1 : SPAN, :])
    write, level = [], None
    later = jnp.zeros_like(totals[0])
    for b in reversed(range(BLOCKS)):
        w = (totals[b] - inside[b]) + later + gate[b]
        later = later + totals[b]
        write.insert(0, w)
        top = jnp.max(w, axis=0, keepdims=True)
        level = top if level is None else jnp.maximum(level, top)
    weight = [jnp.exp(w - level) for w in write]
    numbers = thirds(later) + thirds(level)

    taps = taps_ref[:, pl.ds(pl.multiple_of(tp * (HEADS * DQK), 128), HEADS * DQK)].astype(F32)
    for h in range(HEADS):
        lanes = slice(h * DQK, (h + 1) * DQK)
        for b in range(BLOCKS):
            rows = slice(b * SPAN, (b + 1) * SPAN)
            key_ref[rows, lanes] = (mixed_rows(pre_ref, taps, lanes, b * SPAN, SPAN) * DQK**-0.5).astype(BF)
    ones = jnp.ones((ROWS, 128), BF)
    copies = []
    dims = (((0,), (0,)), ((), ()))
    for h in range(HEADS):
        lanes = slice(h * DQK, (h + 1) * DQK)
        weighted = jnp.concatenate(
            [
                (key_ref[b * SPAN : (b + 1) * SPAN, lanes].astype(F32) * weight[b][:, h : h + 1]).astype(BF)
                for b in range(BLOCKS)
            ],
            axis=0,
        )
        memory = lax.dot_general(weighted, value_ref[:, h * DV : (h + 1) * DV], dims, preferred_element_type=F32)
        extra = lax.dot_general(weighted, ones, dims, preferred_element_type=F32)
        for n, number in enumerate(numbers):
            extra = jnp.where(lane == n + 1, number[:, h : h + 1], extra)
        out = slice(h * DQK, (h + 1) * DQK)
        piece_ref[out, :DV] = memory.astype(BF)
        piece_ref[out, DV:] = extra.astype(BF)
        copy = pltpu.make_async_copy(piece_ref.at[pl.ds(h * DQK, DQK)], piece_out.at[pl.ds(h * DQK, DQK)], sems.at[h])
        copy.start()
        copies.append(copy)
    wait_all(copies)


def prefix_kernel(piece_ref, place_ref, wout_hbm, out_ref, wout_ref, sems):
    copies = started(by_rows(wout_hbm.at[pl.ds(0, wout_ref.shape[0])], wout_ref, 4), sems)
    count = piece_ref.shape[0] // 8
    tall = piece_ref.shape[0]

    def iota(shape, dim):
        return lax.broadcasted_iota(jnp.int32, shape, dim)

    def ones_where(test):
        return jnp.where(test, 1.0, 0.0).astype(BF)

    first = ones_where(iota((count, tall), 1) == 8 * iota((count, tall), 0))
    down = iota((tall, count), 0) - 8 * iota((tall, count), 1)
    spread = ones_where((down >= 0) & (down < 8))
    over = iota((count, tall), 1) - 8 * iota((count, tall), 0)
    spread_over = ones_where((over >= 0) & (over < 8))
    extra = jnp.dot(first, piece_ref[:, DV:], preferred_element_type=F32)
    lane = lane_of((count, 128))

    def number(at):
        return jnp.sum(jnp.where((lane >= at) & (lane < at + 3), extra, 0.0), axis=1, keepdims=True)

    forget, level = number(1), number(4)
    down, over = place_ref[0], place_ref[1]
    steps = jnp.where(down > over, forget, jnp.where(down == over, level, 0.0))
    earlier = over < down
    logs = jnp.dot(jnp.where(earlier, 1.0, 0.0), steps, precision=HIGHEST, preferred_element_type=F32)
    logs = jnp.where(earlier, logs, EMPTY)
    top = jnp.max(logs, axis=1, keepdims=True)
    weight = jnp.where(earlier, jnp.exp(logs - top), 0.0).astype(BF)
    weight = jnp.dot(weight, spread_over, preferred_element_type=F32).astype(BF)
    weight = jnp.dot(spread, weight, preferred_element_type=F32)
    same = (iota((tall, tall), 0) & 7) == (iota((tall, tall), 1) & 7)
    weight = jnp.where(same, weight, 0.0).astype(BF)
    marks = jnp.zeros((count, 128), F32)
    for n, mark in enumerate(thirds(top)):
        marks = jnp.where(lane == n + 1, mark, marks)
    marks = jnp.dot(spread, marks.astype(BF), preferred_element_type=F32)
    state = jnp.dot(weight, piece_ref[...], preferred_element_type=F32)
    lane = lane_of((tall, 128))
    out_ref[:, :DV] = state[:, :DV].astype(BF)
    out_ref[:, DV:] = jnp.where((lane >= 1) & (lane < 4), marks, state[:, DV:]).astype(BF)
    wait_all(copies)


def local_kernel(rows_ref, wq_hbm, key_ref, value_ref, logs_ref, wo_hbm, taps_ref, gain_ref,
                 query_out, wide_out, stats_ref, query_ref, numer_ref, ogate_ref, wq_ref, pre_ref, wo_ref, sems):
    copies = started(by_rows(wq_hbm, wq_ref, 4) + by_rows(wo_hbm, wo_ref, 8), sems)
    tp = lax.axis_index("tp")
    taps = taps_ref[:, pl.ds(pl.multiple_of(tp * (HEADS * DQK), 128), HEADS * DQK)].astype(F32)
    wait_all(copies[:4])
    pre_ref[...] = jnp.dot(rows_ref[...], wq_ref[...], preferred_element_type=F32).astype(BF).astype(F32)
    for h in range(HEADS):
        lanes = slice(h * DQK, (h + 1) * DQK)
        for b in range(BLOCKS):
            rows = slice(b * SPAN, (b + 1) * SPAN)
            query_ref[rows, lanes] = mixed_rows(pre_ref, taps, lanes, b * SPAN, SPAN).astype(BF)
    lane = lane_of((SPAN, 128))
    cols = [logs_ref[b * SPAN : (b + 1) * SPAN, :] for b in range(BLOCKS)]
    flat = [c.T for c in cols]
    ends = [c[SPAN - 1 : SPAN, :] for c in cols]
    causal = lax.broadcasted_iota(jnp.int32, (SPAN, SPAN), 0) >= lax.broadcasted_iota(jnp.int32, (SPAN, SPAN), 1)
    stats = []
    before = jnp.zeros_like(ends[0])
    for b in range(BLOCKS):
        carried = pltpu.roll(cols[b] + before, HEADS, 1)
        before = before + ends[b]
        stats.append(jnp.where((lane >= 2 * HEADS) & (lane < 3 * HEADS), carried, 0.0))
    nt = (((1,), (1,)), ((), ()))
    for h in range(HEADS):
        head = slice(h * DQK, (h + 1) * DQK)
        wide = slice(h * DV, (h + 1) * DV)
        for t in range(BLOCKS):
            rows = slice(t * SPAN, (t + 1) * SPAN)
            seen = (t + 1) * SPAN
            now = cols[t][:, HEADS + h : HEADS + h + 1]
            logs = []
            for s in range(t + 1):
                gate = flat[s][h : h + 1, :]
                past = flat[s][HEADS + h : HEADS + h + 1, :]
                if s == t:
                    logs.append(jnp.where(causal, (now - past) + gate, EMPTY))
                else:
                    rest = ends[s][:, HEADS + h : HEADS + h + 1] - past
                    for c in range(s + 1, t):
                        rest = rest + ends[c][:, HEADS + h : HEADS + h + 1]
                    logs.append(now + (rest + gate))
            top = None
            for x in logs:
                peak = jnp.max(x, axis=1, keepdims=True)
                top = peak if top is None else jnp.maximum(top, peak)
            weight = jnp.concatenate([jnp.exp(x - top) for x in logs], axis=1)
            scores = (
                lax.dot_general(query_ref[rows, head], key_ref[:seen, head], nt, preferred_element_type=F32) * weight
            )
            denom = jnp.sum(scores, axis=1, keepdims=True)
            numer = jnp.dot(scores.astype(BF), value_ref[:seen, wide], preferred_element_type=F32)
            numer_ref[rows, wide] = numer.astype(BF)
            stats[t] = jnp.where(lane == h, denom, jnp.where(lane == HEADS + h, top, stats[t]))
    for t in range(BLOCKS):
        stats_ref[t * SPAN : (t + 1) * SPAN, :] = stats[t]
    wait_all(copies[4:])
    gain = gain_ref[:, pl.ds(pl.multiple_of(tp * (HEADS * DV), 128), HEADS * DV)]
    for c in range(2):
        cols = slice(c * HEADS * DV // 2, (c + 1) * HEADS * DV // 2)
        pre = jnp.dot(rows_ref[pl.ds(TAIL, ROWS), :], wo_ref[:, cols], preferred_element_type=F32).astype(BF).astype(F32)
        ogate_ref[:, cols] = (gain[:, cols] / (1.0 + jnp.exp(-pre))).astype(BF)
    query_out[...] = query_ref[...]
    wide_out[0:ROWS, : HEADS * DV] = numer_ref[...]
    wide_out[0:ROWS, HEADS * DV :] = ogate_ref[...]


def hidden_rows(first, query_ref, wide_ref, state_ref, stats_ref, hidden_ref):
    rows = pl.ds(pl.multiple_of(first, 16), HALF)
    lane = lane_of((HALF, 128))
    stats = stats_ref[rows, :]
    place = lane_of((DQK, 128))
    norms, level = [], jnp.zeros((1, 128), F32)
    for h in range(HEADS):
        extra = state_ref[h * DQK : (h + 1) * DQK, DV:].astype(F32)
        norms.append(jnp.where(place == h, extra[:, 0:1], 0.0).astype(BF))
        mark = extra[0:1, 1:2] + extra[0:1, 2:3] + extra[0:1, 3:4]
        level = jnp.where(lane_of((1, 128)) == h, mark, level)
    norms = jnp.concatenate(norms, axis=0)
    query = query_ref[rows, :]
    read_norm = jnp.dot(query, norms, preferred_element_type=F32)
    top = pltpu.roll(stats, 128 - HEADS, 1)
    carried = pltpu.roll(stats, 128 - 2 * HEADS, 1) + level
    peak = jnp.maximum(carried, top)
    one = jnp.exp(carried - peak)
    two = jnp.exp(top - peak)
    denom = one * read_norm + two * stats
    denom = jnp.maximum(jnp.abs(denom), jnp.exp(-peak))
    one = one / denom
    two = two / denom
    for h in range(HEADS):
        wide = slice(h * DV, (h + 1) * DV)
        read = jnp.dot(
            query[:, h * DQK : (h + 1) * DQK], state_ref[h * DQK : (h + 1) * DQK, :DV], preferred_element_type=F32
        )
        cell = one[:, h : h + 1] * read + two[:, h : h + 1] * wide_ref[rows, wide].astype(F32)
        scale = lax.rsqrt(jnp.mean(cell * cell, axis=-1, keepdims=True) + EPS)
        hidden_ref[:, wide] = (cell * scale * wide_ref[rows, HEADS * DV + h * DV : HEADS * DV + (h + 1) * DV].astype(F32)).astype(BF)


def sent_kernel(query_ref, wide_ref, state_ref, stats_ref, upper_ref, wout_hbm, out_ref, lower_ref, hidden_ref, sems):
    deep = upper_ref.shape[0]
    copies = started(by_rows(wout_hbm.at[pl.ds(deep, deep)], lower_ref, 4), sems)
    first = (1 - lax.axis_index("tp")) * HALF
    hidden_rows(first, query_ref, wide_ref, state_ref, stats_ref, hidden_ref)
    part = jnp.dot(hidden_ref[:, :deep], upper_ref[...], preferred_element_type=F32)
    wait_all(copies)
    out_ref[...] = (part + jnp.dot(hidden_ref[:, deep:], lower_ref[...], preferred_element_type=F32)).astype(BF)


def kept_kernel(query_ref, wide_ref, state_ref, stats_ref, upper_ref, lower_ref, out_ref, hidden_ref):
    deep = upper_ref.shape[0]
    first = lax.axis_index("tp") * HALF
    hidden_rows(first, query_ref, wide_ref, state_ref, stats_ref, hidden_ref)
    part = jnp.dot(hidden_ref[:, :deep], upper_ref[...], preferred_element_type=F32)
    out_ref[...] = part + jnp.dot(hidden_ref[:, deep:], lower_ref[...], preferred_element_type=F32)


def far_first(stretches):
    at = np.arange(stretches)
    hops = sum(np.minimum(c, 4 - c) for c in (at // 16, at // 4 % 4, at % 4))
    return np.lexsort((at, -hops))


def body(
    tokens, norm_gain, w_query, w_key, w_value, w_ogate, w_igate, w_fgate, conv_query, conv_key, gate_offset, head_gain, w_out
):
    width = tokens.shape[1]
    stretches = lax.axis_size(SP)
    shape = jax.ShapeDtypeStruct
    other = lax.ppermute(tokens, "tp", [(0, 1), (1, 0)])
    gain = norm_gain.reshape(1, -1)
    head_gain = head_gain.reshape(1, -1)
    order = far_first(stretches)
    groups = [[2 * int(i) + t for i in order] for t in range(2)]
    place = np.stack([np.broadcast_to(order[:, None], (stretches, stretches)), np.broadcast_to(order, (stretches, stretches))])
    place = jnp.asarray(place.astype(np.int32))
    v, m, n = pltpu.VMEM, pltpu.HBM, None
    dma = pltpu.SemaphoreType.DMA
    key_shape, value_shape = shape((ROWS, HEADS * DQK), BF), shape((ROWS, HEADS * DV), BF)
    logs_shape = shape((ROWS, 128), F32)
    rows_shape, pre_shape = shape((TAIL + ROWS, width), BF), shape((TAIL + ROWS, HEADS * DQK), F32)

    def room(like):
        return pltpu.VMEM(like.shape, like.dtype)

    gates_shape = shape((width, 128), BF), shape((HALF, 128), F32)
    own, wg, gates = call(
        fetch_kernel,
        (shape(tokens.shape, BF), *gates_shape),
        (v, v, v),
        [m, m, m, m],
        [room(tokens), room(gain), *[pltpu.VMEM((w_igate.shape[1], width), BF)] * 2, pltpu.VMEM((128, width), F32), dma((4,))],
        flops=100_000_000_000,
    )(tokens, gain, w_igate.T, w_fgate.T)
    rows, last = call(spread_kernel, (rows_shape, shape((TAIL, width), BF)), (v, n), [v, n, n], flops=100_000_000)(own, other, gain)
    tail = lax.ppermute(last, SP, [(i, i + 1) for i in range(stretches - 1)])
    own_pre_shape = shape((ROWS, HEADS * DQK), F32)
    own_pre, value, both = call(
        project_kernel,
        (own_pre_shape, value_shape, logs_shape),
        (v, v, v),
        [v, n, n, v, v],
        flops=3_000_000_000,
    )(rows, w_key, w_value, wg, gates)
    rows, key, logs, pieces = call(
        summary_kernel,
        (rows_shape, key_shape, logs_shape, shape((HEADS * DQK, WIDTH), BF)),
        (v, v, v, m),
        [v, n, n, v, v, v, n, n],
        [room(pre_shape), pltpu.VMEM((HEADS * DQK, WIDTH), BF), dma((HEADS,))],
        flops=1_000_000_000,
        aliases={0: 0},
    )(rows, tail, w_key, own_pre, value, both, conv_key, gate_offset.transpose(1, 0, 2))
    pieces = lax.all_to_all(pieces.reshape(stretches, 8, WIDTH), SP_TP, 0, 0, axis_index_groups=groups, tiled=True)
    query, wide, stats = call(
        local_kernel,
        (key_shape, rows_shape, logs_shape),
        (v, v, v),
        [v, m, v, v, v, m, n, n],
        [room(key_shape), room(value_shape), room(value_shape), room(w_query), room(pre_shape), room(w_ogate), dma((12,))],
        flops=6_000_000_000,
        limit=16,
        aliases={2: 0, 0: 1, 4: 2},
    )(rows, w_query, key, value, logs, w_ogate, conv_query, head_gain)
    pieces, query, wide, stats = lax.optimization_barrier((pieces, query, wide, stats))
    piece_shape = shape((stretches * 8, WIDTH), BF)
    half_shape = shape((w_out.shape[0] // 2, width), BF)
    state, upper = call(
        prefix_kernel, (piece_shape, half_shape), (n, v), [n, n, m], [dma((4,))], flops=100_000_000
    )(pieces.reshape(piece_shape.shape), place, w_out)
    state = lax.all_to_all(state.reshape(stretches, 8, WIDTH), SP_TP, 0, 0, axis_index_groups=groups, tiled=True)
    state = state.reshape(HEADS * DQK, WIDTH)
    hidden = pltpu.VMEM((HALF, HEADS * DV), BF)
    sent, lower = call(
        sent_kernel,
        (shape((HALF, width), BF), half_shape),
        (n, v),
        [v, v, n, v, v, m],
        [hidden, dma((4,))],
        flops=1_000_000_000,
    )(query, wide, state, stats, upper, w_out)
    got = lax.ppermute(sent, "tp", [(0, 1), (1, 0)])
    kept = call(kept_kernel, shape((HALF, width), F32), n, [v, v, n, v, v, v], [hidden], flops=1_000_000_000)(
        query, wide, state, stats, upper, lower
    )
    return (kept + got.astype(F32)).astype(BF)


def solution(mesh):
    split = Mesh(mesh.devices.reshape(4, 4, 4, mesh.shape["tp"]), ("sp_0", "sp_1", "sp_2", "tp"))
    placed = (
        P(SP_TP, None),
        P(),
        P(None, "tp"),
        P(None, "tp"),
        P(None, "tp"),
        P(None, "tp"),
        P(),
        P(),
        P(),
        P(),
        P(None, SP, "tp"),
        P(),
        P("tp", None),
    )
    return jax.shard_map(body, mesh=split, in_specs=placed, out_specs=P(SP_TP, None), check_vma=False)
```

```python
import jax
import jax.numpy as jnp
import numpy as np
from jax import lax
from jax.experimental import pallas as pl
from jax.experimental.pallas import tpu as pltpu
from jax.sharding import Mesh
from jax.sharding import PartitionSpec as P


SPAN = 128
SP = ("sp_0", "sp_1", "sp_2")
SP_TP = ("sp_0", "sp_1", "sp_2", "tp")
EPS = 1e-06
EMPTY = -1e30
TAIL = 16
HEADS = 4
DQK = 128
DV = 256
WIDTH = DV + 128
BLOCKS = 3
ROWS = BLOCKS * SPAN
HALF = ROWS // 2
HIGHEST = lax.Precision.HIGHEST
BF = jnp.bfloat16
F32 = jnp.float32
MIB = 1 << 20


def call(kernel, outs, out_spaces, spaces, scratch=(), flops=0, limit=8, aliases=None):
    def spec(space):
        return pl.BlockSpec(memory_space=pltpu.VMEM if space is None else space)

    def placed(like, space):
        return like if space is None else space(like.shape, like.dtype)

    several = isinstance(outs, tuple)
    run = pl.pallas_call(
        kernel,
        out_shape=tuple(map(placed, outs, out_spaces)) if several else placed(outs, out_spaces),
        in_specs=[spec(space) for space in spaces],
        out_specs=tuple(map(spec, out_spaces)) if several else spec(out_spaces),
        scratch_shapes=list(scratch),
        input_output_aliases=aliases or {},
        cost_estimate=pl.CostEstimate(flops=flops, transcendentals=0, bytes_accessed=1 << 20),
        compiler_params=pltpu.CompilerParams(vmem_limit_bytes=limit * MIB),
    )

    def kept(x, space):
        return x if space is None else pltpu.with_memory_space_constraint(x, space)

    return lambda *args: run(*map(kept, args, spaces))


def started(pairs, sems):
    copies = [pltpu.make_async_copy(src, dst, sems.at[n]) for n, (src, dst) in enumerate(pairs)]
    for copy in copies:
        copy.start()
    return copies


def by_rows(src, dst, parts):
    rows = src.shape[0] // parts
    return [(src.at[pl.ds(c * rows, rows)], dst.at[pl.ds(c * rows, rows)]) for c in range(parts)]


def wait_all(copies):
    for copy in copies:
        copy.wait()


def thirds(x):
    hi = x.astype(BF).astype(F32)
    rest = x - hi
    mid = rest.astype(BF).astype(F32)
    return hi, mid, (rest - mid).astype(BF).astype(F32)


def lane_of(shape):
    return lax.broadcasted_iota(jnp.int32, shape, len(shape) - 1)


def mixed_rows(pre_ref, taps, lanes, first, rows):
    acc = None
    for j in range(4):
        term = taps[j : j + 1, lanes] * pre_ref[pl.ds(first + TAIL - 3 + j, rows), lanes]
        acc = term if acc is None else acc + term
    return acc * (1.0 / (1.0 + jnp.exp(-acc)))


def row_scale(x):
    return lax.rsqrt(jnp.mean(x * x, axis=-1, keepdims=True) + EPS)


def normalized(x, gain):
    x = x.astype(F32)
    return (x * row_scale(x) * gain).astype(BF)


def fetch_kernel(own_hbm, gain_hbm, wi_hbm, wf_hbm,
                 rows_ref, wg_ref, gates_ref, own_ref, gain_ref, wi_ref, wf_ref, flat_ref, sems):
    copies = started([(own_hbm, own_ref), (gain_hbm, gain_ref), (wi_hbm, wi_ref), (wf_hbm, wf_ref)], sems)
    copies[0].wait()
    parts = [slice(at, at + 48) for at in range(0, HALF, 48)]
    scales = [row_scale(own_ref[part, :].astype(F32)) for part in parts]
    copies[1].wait()
    gain = gain_ref[...]
    for part, scale in zip(parts, scales):
        rows_ref[part, :] = (own_ref[part, :].astype(F32) * scale * gain).astype(BF)
    wait_all(copies[2:4])
    all_heads = wi_ref.shape[0]
    flat_ref[...] = jnp.zeros_like(flat_ref)
    flat_ref[0:all_heads, :] = wi_ref[...].astype(F32)
    flat_ref[all_heads : 2 * all_heads, :] = wf_ref[...].astype(F32)
    for at in range(0, wg_ref.shape[0], 128):
        wg_ref[at : at + 128, :] = flat_ref[:, at : at + 128].T.astype(BF)
    gates_ref[...] = jnp.dot(rows_ref[...], wg_ref[...], preferred_element_type=F32)


def spread_kernel(own_ref, oth_ref, gain_ref, rows_ref, tail_ref):
    tp = lax.axis_index("tp")
    gain = gain_ref[...]
    rows_ref[0:TAIL, :] = jnp.zeros((TAIL, rows_ref.shape[1]), BF)
    rows_ref[pl.ds(pl.multiple_of(TAIL + tp * HALF, 16), HALF), :] = own_ref[...]
    for part in range(HALF // 48):
        to = pl.multiple_of(TAIL + (1 - tp) * HALF + part * 48, 16)
        rows_ref[pl.ds(to, 48), :] = normalized(oth_ref[part * 48 : part * 48 + 48, :], gain)
    tail_ref[...] = rows_ref[ROWS : ROWS + TAIL, :]


def project_kernel(rows_ref, wk_ref, wv_ref, wg_ref, gates_ref, pre_ref, value_ref, both_ref):
    tp = lax.axis_index("tp")
    own = pl.ds(TAIL, ROWS)
    both_ref[pl.ds(pl.multiple_of(tp * HALF, 8), HALF), :] = gates_ref[...]
    both_ref[pl.ds(pl.multiple_of((1 - tp) * HALF, 8), HALF), :] = jnp.dot(
        rows_ref[pl.ds(pl.multiple_of(TAIL + (1 - tp) * HALF, 16), HALF), :], wg_ref[...], preferred_element_type=F32
    )
    pre_ref[...] = jnp.dot(rows_ref[own, :], wk_ref[...], preferred_element_type=F32).astype(BF).astype(F32)
    value_ref[...] = jnp.dot(rows_ref[own, :], wv_ref[...], preferred_element_type=F32).astype(BF)


def summary_kernel(rows_ref, tail_ref, wk_ref, own_pre_ref, value_ref, both_ref, taps_ref, offs_ref,
                   rows_out, key_ref, logs_ref, piece_out, pre_ref, piece_ref, sems):
    tp = lax.axis_index("tp")
    rows_out[0:TAIL, :] = tail_ref[...]
    pre_ref[0:TAIL, :] = jnp.dot(tail_ref[...], wk_ref[...], preferred_element_type=F32).astype(BF).astype(F32)
    pre_ref[TAIL : TAIL + ROWS, :] = own_pre_ref[...]
    gates = both_ref[...]
    gates = jnp.where(tp == 0, gates, pltpu.roll(gates, 128 - HEADS, 1))
    lane = lane_of((SPAN, 128))
    tri = (lax.broadcasted_iota(jnp.int32, (SPAN, SPAN), 0) >= lax.broadcasted_iota(jnp.int32, (SPAN, SPAN), 1)).astype(F32)
    gate, inside, totals = [], [], []
    for b in range(BLOCKS):
        offs = jnp.zeros((1, 128), F32)
        for h in range(HEADS):
            for row, at in ((0, h), (1, 2 * HEADS + h)):
                offs = jnp.where(lane_of((1, 128)) == at, offs_ref[b, row : row + 1, h : h + 1], offs)
        g = gates[b * SPAN : (b + 1) * SPAN] + offs
        soft = jnp.minimum(g, 0.0) - jnp.log1p(jnp.exp(-jnp.abs(g)))
        total = jnp.dot(tri, soft, precision=HIGHEST, preferred_element_type=F32)
        logs_ref[b * SPAN : (b + 1) * SPAN, :] = jnp.where(lane < HEADS, g, pltpu.roll(total, 128 - HEADS, 1))
        total = pltpu.roll(total, 128 - 2 * HEADS, 1)
        gate.append(g)
        inside.append(total)
        totals.append(total[SPAN - 1 : SPAN, :])
    write, level = [], None
    later = jnp.zeros_like(totals[0])
    for b in reversed(range(BLOCKS)):
        w = (totals[b] - inside[b]) + later + gate[b]
        later = later + totals[b]
        write.insert(0, w)
        top = jnp.max(w, axis=0, keepdims=True)
        level = top if level is None else jnp.maximum(level, top)
    weight = [jnp.exp(w - level) for w in write]
    numbers = thirds(later) + thirds(level)

    taps = taps_ref[:, pl.ds(pl.multiple_of(tp * (HEADS * DQK), 128), HEADS * DQK)].astype(F32)
    for h in range(HEADS):
        lanes = slice(h * DQK, (h + 1) * DQK)
        for b in range(BLOCKS):
            rows = slice(b * SPAN, (b + 1) * SPAN)
            key_ref[rows, lanes] = (mixed_rows(pre_ref, taps, lanes, b * SPAN, SPAN) * DQK**-0.5).astype(BF)
    ones = jnp.ones((ROWS, 128), BF)
    copies = []
    dims = (((0,), (0,)), ((), ()))
    for h in range(HEADS):
        lanes = slice(h * DQK, (h + 1) * DQK)
        weighted = jnp.concatenate(
            [
                (key_ref[b * SPAN : (b + 1) * SPAN, lanes].astype(F32) * weight[b][:, h : h + 1]).astype(BF)
                for b in range(BLOCKS)
            ],
            axis=0,
        )
        memory = lax.dot_general(weighted, value_ref[:, h * DV : (h + 1) * DV], dims, preferred_element_type=F32)
        extra = lax.dot_general(weighted, ones, dims, preferred_element_type=F32)
        for n, number in enumerate(numbers):
            extra = jnp.where(lane == n + 1, number[:, h : h + 1], extra)
        out = slice(h * DQK, (h + 1) * DQK)
        piece_ref[out, :DV] = memory.astype(BF)
        piece_ref[out, DV:] = extra.astype(BF)
        copy = pltpu.make_async_copy(piece_ref.at[pl.ds(h * DQK, DQK)], piece_out.at[pl.ds(h * DQK, DQK)], sems.at[h])
        copy.start()
        copies.append(copy)
    wait_all(copies)


def prefix_kernel(piece_ref, place_ref, out_ref):
    count = piece_ref.shape[0] // 8
    tall = piece_ref.shape[0]

    def iota(shape, dim):
        return lax.broadcasted_iota(jnp.int32, shape, dim)

    def ones_where(test):
        return jnp.where(test, 1.0, 0.0).astype(BF)

    first = ones_where(iota((count, tall), 1) == 8 * iota((count, tall), 0))
    down = iota((tall, count), 0) - 8 * iota((tall, count), 1)
    spread = ones_where((down >= 0) & (down < 8))
    over = iota((count, tall), 1) - 8 * iota((count, tall), 0)
    spread_over = ones_where((over >= 0) & (over < 8))
    extra = jnp.dot(first, piece_ref[:, DV:], preferred_element_type=F32)
    lane = lane_of((count, 128))

    def number(at):
        return jnp.sum(jnp.where((lane >= at) & (lane < at + 3), extra, 0.0), axis=1, keepdims=True)

    forget, level = number(1), number(4)
    down, over = place_ref[0], place_ref[1]
    steps = jnp.where(down > over, forget, jnp.where(down == over, level, 0.0))
    earlier = over < down
    logs = jnp.dot(jnp.where(earlier, 1.0, 0.0), steps, precision=HIGHEST, preferred_element_type=F32)
    logs = jnp.where(earlier, logs, EMPTY)
    top = jnp.max(logs, axis=1, keepdims=True)
    weight = jnp.where(earlier, jnp.exp(logs - top), 0.0).astype(BF)
    weight = jnp.dot(weight, spread_over, preferred_element_type=F32).astype(BF)
    weight = jnp.dot(spread, weight, preferred_element_type=F32)
    same = (iota((tall, tall), 0) & 7) == (iota((tall, tall), 1) & 7)
    weight = jnp.where(same, weight, 0.0).astype(BF)
    marks = jnp.zeros((count, 128), F32)
    for n, mark in enumerate(thirds(top)):
        marks = jnp.where(lane == n + 1, mark, marks)
    marks = jnp.dot(spread, marks.astype(BF), preferred_element_type=F32)
    state = jnp.dot(weight, piece_ref[...], preferred_element_type=F32)
    lane = lane_of((tall, 128))
    out_ref[:, :DV] = state[:, :DV].astype(BF)
    out_ref[:, DV:] = jnp.where((lane >= 1) & (lane < 4), marks, state[:, DV:]).astype(BF)


def local_kernel(rows_ref, wq_hbm, key_ref, value_ref, logs_ref, wo_hbm, taps_ref, gain_ref,
                 query_out, wide_out, stats_ref, query_ref, numer_ref, ogate_ref, wq_ref, pre_ref, wo_ref, weight_ref, sems):
    copies = started(by_rows(wq_hbm, wq_ref, 4) + by_rows(wo_hbm, wo_ref, 8), sems)
    tp = lax.axis_index("tp")
    taps = taps_ref[:, pl.ds(pl.multiple_of(tp * (HEADS * DQK), 128), HEADS * DQK)].astype(F32)
    lane = lane_of((SPAN, 128))
    cols = [logs_ref[b * SPAN : (b + 1) * SPAN, :] for b in range(BLOCKS)]
    flat = [c.T for c in cols]
    ends = [c[SPAN - 1 : SPAN, :] for c in cols]
    causal = lax.broadcasted_iota(jnp.int32, (SPAN, SPAN), 0) >= lax.broadcasted_iota(jnp.int32, (SPAN, SPAN), 1)
    stats = []
    before = jnp.zeros_like(ends[0])
    for b in range(BLOCKS):
        carried = pltpu.roll(cols[b] + before, HEADS, 1)
        before = before + ends[b]
        stats.append(jnp.where((lane >= 2 * HEADS) & (lane < 3 * HEADS), carried, 0.0))
    nt = (((1,), (1,)), ((), ()))
    for h in range(HEADS):
        head = slice(h * DQK, (h + 1) * DQK)
        wide = slice(h * DV, (h + 1) * DV)
        for t in range(BLOCKS):
            rows = slice(t * SPAN, (t + 1) * SPAN)
            seen = (t + 1) * SPAN
            now = cols[t][:, HEADS + h : HEADS + h + 1]
            logs = []
            for s in range(t + 1):
                gate = flat[s][h : h + 1, :]
                past = flat[s][HEADS + h : HEADS + h + 1, :]
                if s == t:
                    logs.append(jnp.where(causal, (now - past) + gate, EMPTY))
                else:
                    rest = ends[s][:, HEADS + h : HEADS + h + 1] - past
                    for c in range(s + 1, t):
                        rest = rest + ends[c][:, HEADS + h : HEADS + h + 1]
                    logs.append(now + (rest + gate))
            top = None
            for x in logs:
                peak = jnp.max(x, axis=1, keepdims=True)
                top = peak if top is None else jnp.maximum(top, peak)
            for s, x in enumerate(logs):
                weight_ref[h * ROWS + t * SPAN : h * ROWS + (t + 1) * SPAN, s * SPAN : (s + 1) * SPAN] = jnp.exp(x - top)
            stats[t] = jnp.where(lane == HEADS + h, top, stats[t])
    wait_all(copies[:4])
    pre_ref[...] = jnp.dot(rows_ref[...], wq_ref[...], preferred_element_type=F32).astype(BF).astype(F32)
    for h in range(HEADS):
        lanes = slice(h * DQK, (h + 1) * DQK)
        for b in range(BLOCKS):
            rows = slice(b * SPAN, (b + 1) * SPAN)
            query_ref[rows, lanes] = mixed_rows(pre_ref, taps, lanes, b * SPAN, SPAN).astype(BF)
    for h in range(HEADS):
        head = slice(h * DQK, (h + 1) * DQK)
        wide = slice(h * DV, (h + 1) * DV)
        for t in range(BLOCKS):
            rows = slice(t * SPAN, (t + 1) * SPAN)
            seen = (t + 1) * SPAN
            weight = weight_ref[h * ROWS + t * SPAN : h * ROWS + (t + 1) * SPAN, :seen]
            scores = (
                lax.dot_general(query_ref[rows, head], key_ref[:seen, head], nt, preferred_element_type=F32) * weight
            )
            denom = jnp.sum(scores, axis=1, keepdims=True)
            numer = jnp.dot(scores.astype(BF), value_ref[:seen, wide], preferred_element_type=F32)
            numer_ref[rows, wide] = numer.astype(BF)
            stats[t] = jnp.where(lane == h, denom, stats[t])
    for t in range(BLOCKS):
        stats_ref[t * SPAN : (t + 1) * SPAN, :] = stats[t]
    wait_all(copies[4:])
    gain = gain_ref[:, pl.ds(pl.multiple_of(tp * (HEADS * DV), 128), HEADS * DV)]
    for c in range(2):
        cols = slice(c * HEADS * DV // 2, (c + 1) * HEADS * DV // 2)
        pre = jnp.dot(rows_ref[pl.ds(TAIL, ROWS), :], wo_ref[:, cols], preferred_element_type=F32).astype(BF).astype(F32)
        ogate_ref[:, cols] = (gain[:, cols] / (1.0 + jnp.exp(-pre))).astype(BF)
    query_out[...] = query_ref[...]
    wide_out[0:ROWS, : HEADS * DV] = numer_ref[...]
    wide_out[0:ROWS, HEADS * DV :] = ogate_ref[...]


def hidden_rows(first, query_ref, wide_ref, state_ref, stats_ref, hidden_ref):
    rows = pl.ds(pl.multiple_of(first, 16), HALF)
    lane = lane_of((HALF, 128))
    stats = stats_ref[rows, :]
    place = lane_of((DQK, 128))
    norms, level = [], jnp.zeros((1, 128), F32)
    for h in range(HEADS):
        extra = state_ref[h * DQK : (h + 1) * DQK, DV:].astype(F32)
        norms.append(jnp.where(place == h, extra[:, 0:1], 0.0).astype(BF))
        mark = extra[0:1, 1:2] + extra[0:1, 2:3] + extra[0:1, 3:4]
        level = jnp.where(lane_of((1, 128)) == h, mark, level)
    norms = jnp.concatenate(norms, axis=0)
    query = query_ref[rows, :]
    read_norm = jnp.dot(query, norms, preferred_element_type=F32)
    top = pltpu.roll(stats, 128 - HEADS, 1)
    carried = pltpu.roll(stats, 128 - 2 * HEADS, 1) + level
    peak = jnp.maximum(carried, top)
    one = jnp.exp(carried - peak)
    two = jnp.exp(top - peak)
    denom = one * read_norm + two * stats
    denom = jnp.maximum(jnp.abs(denom), jnp.exp(-peak))
    one = one / denom
    two = two / denom
    for h in range(HEADS):
        wide = slice(h * DV, (h + 1) * DV)
        read = jnp.dot(
            query[:, h * DQK : (h + 1) * DQK], state_ref[h * DQK : (h + 1) * DQK, :DV], preferred_element_type=F32
        )
        cell = one[:, h : h + 1] * read + two[:, h : h + 1] * wide_ref[rows, wide].astype(F32)
        scale = lax.rsqrt(jnp.mean(cell * cell, axis=-1, keepdims=True) + EPS)
        hidden_ref[:, wide] = (cell * scale * wide_ref[rows, HEADS * DV + h * DV : HEADS * DV + (h + 1) * DV].astype(F32)).astype(BF)


def sent_kernel(query_ref, wide_ref, state_ref, stats_ref, wout_ref, out_ref, hidden_ref):
    first = (1 - lax.axis_index("tp")) * HALF
    hidden_rows(first, query_ref, wide_ref, state_ref, stats_ref, hidden_ref)
    out_ref[...] = jnp.dot(hidden_ref[...], wout_ref[...], preferred_element_type=F32).astype(BF)


def kept_kernel(query_ref, wide_ref, state_ref, stats_ref, wout_ref, out_ref, hidden_ref):
    first = lax.axis_index("tp") * HALF
    hidden_rows(first, query_ref, wide_ref, state_ref, stats_ref, hidden_ref)
    out_ref[...] = jnp.dot(hidden_ref[...], wout_ref[...], preferred_element_type=F32)


def far_first(stretches):
    at = np.arange(stretches)
    hops = sum(np.minimum(c, 4 - c) for c in (at // 16, at // 4 % 4, at % 4))
    return np.lexsort((at, -hops))


def body(
    tokens, norm_gain, w_query, w_key, w_value, w_ogate, w_igate, w_fgate, conv_query, conv_key, gate_offset, head_gain, w_out
):
    width = tokens.shape[1]
    stretches = lax.axis_size(SP)
    shape = jax.ShapeDtypeStruct
    other = lax.ppermute(tokens, "tp", [(0, 1), (1, 0)])
    gain = norm_gain.reshape(1, -1)
    head_gain = head_gain.reshape(1, -1)
    order = far_first(stretches)
    groups = [[2 * int(i) + t for i in order] for t in range(2)]
    place = np.stack([np.broadcast_to(order[:, None], (stretches, stretches)), np.broadcast_to(order, (stretches, stretches))])
    place = jnp.asarray(place.astype(np.int32))
    v, m, n = pltpu.VMEM, pltpu.HBM, None
    dma = pltpu.SemaphoreType.DMA
    key_shape, value_shape = shape((ROWS, HEADS * DQK), BF), shape((ROWS, HEADS * DV), BF)
    logs_shape = shape((ROWS, 128), F32)
    rows_shape, pre_shape = shape((TAIL + ROWS, width), BF), shape((TAIL + ROWS, HEADS * DQK), F32)

    def room(like):
        return pltpu.VMEM(like.shape, like.dtype)

    gates_shape = shape((width, 128), BF), shape((HALF, 128), F32)
    own, wg, gates = call(
        fetch_kernel,
        (shape(tokens.shape, BF), *gates_shape),
        (v, v, v),
        [m, m, m, m],
        [room(tokens), room(gain), *[pltpu.VMEM((w_igate.shape[1], width), BF)] * 2, pltpu.VMEM((128, width), F32), dma((4,))],
        flops=100_000_000_000,
    )(tokens, gain, w_igate.T, w_fgate.T)
    rows, last = call(spread_kernel, (rows_shape, shape((TAIL, width), BF)), (v, n), [v, n, n], flops=100_000_000)(own, other, gain)
    tail = lax.ppermute(last, SP, [(i, i + 1) for i in range(stretches - 1)])
    own_pre_shape = shape((ROWS, HEADS * DQK), F32)
    own_pre, value, both = call(
        project_kernel,
        (own_pre_shape, value_shape, logs_shape),
        (v, v, v),
        [v, n, n, v, v],
        flops=3_000_000_000,
    )(rows, w_key, w_value, wg, gates)
    rows, key, logs, pieces = call(
        summary_kernel,
        (rows_shape, key_shape, logs_shape, shape((HEADS * DQK, WIDTH), BF)),
        (v, v, v, m),
        [v, n, n, v, v, v, n, n],
        [room(pre_shape), pltpu.VMEM((HEADS * DQK, WIDTH), BF), dma((HEADS,))],
        flops=1_000_000_000,
        aliases={0: 0},
    )(rows, tail, w_key, own_pre, value, both, conv_key, gate_offset.transpose(1, 0, 2))
    pieces = lax.all_to_all(pieces.reshape(stretches, 8, WIDTH), SP_TP, 0, 0, axis_index_groups=groups, tiled=True)
    query, wide, stats = call(
        local_kernel,
        (key_shape, rows_shape, logs_shape),
        (v, v, v),
        [v, m, v, v, v, m, n, n],
        [room(key_shape), room(value_shape), room(value_shape), room(w_query), room(pre_shape), room(w_ogate), pltpu.VMEM((HEADS * ROWS, ROWS), F32), dma((12,))],
        flops=6_000_000_000,
        limit=16,
        aliases={2: 0, 0: 1, 4: 2},
    )(rows, w_query, key, value, logs, w_ogate, conv_query, head_gain)
    pieces, query, wide, stats = lax.optimization_barrier((pieces, query, wide, stats))
    piece_shape = shape((stretches * 8, WIDTH), BF)
    state = call(prefix_kernel, piece_shape, n, [n, n], flops=100_000_000_000)(pieces.reshape(piece_shape.shape), place)
    state = lax.all_to_all(state.reshape(stretches, 8, WIDTH), SP_TP, 0, 0, axis_index_groups=groups, tiled=True)
    state = state.reshape(HEADS * DQK, WIDTH)
    hidden = pltpu.VMEM((HALF, HEADS * DV), BF)
    sent = call(sent_kernel, shape((HALF, width), BF), n, [v, v, n, v, n], [hidden], flops=1_000_000_000)(
        query, wide, state, stats, w_out
    )
    got = lax.ppermute(sent, "tp", [(0, 1), (1, 0)])
    kept = call(kept_kernel, shape((HALF, width), F32), n, [v, v, n, v, n], [hidden], flops=1_000_000_000)(
        query, wide, state, stats, w_out
    )
    return (kept + got.astype(F32)).astype(BF)


def solution(mesh):
    split = Mesh(mesh.devices.reshape(4, 4, 4, mesh.shape["tp"]), ("sp_0", "sp_1", "sp_2", "tp"))
    placed = (
        P(SP_TP, None),
        P(),
        P(None, "tp"),
        P(None, "tp"),
        P(None, "tp"),
        P(None, "tp"),
        P(),
        P(),
        P(),
        P(),
        P(None, SP, "tp"),
        P(),
        P("tp", None),
    )
    return jax.shard_map(body, mesh=split, in_specs=placed, out_specs=P(SP_TP, None), check_vma=False)
```

```python
import jax
import jax.numpy as jnp
import numpy as np
from jax import lax
from jax.experimental import pallas as pl
from jax.experimental.pallas import tpu as pltpu
from jax.sharding import Mesh
from jax.sharding import PartitionSpec as P


SPAN = 128
SP = ("sp_0", "sp_1", "sp_2")
SP_TP = ("sp_0", "sp_1", "sp_2", "tp")
EPS = 1e-06
EMPTY = -1e30
TAIL = 16
HEADS = 4
DQK = 128
DV = 256
WIDTH = DV + 128
BLOCKS = 3
ROWS = BLOCKS * SPAN
HALF = ROWS // 2
HIGHEST = lax.Precision.HIGHEST
BF = jnp.bfloat16
F32 = jnp.float32
MIB = 1 << 20


def call(kernel, outs, out_spaces, spaces, scratch=(), flops=0, limit=8, aliases=None):
    def spec(space):
        return pl.BlockSpec(memory_space=pltpu.VMEM if space is None else space)

    def placed(like, space):
        return like if space is None else space(like.shape, like.dtype)

    several = isinstance(outs, tuple)
    run = pl.pallas_call(
        kernel,
        out_shape=tuple(map(placed, outs, out_spaces)) if several else placed(outs, out_spaces),
        in_specs=[spec(space) for space in spaces],
        out_specs=tuple(map(spec, out_spaces)) if several else spec(out_spaces),
        scratch_shapes=list(scratch),
        input_output_aliases=aliases or {},
        cost_estimate=pl.CostEstimate(flops=flops, transcendentals=0, bytes_accessed=1 << 20),
        compiler_params=pltpu.CompilerParams(vmem_limit_bytes=limit * MIB),
    )

    def kept(x, space):
        return x if space is None else pltpu.with_memory_space_constraint(x, space)

    return lambda *args: run(*map(kept, args, spaces))


def started(pairs, sems):
    copies = [pltpu.make_async_copy(src, dst, sems.at[n]) for n, (src, dst) in enumerate(pairs)]
    for copy in copies:
        copy.start()
    return copies


def by_rows(src, dst, parts):
    rows = src.shape[0] // parts
    return [(src.at[pl.ds(c * rows, rows)], dst.at[pl.ds(c * rows, rows)]) for c in range(parts)]


def wait_all(copies):
    for copy in copies:
        copy.wait()


def thirds(x):
    hi = x.astype(BF).astype(F32)
    rest = x - hi
    mid = rest.astype(BF).astype(F32)
    return hi, mid, (rest - mid).astype(BF).astype(F32)


def lane_of(shape):
    return lax.broadcasted_iota(jnp.int32, shape, len(shape) - 1)


def mixed_rows(pre_ref, taps, lanes, first, rows):
    acc = None
    for j in range(4):
        term = taps[j : j + 1, lanes] * pre_ref[pl.ds(first + TAIL - 3 + j, rows), lanes]
        acc = term if acc is None else acc + term
    return acc * (1.0 / (1.0 + jnp.exp(-acc)))


def row_scale(x):
    return lax.rsqrt(jnp.mean(x * x, axis=-1, keepdims=True) + EPS)


def normalized(x, gain):
    x = x.astype(F32)
    return (x * row_scale(x) * gain).astype(BF)


def fetch_kernel(own_hbm, gain_hbm, wi_hbm, wf_hbm,
                 rows_ref, wg_ref, gates_ref, own_ref, gain_ref, wi_ref, wf_ref, flat_ref, sems):
    copies = started([(own_hbm, own_ref), (gain_hbm, gain_ref), (wi_hbm, wi_ref), (wf_hbm, wf_ref)], sems)
    copies[0].wait()
    parts = [slice(at, at + 48) for at in range(0, HALF, 48)]
    scales = [row_scale(own_ref[part, :].astype(F32)) for part in parts]
    copies[1].wait()
    gain = gain_ref[...]
    for part, scale in zip(parts, scales):
        rows_ref[part, :] = (own_ref[part, :].astype(F32) * scale * gain).astype(BF)
    wait_all(copies[2:4])
    all_heads = wi_ref.shape[0]
    flat_ref[...] = jnp.zeros_like(flat_ref)
    flat_ref[0:all_heads, :] = wi_ref[...].astype(F32)
    flat_ref[all_heads : 2 * all_heads, :] = wf_ref[...].astype(F32)
    for at in range(0, wg_ref.shape[0], 128):
        wg_ref[at : at + 128, :] = flat_ref[:, at : at + 128].T.astype(BF)
    gates_ref[...] = jnp.dot(rows_ref[...], wg_ref[...], preferred_element_type=F32)


def spread_kernel(own_ref, oth_ref, gain_ref, rows_ref, tail_ref):
    tp = lax.axis_index("tp")
    gain = gain_ref[...]
    rows_ref[0:TAIL, :] = jnp.zeros((TAIL, rows_ref.shape[1]), BF)
    rows_ref[pl.ds(pl.multiple_of(TAIL + tp * HALF, 16), HALF), :] = own_ref[...]
    for part in range(HALF // 48):
        to = pl.multiple_of(TAIL + (1 - tp) * HALF + part * 48, 16)
        rows_ref[pl.ds(to, 48), :] = normalized(oth_ref[part * 48 : part * 48 + 48, :], gain)
    tail_ref[...] = rows_ref[ROWS : ROWS + TAIL, :]


def project_kernel(rows_ref, wk_ref, wv_ref, wg_ref, gates_ref, pre_ref, value_ref, both_ref):
    tp = lax.axis_index("tp")
    own = pl.ds(TAIL, ROWS)
    both_ref[pl.ds(pl.multiple_of(tp * HALF, 8), HALF), :] = gates_ref[...]
    both_ref[pl.ds(pl.multiple_of((1 - tp) * HALF, 8), HALF), :] = jnp.dot(
        rows_ref[pl.ds(pl.multiple_of(TAIL + (1 - tp) * HALF, 16), HALF), :], wg_ref[...], preferred_element_type=F32
    )
    pre_ref[...] = jnp.dot(rows_ref[own, :], wk_ref[...], preferred_element_type=F32).astype(BF).astype(F32)
    value_ref[...] = jnp.dot(rows_ref[own, :], wv_ref[...], preferred_element_type=F32).astype(BF)


def summary_kernel(rows_ref, tail_ref, wk_ref, own_pre_ref, value_ref, both_ref, taps_ref, offs_ref,
                   rows_out, key_ref, logs_ref, piece_out, pre_ref, piece_ref, sems):
    tp = lax.axis_index("tp")
    later = sum(lax.axis_index(axis) for axis in SP) > 0
    rows_out[0:TAIL, :] = jnp.where(later, tail_ref[...], jnp.zeros_like(tail_ref))
    pre_ref[0:TAIL, :] = jnp.dot(rows_out[0:TAIL, :], wk_ref[...], preferred_element_type=F32).astype(BF).astype(F32)
    pre_ref[TAIL : TAIL + ROWS, :] = own_pre_ref[...]
    gates = both_ref[...]
    gates = jnp.where(tp == 0, gates, pltpu.roll(gates, 128 - HEADS, 1))
    lane = lane_of((SPAN, 128))
    tri = (lax.broadcasted_iota(jnp.int32, (SPAN, SPAN), 0) >= lax.broadcasted_iota(jnp.int32, (SPAN, SPAN), 1)).astype(F32)
    gate, inside, totals = [], [], []
    for b in range(BLOCKS):
        offs = jnp.zeros((1, 128), F32)
        for h in range(HEADS):
            for row, at in ((0, h), (1, 2 * HEADS + h)):
                offs = jnp.where(lane_of((1, 128)) == at, offs_ref[b, row : row + 1, h : h + 1], offs)
        g = gates[b * SPAN : (b + 1) * SPAN] + offs
        soft = jnp.minimum(g, 0.0) - jnp.log1p(jnp.exp(-jnp.abs(g)))
        total = jnp.dot(tri, soft, precision=HIGHEST, preferred_element_type=F32)
        logs_ref[b * SPAN : (b + 1) * SPAN, :] = jnp.where(lane < HEADS, g, pltpu.roll(total, 128 - HEADS, 1))
        total = pltpu.roll(total, 128 - 2 * HEADS, 1)
        gate.append(g)
        inside.append(total)
        totals.append(total[SPAN - 1 : SPAN, :])
    write, level = [], None
    later = jnp.zeros_like(totals[0])
    for b in reversed(range(BLOCKS)):
        w = (totals[b] - inside[b]) + later + gate[b]
        later = later + totals[b]
        write.insert(0, w)
        top = jnp.max(w, axis=0, keepdims=True)
        level = top if level is None else jnp.maximum(level, top)
    weight = [jnp.exp(w - level) for w in write]
    numbers = thirds(later) + thirds(level)

    taps = taps_ref[:, pl.ds(pl.multiple_of(tp * (HEADS * DQK), 128), HEADS * DQK)].astype(F32)
    for h in range(HEADS):
        lanes = slice(h * DQK, (h + 1) * DQK)
        for b in range(BLOCKS):
            rows = slice(b * SPAN, (b + 1) * SPAN)
            key_ref[rows, lanes] = (mixed_rows(pre_ref, taps, lanes, b * SPAN, SPAN) * DQK**-0.5).astype(BF)
    ones = jnp.ones((ROWS, 128), BF)
    copies = []
    dims = (((0,), (0,)), ((), ()))
    for h in range(HEADS):
        lanes = slice(h * DQK, (h + 1) * DQK)
        weighted = jnp.concatenate(
            [
                (key_ref[b * SPAN : (b + 1) * SPAN, lanes].astype(F32) * weight[b][:, h : h + 1]).astype(BF)
                for b in range(BLOCKS)
            ],
            axis=0,
        )
        memory = lax.dot_general(weighted, value_ref[:, h * DV : (h + 1) * DV], dims, preferred_element_type=F32)
        extra = lax.dot_general(weighted, ones, dims, preferred_element_type=F32)
        for n, number in enumerate(numbers):
            extra = jnp.where(lane == n + 1, number[:, h : h + 1], extra)
        out = slice(h * DQK, (h + 1) * DQK)
        piece_ref[out, :DV] = memory.astype(BF)
        piece_ref[out, DV:] = extra.astype(BF)
        copy = pltpu.make_async_copy(piece_ref.at[pl.ds(h * DQK, DQK)], piece_out.at[pl.ds(h * DQK, DQK)], sems.at[h])
        copy.start()
        copies.append(copy)
    wait_all(copies)


def prefix_kernel(piece_ref, place_ref, out_ref):
    count = piece_ref.shape[0] // 8
    tall = piece_ref.shape[0]

    def iota(shape, dim):
        return lax.broadcasted_iota(jnp.int32, shape, dim)

    def ones_where(test):
        return jnp.where(test, 1.0, 0.0).astype(BF)

    first = ones_where(iota((count, tall), 1) == 8 * iota((count, tall), 0))
    down = iota((tall, count), 0) - 8 * iota((tall, count), 1)
    spread = ones_where((down >= 0) & (down < 8))
    over = iota((count, tall), 1) - 8 * iota((count, tall), 0)
    spread_over = ones_where((over >= 0) & (over < 8))
    extra = jnp.dot(first, piece_ref[:, DV:], preferred_element_type=F32)
    lane = lane_of((count, 128))

    def number(at):
        return jnp.sum(jnp.where((lane >= at) & (lane < at + 3), extra, 0.0), axis=1, keepdims=True)

    forget, level = number(1), number(4)
    down, over = place_ref[0], place_ref[1]
    steps = jnp.where(down > over, forget, jnp.where(down == over, level, 0.0))
    earlier = over < down
    logs = jnp.dot(jnp.where(earlier, 1.0, 0.0), steps, precision=HIGHEST, preferred_element_type=F32)
    logs = jnp.where(earlier, logs, EMPTY)
    top = jnp.max(logs, axis=1, keepdims=True)
    weight = jnp.where(earlier, jnp.exp(logs - top), 0.0).astype(BF)
    weight = jnp.dot(weight, spread_over, preferred_element_type=F32).astype(BF)
    weight = jnp.dot(spread, weight, preferred_element_type=F32)
    same = (iota((tall, tall), 0) & 7) == (iota((tall, tall), 1) & 7)
    weight = jnp.where(same, weight, 0.0).astype(BF)
    marks = jnp.zeros((count, 128), F32)
    for n, mark in enumerate(thirds(top)):
        marks = jnp.where(lane == n + 1, mark, marks)
    marks = jnp.dot(spread, marks.astype(BF), preferred_element_type=F32)
    state = jnp.dot(weight, piece_ref[...], preferred_element_type=F32)
    lane = lane_of((tall, 128))
    out_ref[:, :DV] = state[:, :DV].astype(BF)
    out_ref[:, DV:] = jnp.where((lane >= 1) & (lane < 4), marks, state[:, DV:]).astype(BF)


def local_kernel(rows_ref, wq_hbm, key_ref, value_ref, logs_ref, wo_hbm, taps_ref, gain_ref,
                 query_out, wide_out, stats_ref, query_ref, numer_ref, ogate_ref, wq_ref, pre_ref, wo_ref, weight_ref, sems):
    copies = started(by_rows(wq_hbm, wq_ref, 4) + by_rows(wo_hbm, wo_ref, 8), sems)
    tp = lax.axis_index("tp")
    taps = taps_ref[:, pl.ds(pl.multiple_of(tp * (HEADS * DQK), 128), HEADS * DQK)].astype(F32)
    lane = lane_of((SPAN, 128))
    cols = [logs_ref[b * SPAN : (b + 1) * SPAN, :] for b in range(BLOCKS)]
    flat = [c.T for c in cols]
    ends = [c[SPAN - 1 : SPAN, :] for c in cols]
    causal = lax.broadcasted_iota(jnp.int32, (SPAN, SPAN), 0) >= lax.broadcasted_iota(jnp.int32, (SPAN, SPAN), 1)
    stats = []
    before = jnp.zeros_like(ends[0])
    for b in range(BLOCKS):
        carried = pltpu.roll(cols[b] + before, HEADS, 1)
        before = before + ends[b]
        stats.append(jnp.where((lane >= 2 * HEADS) & (lane < 3 * HEADS), carried, 0.0))
    nt = (((1,), (1,)), ((), ()))
    for h in range(HEADS):
        head = slice(h * DQK, (h + 1) * DQK)
        wide = slice(h * DV, (h + 1) * DV)
        for t in range(BLOCKS):
            rows = slice(t * SPAN, (t + 1) * SPAN)
            seen = (t + 1) * SPAN
            now = cols[t][:, HEADS + h : HEADS + h + 1]
            logs = []
            for s in range(t + 1):
                gate = flat[s][h : h + 1, :]
                past = flat[s][HEADS + h : HEADS + h + 1, :]
                if s == t:
                    logs.append(jnp.where(causal, (now - past) + gate, EMPTY))
                else:
                    rest = ends[s][:, HEADS + h : HEADS + h + 1] - past
                    for c in range(s + 1, t):
                        rest = rest + ends[c][:, HEADS + h : HEADS + h + 1]
                    logs.append(now + (rest + gate))
            top = None
            for x in logs:
                peak = jnp.max(x, axis=1, keepdims=True)
                top = peak if top is None else jnp.maximum(top, peak)
            for s, x in enumerate(logs):
                weight_ref[h * ROWS + t * SPAN : h * ROWS + (t + 1) * SPAN, s * SPAN : (s + 1) * SPAN] = jnp.exp(x - top)
            stats[t] = jnp.where(lane == HEADS + h, top, stats[t])
    wait_all(copies[:4])
    pre_ref[...] = jnp.dot(rows_ref[...], wq_ref[...], preferred_element_type=F32).astype(BF).astype(F32)
    for h in range(HEADS):
        lanes = slice(h * DQK, (h + 1) * DQK)
        for b in range(BLOCKS):
            rows = slice(b * SPAN, (b + 1) * SPAN)
            query_ref[rows, lanes] = mixed_rows(pre_ref, taps, lanes, b * SPAN, SPAN).astype(BF)
    for h in range(HEADS):
        head = slice(h * DQK, (h + 1) * DQK)
        wide = slice(h * DV, (h + 1) * DV)
        for t in range(BLOCKS):
            rows = slice(t * SPAN, (t + 1) * SPAN)
            seen = (t + 1) * SPAN
            weight = weight_ref[h * ROWS + t * SPAN : h * ROWS + (t + 1) * SPAN, :seen]
            scores = (
                lax.dot_general(query_ref[rows, head], key_ref[:seen, head], nt, preferred_element_type=F32) * weight
            )
            denom = jnp.sum(scores, axis=1, keepdims=True)
            numer = jnp.dot(scores.astype(BF), value_ref[:seen, wide], preferred_element_type=F32)
            numer_ref[rows, wide] = numer.astype(BF)
            stats[t] = jnp.where(lane == h, denom, stats[t])
    for t in range(BLOCKS):
        stats_ref[t * SPAN : (t + 1) * SPAN, :] = stats[t]
    wait_all(copies[4:])
    gain = gain_ref[:, pl.ds(pl.multiple_of(tp * (HEADS * DV), 128), HEADS * DV)]
    for c in range(2):
        cols = slice(c * HEADS * DV // 2, (c + 1) * HEADS * DV // 2)
        pre = jnp.dot(rows_ref[pl.ds(TAIL, ROWS), :], wo_ref[:, cols], preferred_element_type=F32).astype(BF).astype(F32)
        ogate_ref[:, cols] = (gain[:, cols] / (1.0 + jnp.exp(-pre))).astype(BF)
    query_out[...] = query_ref[...]
    wide_out[0:ROWS, : HEADS * DV] = numer_ref[...]
    wide_out[0:ROWS, HEADS * DV :] = ogate_ref[...]


def hidden_rows(first, query_ref, wide_ref, state_ref, stats_ref, hidden_ref):
    rows = pl.ds(pl.multiple_of(first, 16), HALF)
    lane = lane_of((HALF, 128))
    stats = stats_ref[rows, :]
    place = lane_of((DQK, 128))
    norms, level = [], jnp.zeros((1, 128), F32)
    for h in range(HEADS):
        extra = state_ref[h * DQK : (h + 1) * DQK, DV:].astype(F32)
        norms.append(jnp.where(place == h, extra[:, 0:1], 0.0).astype(BF))
        mark = extra[0:1, 1:2] + extra[0:1, 2:3] + extra[0:1, 3:4]
        level = jnp.where(lane_of((1, 128)) == h, mark, level)
    norms = jnp.concatenate(norms, axis=0)
    query = query_ref[rows, :]
    read_norm = jnp.dot(query, norms, preferred_element_type=F32)
    top = pltpu.roll(stats, 128 - HEADS, 1)
    carried = pltpu.roll(stats, 128 - 2 * HEADS, 1) + level
    peak = jnp.maximum(carried, top)
    one = jnp.exp(carried - peak)
    two = jnp.exp(top - peak)
    denom = one * read_norm + two * stats
    denom = jnp.maximum(jnp.abs(denom), jnp.exp(-peak))
    one = one / denom
    two = two / denom
    for h in range(HEADS):
        wide = slice(h * DV, (h + 1) * DV)
        read = jnp.dot(
            query[:, h * DQK : (h + 1) * DQK], state_ref[h * DQK : (h + 1) * DQK, :DV], preferred_element_type=F32
        )
        cell = one[:, h : h + 1] * read + two[:, h : h + 1] * wide_ref[rows, wide].astype(F32)
        scale = lax.rsqrt(jnp.mean(cell * cell, axis=-1, keepdims=True) + EPS)
        hidden_ref[:, wide] = (cell * scale * wide_ref[rows, HEADS * DV + h * DV : HEADS * DV + (h + 1) * DV].astype(F32)).astype(BF)


def sent_kernel(query_ref, wide_ref, state_ref, stats_ref, wout_ref, out_ref, hidden_ref):
    first = (1 - lax.axis_index("tp")) * HALF
    hidden_rows(first, query_ref, wide_ref, state_ref, stats_ref, hidden_ref)
    out_ref[...] = jnp.dot(hidden_ref[...], wout_ref[...], preferred_element_type=F32).astype(BF)


def kept_kernel(query_ref, wide_ref, state_ref, stats_ref, wout_ref, out_ref, hidden_ref):
    first = lax.axis_index("tp") * HALF
    hidden_rows(first, query_ref, wide_ref, state_ref, stats_ref, hidden_ref)
    out_ref[...] = jnp.dot(hidden_ref[...], wout_ref[...], preferred_element_type=F32)


def far_first(stretches):
    at = np.arange(stretches)
    hops = sum(np.minimum(c, 4 - c) for c in (at // 16, at // 4 % 4, at % 4))
    return np.lexsort((at, -hops))


def body(
    tokens, norm_gain, w_query, w_key, w_value, w_ogate, w_igate, w_fgate, conv_query, conv_key, gate_offset, head_gain, w_out
):
    width = tokens.shape[1]
    stretches = lax.axis_size(SP)
    shape = jax.ShapeDtypeStruct
    other = lax.ppermute(tokens, "tp", [(0, 1), (1, 0)])
    gain = norm_gain.reshape(1, -1)
    head_gain = head_gain.reshape(1, -1)
    order = far_first(stretches)
    groups = [[2 * int(i) + t for i in order] for t in range(2)]
    place = np.stack([np.broadcast_to(order[:, None], (stretches, stretches)), np.broadcast_to(order, (stretches, stretches))])
    place = jnp.asarray(place.astype(np.int32))
    v, m, n = pltpu.VMEM, pltpu.HBM, None
    dma = pltpu.SemaphoreType.DMA
    key_shape, value_shape = shape((ROWS, HEADS * DQK), BF), shape((ROWS, HEADS * DV), BF)
    logs_shape = shape((ROWS, 128), F32)
    rows_shape, pre_shape = shape((TAIL + ROWS, width), BF), shape((TAIL + ROWS, HEADS * DQK), F32)

    def room(like):
        return pltpu.VMEM(like.shape, like.dtype)

    gates_shape = shape((width, 128), BF), shape((HALF, 128), F32)
    own, wg, gates = call(
        fetch_kernel,
        (shape(tokens.shape, BF), *gates_shape),
        (v, v, v),
        [m, m, m, m],
        [room(tokens), room(gain), *[pltpu.VMEM((w_igate.shape[1], width), BF)] * 2, pltpu.VMEM((128, width), F32), dma((4,))],
        flops=100_000_000_000,
    )(tokens, gain, w_igate.T, w_fgate.T)
    rows, last = call(spread_kernel, (rows_shape, shape((TAIL, width), BF)), (v, n), [v, n, n], flops=100_000_000)(own, other, gain)
    tail = lax.ppermute(last, SP, [(i, (i + 1) % stretches) for i in range(stretches)])
    own_pre_shape = shape((ROWS, HEADS * DQK), F32)
    own_pre, value, both = call(
        project_kernel,
        (own_pre_shape, value_shape, logs_shape),
        (v, v, v),
        [v, n, n, v, v],
        flops=3_000_000_000,
    )(rows, w_key, w_value, wg, gates)
    rows, key, logs, pieces = call(
        summary_kernel,
        (rows_shape, key_shape, logs_shape, shape((HEADS * DQK, WIDTH), BF)),
        (v, v, v, m),
        [v, n, n, v, v, v, n, n],
        [room(pre_shape), pltpu.VMEM((HEADS * DQK, WIDTH), BF), dma((HEADS,))],
        flops=1_000_000_000,
        aliases={0: 0},
    )(rows, tail, w_key, own_pre, value, both, conv_key, gate_offset.transpose(1, 0, 2))
    pieces = lax.all_to_all(pieces.reshape(stretches, 8, WIDTH), SP_TP, 0, 0, axis_index_groups=groups, tiled=True)
    query, wide, stats = call(
        local_kernel,
        (key_shape, rows_shape, logs_shape),
        (v, v, v),
        [v, m, v, v, v, m, n, n],
        [room(key_shape), room(value_shape), room(value_shape), room(w_query), room(pre_shape), room(w_ogate), pltpu.VMEM((HEADS * ROWS, ROWS), F32), dma((12,))],
        flops=6_000_000_000,
        limit=16,
        aliases={2: 0, 0: 1, 4: 2},
    )(rows, w_query, key, value, logs, w_ogate, conv_query, head_gain)
    pieces, query, wide, stats = lax.optimization_barrier((pieces, query, wide, stats))
    piece_shape = shape((stretches * 8, WIDTH), BF)
    state = call(prefix_kernel, piece_shape, n, [n, n], flops=100_000_000_000)(pieces.reshape(piece_shape.shape), place)
    state = lax.all_to_all(state.reshape(stretches, 8, WIDTH), SP_TP, 0, 0, axis_index_groups=groups, tiled=True)
    state = state.reshape(HEADS * DQK, WIDTH)
    hidden = pltpu.VMEM((HALF, HEADS * DV), BF)
    sent = call(sent_kernel, shape((HALF, width), BF), n, [v, v, n, v, n], [hidden], flops=1_000_000_000)(
        query, wide, state, stats, w_out
    )
    got = lax.ppermute(sent, "tp", [(0, 1), (1, 0)])
    kept = call(kept_kernel, shape((HALF, width), F32), n, [v, v, n, v, n], [hidden], flops=1_000_000_000)(
        query, wide, state, stats, w_out
    )
    return (kept + got.astype(F32)).astype(BF)


def solution(mesh):
    split = Mesh(mesh.devices.reshape(4, 4, 4, mesh.shape["tp"]), ("sp_0", "sp_1", "sp_2", "tp"))
    placed = (
        P(SP_TP, None),
        P(),
        P(None, "tp"),
        P(None, "tp"),
        P(None, "tp"),
        P(None, "tp"),
        P(),
        P(),
        P(),
        P(),
        P(None, SP, "tp"),
        P(),
        P("tp", None),
    )
    return jax.shard_map(body, mesh=split, in_specs=placed, out_specs=P(SP_TP, None), check_vma=False)
```

```python
import jax
import jax.numpy as jnp
import numpy as np
from jax import lax
from jax.experimental import pallas as pl
from jax.experimental.pallas import tpu as pltpu
from jax.sharding import Mesh
from jax.sharding import PartitionSpec as P


SPAN = 128
SP = ("sp_0", "sp_1", "sp_2")
SP_TP = ("sp_0", "sp_1", "sp_2", "tp")
EPS = 1e-06
EMPTY = -1e30
TAIL = 16
HEADS = 4
DQK = 128
DV = 256
WIDTH = DV + 128
BLOCKS = 3
ROWS = BLOCKS * SPAN
HALF = ROWS // 2
HIGHEST = lax.Precision.HIGHEST
BF = jnp.bfloat16
F32 = jnp.float32
MIB = 1 << 20


def call(kernel, outs, out_spaces, spaces, scratch=(), flops=0, limit=8, aliases=None):
    def spec(space):
        return pl.BlockSpec(memory_space=pltpu.VMEM if space is None else space)

    def placed(like, space):
        return like if space is None else space(like.shape, like.dtype)

    several = isinstance(outs, tuple)
    run = pl.pallas_call(
        kernel,
        out_shape=tuple(map(placed, outs, out_spaces)) if several else placed(outs, out_spaces),
        in_specs=[spec(space) for space in spaces],
        out_specs=tuple(map(spec, out_spaces)) if several else spec(out_spaces),
        scratch_shapes=list(scratch),
        input_output_aliases=aliases or {},
        cost_estimate=pl.CostEstimate(flops=flops, transcendentals=0, bytes_accessed=1 << 20),
        compiler_params=pltpu.CompilerParams(vmem_limit_bytes=limit * MIB),
    )

    def kept(x, space):
        return x if space is None else pltpu.with_memory_space_constraint(x, space)

    return lambda *args: run(*map(kept, args, spaces))


def started(pairs, sems):
    copies = [pltpu.make_async_copy(src, dst, sems.at[n]) for n, (src, dst) in enumerate(pairs)]
    for copy in copies:
        copy.start()
    return copies


def by_rows(src, dst, parts):
    rows = src.shape[0] // parts
    return [(src.at[pl.ds(c * rows, rows)], dst.at[pl.ds(c * rows, rows)]) for c in range(parts)]


def wait_all(copies):
    for copy in copies:
        copy.wait()


def thirds(x):
    hi = x.astype(BF).astype(F32)
    rest = x - hi
    mid = rest.astype(BF).astype(F32)
    return hi, mid, (rest - mid).astype(BF).astype(F32)


def lane_of(shape):
    return lax.broadcasted_iota(jnp.int32, shape, len(shape) - 1)


def mixed_rows(pre_ref, taps, lanes, first, rows):
    acc = None
    for j in range(4):
        term = taps[j : j + 1, lanes] * pre_ref[pl.ds(first + TAIL - 3 + j, rows), lanes]
        acc = term if acc is None else acc + term
    return acc * (1.0 / (1.0 + jnp.exp(-acc)))


def row_scale(x):
    return lax.rsqrt(jnp.mean(x * x, axis=-1, keepdims=True) + EPS)


def normalized(x, gain):
    x = x.astype(F32)
    return (x * row_scale(x) * gain).astype(BF)


def fetch_kernel(own_hbm, gain_hbm, wi_hbm, wf_hbm,
                 rows_ref, wg_ref, gates_ref, own_ref, gain_ref, wi_ref, wf_ref, flat_ref, sems):
    copies = started([(own_hbm, own_ref), (gain_hbm, gain_ref), (wi_hbm, wi_ref), (wf_hbm, wf_ref)], sems)
    copies[0].wait()
    parts = [slice(at, at + 48) for at in range(0, HALF, 48)]
    scales = [row_scale(own_ref[part, :].astype(F32)) for part in parts]
    copies[1].wait()
    gain = gain_ref[...]
    for part, scale in zip(parts, scales):
        rows_ref[part, :] = (own_ref[part, :].astype(F32) * scale * gain).astype(BF)
    wait_all(copies[2:4])
    all_heads = wi_ref.shape[0]
    flat_ref[...] = jnp.zeros_like(flat_ref)
    flat_ref[0:all_heads, :] = wi_ref[...].astype(F32)
    flat_ref[all_heads : 2 * all_heads, :] = wf_ref[...].astype(F32)
    for at in range(0, wg_ref.shape[0], 128):
        wg_ref[at : at + 128, :] = flat_ref[:, at : at + 128].T.astype(BF)
    gates_ref[...] = jnp.dot(rows_ref[...], wg_ref[...], preferred_element_type=F32)


def spread_kernel(own_ref, oth_ref, gain_ref, rows_ref, tail_ref):
    tp = lax.axis_index("tp")
    gain = gain_ref[...]
    rows_ref[0:TAIL, :] = jnp.zeros((TAIL, rows_ref.shape[1]), BF)
    rows_ref[pl.ds(pl.multiple_of(TAIL + tp * HALF, 16), HALF), :] = own_ref[...]
    for part in range(HALF // 48):
        to = pl.multiple_of(TAIL + (1 - tp) * HALF + part * 48, 16)
        rows_ref[pl.ds(to, 48), :] = normalized(oth_ref[part * 48 : part * 48 + 48, :], gain)
    tail_ref[...] = rows_ref[ROWS : ROWS + TAIL, :]


def project_kernel(rows_ref, wk_ref, wv_ref, wg_ref, gates_ref, pre_ref, value_ref, both_ref):
    tp = lax.axis_index("tp")
    own = pl.ds(TAIL, ROWS)
    both_ref[pl.ds(pl.multiple_of(tp * HALF, 8), HALF), :] = gates_ref[...]
    both_ref[pl.ds(pl.multiple_of((1 - tp) * HALF, 8), HALF), :] = jnp.dot(
        rows_ref[pl.ds(pl.multiple_of(TAIL + (1 - tp) * HALF, 16), HALF), :], wg_ref[...], preferred_element_type=F32
    )
    pre_ref[...] = jnp.dot(rows_ref[own, :], wk_ref[...], preferred_element_type=F32).astype(BF).astype(F32)
    value_ref[...] = jnp.dot(rows_ref[own, :], wv_ref[...], preferred_element_type=F32).astype(BF)


def summary_kernel(rows_ref, tail_ref, wk_ref, own_pre_ref, value_ref, both_ref, taps_ref, offs_ref,
                   rows_out, key_ref, logs_ref, piece_out, pre_ref, piece_ref, sems):
    tp = lax.axis_index("tp")
    later = sum(lax.axis_index(axis) for axis in SP) > 0
    rows_out[0:TAIL, :] = jnp.where(later, tail_ref[...], jnp.zeros_like(tail_ref))
    pre_ref[0:TAIL, :] = jnp.dot(rows_out[0:TAIL, :], wk_ref[...], preferred_element_type=F32).astype(BF).astype(F32)
    pre_ref[TAIL : TAIL + ROWS, :] = own_pre_ref[...]
    gates = both_ref[...]
    gates = jnp.where(tp == 0, gates, pltpu.roll(gates, 128 - HEADS, 1))
    lane = lane_of((SPAN, 128))
    tri = (lax.broadcasted_iota(jnp.int32, (SPAN, SPAN), 0) >= lax.broadcasted_iota(jnp.int32, (SPAN, SPAN), 1)).astype(F32)
    gate, inside, totals = [], [], []
    for b in range(BLOCKS):
        offs = jnp.zeros((1, 128), F32)
        for h in range(HEADS):
            for row, at in ((0, h), (1, 2 * HEADS + h)):
                offs = jnp.where(lane_of((1, 128)) == at, offs_ref[b, row : row + 1, h : h + 1], offs)
        g = gates[b * SPAN : (b + 1) * SPAN] + offs
        soft = jnp.minimum(g, 0.0) - jnp.log1p(jnp.exp(-jnp.abs(g)))
        total = jnp.dot(tri, soft, precision=HIGHEST, preferred_element_type=F32)
        logs_ref[b * SPAN : (b + 1) * SPAN, :] = jnp.where(lane < HEADS, g, pltpu.roll(total, 128 - HEADS, 1))
        total = pltpu.roll(total, 128 - 2 * HEADS, 1)
        gate.append(g)
        inside.append(total)
        totals.append(total[SPAN - 1 : SPAN, :])
    write, level = [], None
    later = jnp.zeros_like(totals[0])
    for b in reversed(range(BLOCKS)):
        w = (totals[b] - inside[b]) + later + gate[b]
        later = later + totals[b]
        write.insert(0, w)
        top = jnp.max(w, axis=0, keepdims=True)
        level = top if level is None else jnp.maximum(level, top)
    weight = [jnp.exp(w - level) for w in write]
    numbers = thirds(later) + thirds(level)

    taps = taps_ref[:, pl.ds(pl.multiple_of(tp * (HEADS * DQK), 128), HEADS * DQK)].astype(F32)
    for h in range(HEADS):
        lanes = slice(h * DQK, (h + 1) * DQK)
        for b in range(BLOCKS):
            rows = slice(b * SPAN, (b + 1) * SPAN)
            key_ref[rows, lanes] = (mixed_rows(pre_ref, taps, lanes, b * SPAN, SPAN) * DQK**-0.5).astype(BF)
    ones = jnp.ones((ROWS, 128), BF)
    copies = []
    dims = (((0,), (0,)), ((), ()))
    for h in range(HEADS):
        lanes = slice(h * DQK, (h + 1) * DQK)
        weighted = jnp.concatenate(
            [
                (key_ref[b * SPAN : (b + 1) * SPAN, lanes].astype(F32) * weight[b][:, h : h + 1]).astype(BF)
                for b in range(BLOCKS)
            ],
            axis=0,
        )
        memory = lax.dot_general(weighted, value_ref[:, h * DV : (h + 1) * DV], dims, preferred_element_type=F32)
        extra = lax.dot_general(weighted, ones, dims, preferred_element_type=F32)
        for n, number in enumerate(numbers):
            extra = jnp.where(lane == n + 1, number[:, h : h + 1], extra)
        out = slice(h * DQK, (h + 1) * DQK)
        piece_ref[out, :DV] = memory.astype(BF)
        piece_ref[out, DV:] = extra.astype(BF)
        copy = pltpu.make_async_copy(piece_ref.at[pl.ds(h * DQK, DQK)], piece_out.at[pl.ds(h * DQK, DQK)], sems.at[h])
        copy.start()
        copies.append(copy)
    wait_all(copies)


def prefix_kernel(piece_ref, place_ref, out_ref):
    count = piece_ref.shape[0] // 8
    tall = piece_ref.shape[0]

    def iota(shape, dim):
        return lax.broadcasted_iota(jnp.int32, shape, dim)

    def ones_where(test):
        return jnp.where(test, 1.0, 0.0).astype(BF)

    first = ones_where(iota((count, tall), 1) == 8 * iota((count, tall), 0))
    down = iota((tall, count), 0) - 8 * iota((tall, count), 1)
    spread = ones_where((down >= 0) & (down < 8))
    over = iota((count, tall), 1) - 8 * iota((count, tall), 0)
    spread_over = ones_where((over >= 0) & (over < 8))
    extra = jnp.dot(first, piece_ref[:, DV:], preferred_element_type=F32)
    lane = lane_of((count, 128))

    def number(at):
        return jnp.sum(jnp.where((lane >= at) & (lane < at + 3), extra, 0.0), axis=1, keepdims=True)

    forget, level = number(1), number(4)
    down, over = place_ref[0], place_ref[1]
    steps = jnp.where(down > over, forget, jnp.where(down == over, level, 0.0))
    earlier = over < down
    logs = jnp.dot(jnp.where(earlier, 1.0, 0.0), steps, precision=HIGHEST, preferred_element_type=F32)
    logs = jnp.where(earlier, logs, EMPTY)
    top = jnp.max(logs, axis=1, keepdims=True)
    weight = jnp.where(earlier, jnp.exp(logs - top), 0.0).astype(BF)
    weight = jnp.dot(weight, spread_over, preferred_element_type=F32).astype(BF)
    weight = jnp.dot(spread, weight, preferred_element_type=F32)
    same = (iota((tall, tall), 0) & 7) == (iota((tall, tall), 1) & 7)
    weight = jnp.where(same, weight, 0.0).astype(BF)
    marks = jnp.zeros((count, 128), F32)
    for n, mark in enumerate(thirds(top)):
        marks = jnp.where(lane == n + 1, mark, marks)
    marks = jnp.dot(spread, marks.astype(BF), preferred_element_type=F32)
    state = jnp.dot(weight, piece_ref[...], preferred_element_type=F32)
    lane = lane_of((tall, 128))
    out_ref[:, :DV] = state[:, :DV].astype(BF)
    out_ref[:, DV:] = jnp.where((lane >= 1) & (lane < 4), marks, state[:, DV:]).astype(BF)


def local_kernel(rows_ref, wq_hbm, key_ref, value_ref, logs_ref, wo_hbm, taps_ref, gain_ref,
                 query_out, wide_out, stats_ref, query_ref, numer_ref, ogate_ref, wq_ref, pre_ref, wo_ref, weight_ref, sems):
    copies = started(by_rows(wq_hbm, wq_ref, 4) + by_rows(wo_hbm, wo_ref, 8), sems)
    tp = lax.axis_index("tp")
    taps = taps_ref[:, pl.ds(pl.multiple_of(tp * (HEADS * DQK), 128), HEADS * DQK)].astype(F32)
    lane = lane_of((SPAN, 128))
    cols = [logs_ref[b * SPAN : (b + 1) * SPAN, :] for b in range(BLOCKS)]
    flat = [c.T for c in cols]
    ends = [c[SPAN - 1 : SPAN, :] for c in cols]
    causal = lax.broadcasted_iota(jnp.int32, (SPAN, SPAN), 0) >= lax.broadcasted_iota(jnp.int32, (SPAN, SPAN), 1)
    stats = []
    before = jnp.zeros_like(ends[0])
    for b in range(BLOCKS):
        carried = pltpu.roll(cols[b] + before, HEADS, 1)
        before = before + ends[b]
        stats.append(jnp.where((lane >= 2 * HEADS) & (lane < 3 * HEADS), carried, 0.0))
    nt = (((1,), (1,)), ((), ()))
    for h in range(HEADS):
        head = slice(h * DQK, (h + 1) * DQK)
        wide = slice(h * DV, (h + 1) * DV)
        for t in range(BLOCKS):
            rows = slice(t * SPAN, (t + 1) * SPAN)
            seen = (t + 1) * SPAN
            now = cols[t][:, HEADS + h : HEADS + h + 1]
            logs = []
            for s in range(t + 1):
                gate = flat[s][h : h + 1, :]
                past = flat[s][HEADS + h : HEADS + h + 1, :]
                if s == t:
                    logs.append(jnp.where(causal, (now - past) + gate, EMPTY))
                else:
                    rest = ends[s][:, HEADS + h : HEADS + h + 1] - past
                    for c in range(s + 1, t):
                        rest = rest + ends[c][:, HEADS + h : HEADS + h + 1]
                    logs.append(now + (rest + gate))
            top = None
            for x in logs:
                peak = jnp.max(x, axis=1, keepdims=True)
                top = peak if top is None else jnp.maximum(top, peak)
            for s, x in enumerate(logs):
                weight_ref[h * ROWS + t * SPAN : h * ROWS + (t + 1) * SPAN, s * SPAN : (s + 1) * SPAN] = jnp.exp(x - top)
            stats[t] = jnp.where(lane == HEADS + h, top, stats[t])
    deep = wq_ref.shape[0] // 4
    for c in range(4):
        copies[c].wait()
        depth = slice(c * deep, (c + 1) * deep)
        part = jnp.dot(rows_ref[:, depth], wq_ref[depth, :], preferred_element_type=F32)
        if c < 3:
            pre_ref[...] = part if c == 0 else pre_ref[...] + part
        else:
            pre_ref[...] = (pre_ref[...] + part).astype(BF).astype(F32)
    for h in range(HEADS):
        lanes = slice(h * DQK, (h + 1) * DQK)
        for b in range(BLOCKS):
            rows = slice(b * SPAN, (b + 1) * SPAN)
            query_ref[rows, lanes] = mixed_rows(pre_ref, taps, lanes, b * SPAN, SPAN).astype(BF)
    for h in range(HEADS):
        head = slice(h * DQK, (h + 1) * DQK)
        wide = slice(h * DV, (h + 1) * DV)
        for t in range(BLOCKS):
            rows = slice(t * SPAN, (t + 1) * SPAN)
            seen = (t + 1) * SPAN
            weight = weight_ref[h * ROWS + t * SPAN : h * ROWS + (t + 1) * SPAN, :seen]
            scores = (
                lax.dot_general(query_ref[rows, head], key_ref[:seen, head], nt, preferred_element_type=F32) * weight
            )
            denom = jnp.sum(scores, axis=1, keepdims=True)
            numer = jnp.dot(scores.astype(BF), value_ref[:seen, wide], preferred_element_type=F32)
            numer_ref[rows, wide] = numer.astype(BF)
            stats[t] = jnp.where(lane == h, denom, stats[t])
    for t in range(BLOCKS):
        stats_ref[t * SPAN : (t + 1) * SPAN, :] = stats[t]
    wait_all(copies[4:])
    gain = gain_ref[:, pl.ds(pl.multiple_of(tp * (HEADS * DV), 128), HEADS * DV)]
    for c in range(2):
        cols = slice(c * HEADS * DV // 2, (c + 1) * HEADS * DV // 2)
        pre = jnp.dot(rows_ref[pl.ds(TAIL, ROWS), :], wo_ref[:, cols], preferred_element_type=F32).astype(BF).astype(F32)
        ogate_ref[:, cols] = (gain[:, cols] / (1.0 + jnp.exp(-pre))).astype(BF)
    query_out[...] = query_ref[...]
    wide_out[0:ROWS, : HEADS * DV] = numer_ref[...]
    wide_out[0:ROWS, HEADS * DV :] = ogate_ref[...]


def hidden_rows(first, query_ref, wide_ref, state_ref, stats_ref, hidden_ref):
    rows = pl.ds(pl.multiple_of(first, 16), HALF)
    lane = lane_of((HALF, 128))
    stats = stats_ref[rows, :]
    place = lane_of((DQK, 128))
    norms, level = [], jnp.zeros((1, 128), F32)
    for h in range(HEADS):
        extra = state_ref[h * DQK : (h + 1) * DQK, DV:].astype(F32)
        norms.append(jnp.where(place == h, extra[:, 0:1], 0.0).astype(BF))
        mark = extra[0:1, 1:2] + extra[0:1, 2:3] + extra[0:1, 3:4]
        level = jnp.where(lane_of((1, 128)) == h, mark, level)
    norms = jnp.concatenate(norms, axis=0)
    query = query_ref[rows, :]
    read_norm = jnp.dot(query, norms, preferred_element_type=F32)
    top = pltpu.roll(stats, 128 - HEADS, 1)
    carried = pltpu.roll(stats, 128 - 2 * HEADS, 1) + level
    peak = jnp.maximum(carried, top)
    one = jnp.exp(carried - peak)
    two = jnp.exp(top - peak)
    denom = one * read_norm + two * stats
    denom = jnp.maximum(jnp.abs(denom), jnp.exp(-peak))
    one = one / denom
    two = two / denom
    for h in range(HEADS):
        wide = slice(h * DV, (h + 1) * DV)
        read = jnp.dot(
            query[:, h * DQK : (h + 1) * DQK], state_ref[h * DQK : (h + 1) * DQK, :DV], preferred_element_type=F32
        )
        cell = one[:, h : h + 1] * read + two[:, h : h + 1] * wide_ref[rows, wide].astype(F32)
        scale = lax.rsqrt(jnp.mean(cell * cell, axis=-1, keepdims=True) + EPS)
        hidden_ref[:, wide] = (cell * scale * wide_ref[rows, HEADS * DV + h * DV : HEADS * DV + (h + 1) * DV].astype(F32)).astype(BF)


def sent_kernel(query_ref, wide_ref, state_ref, stats_ref, wout_ref, out_ref, hidden_ref):
    first = (1 - lax.axis_index("tp")) * HALF
    hidden_rows(first, query_ref, wide_ref, state_ref, stats_ref, hidden_ref)
    out_ref[...] = jnp.dot(hidden_ref[...], wout_ref[...], preferred_element_type=F32).astype(BF)


def kept_kernel(query_ref, wide_ref, state_ref, stats_ref, wout_ref, out_ref, hidden_ref):
    first = lax.axis_index("tp") * HALF
    hidden_rows(first, query_ref, wide_ref, state_ref, stats_ref, hidden_ref)
    out_ref[...] = jnp.dot(hidden_ref[...], wout_ref[...], preferred_element_type=F32)


def far_first(stretches):
    at = np.arange(stretches)
    hops = sum(np.minimum(c, 4 - c) for c in (at // 16, at // 4 % 4, at % 4))
    return np.lexsort((-at, -hops))


def body(
    tokens, norm_gain, w_query, w_key, w_value, w_ogate, w_igate, w_fgate, conv_query, conv_key, gate_offset, head_gain, w_out
):
    width = tokens.shape[1]
    stretches = lax.axis_size(SP)
    shape = jax.ShapeDtypeStruct
    other = lax.ppermute(tokens, "tp", [(0, 1), (1, 0)])
    gain = norm_gain.reshape(1, -1)
    head_gain = head_gain.reshape(1, -1)
    order = far_first(stretches)
    groups = [[2 * int(i) + t for i in order] for t in range(2)]
    place = np.stack([np.broadcast_to(order[:, None], (stretches, stretches)), np.broadcast_to(order, (stretches, stretches))])
    place = jnp.asarray(place.astype(np.int32))
    v, m, n = pltpu.VMEM, pltpu.HBM, None
    dma = pltpu.SemaphoreType.DMA
    key_shape, value_shape = shape((ROWS, HEADS * DQK), BF), shape((ROWS, HEADS * DV), BF)
    logs_shape = shape((ROWS, 128), F32)
    rows_shape, pre_shape = shape((TAIL + ROWS, width), BF), shape((TAIL + ROWS, HEADS * DQK), F32)

    def room(like):
        return pltpu.VMEM(like.shape, like.dtype)

    gates_shape = shape((width, 128), BF), shape((HALF, 128), F32)
    own, wg, gates = call(
        fetch_kernel,
        (shape(tokens.shape, BF), *gates_shape),
        (v, v, v),
        [m, m, m, m],
        [room(tokens), room(gain), *[pltpu.VMEM((w_igate.shape[1], width), BF)] * 2, pltpu.VMEM((128, width), F32), dma((4,))],
        flops=100_000_000_000,
    )(tokens, gain, w_igate.T, w_fgate.T)
    rows, last = call(spread_kernel, (rows_shape, shape((TAIL, width), BF)), (v, n), [v, n, n], flops=100_000_000)(own, other, gain)
    tail = lax.ppermute(last, SP, [(i, (i + 1) % stretches) for i in range(stretches)])
    own_pre_shape = shape((ROWS, HEADS * DQK), F32)
    own_pre, value, both = call(
        project_kernel,
        (own_pre_shape, value_shape, logs_shape),
        (v, v, v),
        [v, n, n, v, v],
        flops=3_000_000_000,
    )(rows, w_key, w_value, wg, gates)
    rows, key, logs, pieces = call(
        summary_kernel,
        (rows_shape, key_shape, logs_shape, shape((HEADS * DQK, WIDTH), BF)),
        (v, v, v, m),
        [v, n, n, v, v, v, n, n],
        [room(pre_shape), pltpu.VMEM((HEADS * DQK, WIDTH), BF), dma((HEADS,))],
        flops=1_000_000_000,
        aliases={0: 0},
    )(rows, tail, w_key, own_pre, value, both, conv_key, gate_offset.transpose(1, 0, 2))
    pieces = lax.all_to_all(pieces.reshape(stretches, 8, WIDTH), SP_TP, 0, 0, axis_index_groups=groups, tiled=True)
    query, wide, stats = call(
        local_kernel,
        (key_shape, rows_shape, logs_shape),
        (v, v, v),
        [v, m, v, v, v, m, n, n],
        [room(key_shape), room(value_shape), room(value_shape), room(w_query), room(pre_shape), room(w_ogate), pltpu.VMEM((HEADS * ROWS, ROWS), F32), dma((12,))],
        flops=6_000_000_000,
        limit=16,
        aliases={2: 0, 0: 1, 4: 2},
    )(rows, w_query, key, value, logs, w_ogate, conv_query, head_gain)
    pieces, query, wide, stats = lax.optimization_barrier((pieces, query, wide, stats))
    piece_shape = shape((stretches * 8, WIDTH), BF)
    state = call(prefix_kernel, piece_shape, n, [n, n], flops=100_000_000_000)(pieces.reshape(piece_shape.shape), place)
    state = lax.all_to_all(state.reshape(stretches, 8, WIDTH), SP_TP, 0, 0, axis_index_groups=groups, tiled=True)
    state = state.reshape(HEADS * DQK, WIDTH)
    hidden = pltpu.VMEM((HALF, HEADS * DV), BF)
    sent = call(sent_kernel, shape((HALF, width), BF), n, [v, v, n, v, n], [hidden], flops=1_000_000_000)(
        query, wide, state, stats, w_out
    )
    got = lax.ppermute(sent, "tp", [(0, 1), (1, 0)])
    kept = call(kept_kernel, shape((HALF, width), F32), n, [v, v, n, v, n], [hidden], flops=1_000_000_000)(
        query, wide, state, stats, w_out
    )
    return (kept + got.astype(F32)).astype(BF)


def solution(mesh):
    split = Mesh(mesh.devices.reshape(4, 4, 4, mesh.shape["tp"]), ("sp_0", "sp_1", "sp_2", "tp"))
    placed = (
        P(SP_TP, None),
        P(),
        P(None, "tp"),
        P(None, "tp"),
        P(None, "tp"),
        P(None, "tp"),
        P(),
        P(),
        P(),
        P(),
        P(None, SP, "tp"),
        P(),
        P("tp", None),
    )
    return jax.shard_map(body, mesh=split, in_specs=placed, out_specs=P(SP_TP, None), check_vma=False)
```
